32 devices in a mesh: grp: 2 (over y), sp: 4 (over z), tp: 4 (over x, core).
Axes of the slice: x: 2, y: 2, z: 4, core: 2. Of those that a mesh axis runs over, the one named last changes fastest.
Arguments:
- queries: bfloat16 [6144, 512], P(('grp', 'sp'), 'tp'), parts along dimension 0, may hold values from -6 to 6
- key_projected: bfloat16 [6144, 512], P(('grp', 'sp'), 'tp'), parts along dimension 0, may hold values from -6 to 6
- values: bfloat16 [6144, 1024], P(('grp', 'sp'), 'tp'), parts along dimension 0, may hold values from -6 to 6
- output_gate_preact: bfloat16 [6144, 1024], P(('grp', 'sp'), 'tp'), parts along dimension 0, may hold values from -6 to 6
- forward_decay_logits: bfloat16 [6144, 512], P(('grp', 'sp'), 'tp'), parts along dimension 0, may hold values from -3.8 to 3.8
- backward_decay_logits: bfloat16 [6144, 512], P(('grp', 'sp'), 'tp'), parts along dimension 0, may hold values from -3.8 to 3.8
- decay_logit_shift: float32 [2, 512], P(None, 'tp'), may hold values from -1 to 13
- decay_spike_values: float32 [8, 6144], P('tp', ('grp', 'sp')), parts along dimension 1, may hold values from -2.1 to 0
- residual: bfloat16 [6144, 2048], P(('grp', 'sp', 'tp')), parts along dimension 0, may hold values from -6 to 6
- head_norm_gain: float32 [1024], P('tp'), may hold values from 0.1 to 1.9
- output_projection: bfloat16 [1024, 2048], P('tp'), may hold values from -0.1875 to 0.1875
- prenorm_gain: float32 [2048], replicated, may hold values from 0.1 to 1.9
- gate_projection: bfloat16 [2048, 5120], P('sp', 'tp'), may hold values from -0.125 to 0.125
- up_projection: bfloat16 [2048, 5120], P('sp', 'tp'), may hold values from -0.125 to 0.125
- down_projection: bfloat16 [5120, 2048], P('tp', 'sp'), may hold values from -0.078125 to 0.078125
Outputs:
- layer_output: bfloat16 [6144, 2048], P(('grp', 'sp', 'tp')), parts along dimension 0
The draws below stay inside these ranges and needn't reach their ends.
There are 2 independent parts, one for each index of `grp`. The reference program is written for one: setup_inputs(seed, part) draws one part's arguments, and reference() takes and returns one part's arrays. A program takes and returns all parts, laid end to end along the dimension named above; an argument that names none is the same for every part. Nothing has to cross between parts.
All inputs are finite; a program needn't handle non-finite values.
Results may differ from the reference program's by a relative error of at most 0.014.
Values may be sent and summed in bfloat16 or wider, within the bound.
A program may use at most 64 MiB of HBM per device.

```python
import jax
import jax.numpy as jnp
from jax import lax

D = 2048
HEAD_TOTAL = 8
KEY_CHANNELS = 64
HEAD_V = 128
FF = 5120
BLOCK = 64
TOK_DEV = 768
TOKENS = 3072
N_TP = 4


def logit_draw(key):
    noise_key, block_key = jax.random.split(key)
    noise = jnp.clip(0.7 * jax.random.normal(noise_key, (TOKENS, HEAD_TOTAL * KEY_CHANNELS), jnp.float32), -3.0, 3.0)
    shifts = jax.random.uniform(block_key, (TOKENS // TOK_DEV, 1), jnp.float32, -0.8, 0.8)
    return (noise + jnp.repeat(shifts, TOK_DEV, axis=0)).astype(jnp.bfloat16)


def draw_forward_decay_logits(key, part):
    return logit_draw(jax.random.fold_in(key, 11))


def draw_backward_decay_logits(key, part):
    return logit_draw(jax.random.fold_in(key, 12))


def draw_decay_logit_shift(key, part):
    pick_key, slow_key, quick_key = jax.random.split(jax.random.fold_in(key, 13), 3)
    fast_share = 0.5
    fast_heads = jax.random.uniform(pick_key, (2, HEAD_TOTAL), jnp.float32) < fast_share
    fast_channels = jnp.repeat(fast_heads, KEY_CHANNELS, axis=1)
    slow_start = jnp.log(TOKENS / 16.0)
    slow = slow_start + 2.5 * jax.random.uniform(slow_key, (2, HEAD_TOTAL * KEY_CHANNELS), jnp.float32)
    quick = jax.random.uniform(quick_key, (2, HEAD_TOTAL * KEY_CHANNELS), jnp.float32, -1.0, 1.0)
    return jnp.where(fast_channels, quick, slow).astype(jnp.float32)


def draw_decay_spike_values(key, part):
    spot_key, depth_key = jax.random.split(jax.random.fold_in(key, 14))
    spots = jax.random.randint(spot_key, (HEAD_TOTAL, 3), 0, TOKENS)
    depth = jax.random.uniform(depth_key, (HEAD_TOTAL, 3), jnp.float32, -0.69, -0.22)
    places = jnp.arange(TOKENS)[None, None, :] == spots[:, :, None]
    return jnp.sum(jnp.where(places, depth[:, :, None], 0.0), axis=1).astype(jnp.float32)


def block_levels(key, shape, pieces, low, largest):
    def one(position, parts):
        draws = jax.random.uniform(jax.random.fold_in(jax.random.fold_in(key, 6), position), (parts,), jnp.float32, low / len(pieces), largest / len(pieces))
        return jnp.repeat(jnp.exp(draws), shape[position] // parts).reshape((-1,) + (1,) * (len(shape) - position - 1))

    gain = one(*pieces[0])
    for cut in pieces[1:]:
        gain = gain * one(*cut)
    return gain


def gaussian(key, dims, deviation, reach, shards=(), kind=jnp.bfloat16):
    array = deviation * jax.random.normal(key, dims, jnp.float32)
    if shards:
        array = array * block_levels(key, dims, shards, -0.22, 0.18)
    return jnp.clip(array, -reach, reach).astype(kind)


def setup_inputs(seed: int = 0, part: int = 0) -> dict:
    keys = jax.random.split(jax.random.key(seed), 16)
    part_keys = jax.random.split(jax.random.fold_in(keys[15], part), 16)
    queries = gaussian(part_keys[0], (TOKENS, HEAD_TOTAL * KEY_CHANNELS), 1.0, 6.0, ((0, 4), (1, 4)))
    key_projected = gaussian(part_keys[1], (TOKENS, HEAD_TOTAL * KEY_CHANNELS), 1.0, 6.0, ((0, 4), (1, 4)))
    values = gaussian(part_keys[2], (TOKENS, HEAD_TOTAL * HEAD_V), 1.0, 6.0, ((0, 4), (1, 4)))
    output_gate_preact = gaussian(part_keys[3], (TOKENS, HEAD_TOTAL * HEAD_V), 1.0, 6.0, ((0, 4), (1, 4)))
    forward_decay_logits = draw_forward_decay_logits(jax.random.fold_in(jax.random.fold_in(keys[15], part), 71), part)
    backward_decay_logits = draw_backward_decay_logits(jax.random.fold_in(jax.random.fold_in(keys[15], part), 71), part)
    decay_logit_shift = draw_decay_logit_shift(jax.random.fold_in(keys[15], 71), part)
    decay_spike_values = draw_decay_spike_values(jax.random.fold_in(jax.random.fold_in(keys[15], part), 71), part)
    residual = gaussian(part_keys[8], (TOKENS, D), 1.0, 6.0, ((0, 16),))
    head_norm_gain = jnp.clip(1.0 + 0.18 * jax.random.normal(keys[9], (HEAD_TOTAL * HEAD_V,), jnp.float32), 0.1, 1.9)
    output_projection = gaussian(keys[10], (HEAD_TOTAL * HEAD_V, D), (HEAD_TOTAL * HEAD_V) ** -0.5, 0.1875, ((0, 4),))
    prenorm_gain = jnp.clip(1.0 + 0.18 * jax.random.normal(keys[11], (D,), jnp.float32), 0.1, 1.9)
    gate_projection = gaussian(keys[12], (D, FF), D ** -0.5, 0.125, ((0, 4), (1, 4)))
    up_projection = gaussian(keys[13], (D, FF), D ** -0.5, 0.125, ((0, 4), (1, 4)))
    down_projection = gaussian(keys[14], (FF, D), FF ** -0.5, 0.078125, ((0, 4), (1, 4)))
    return dict(queries=queries, key_projected=key_projected, values=values, output_gate_preact=output_gate_preact, forward_decay_logits=forward_decay_logits, backward_decay_logits=backward_decay_logits, decay_logit_shift=decay_logit_shift, decay_spike_values=decay_spike_values, residual=residual, head_norm_gain=head_norm_gain, output_projection=output_projection, prenorm_gain=prenorm_gain, gate_projection=gate_projection, up_projection=up_projection, down_projection=down_projection)


gate_denominator = 16.0
norm_epsilon = 1e-06

def block_sweep(query_in, key_in, values_in, log_decay, span):
    sequence_length, head_count, key_dim = key_in.shape
    block_count = sequence_length // span

    def blocks(tensor):
        return jnp.transpose(tensor.reshape(block_count, span, head_count, tensor.shape[-1]), (0, 2, 1, 3))
    lower_mask = jnp.tril(jnp.ones((span, span), dtype=bool))[:, :, None]

    def advance(carried, inputs):
        memory, offset = carried
        key_blk, value_blk, decay_blk, query_blk = inputs
        within = jnp.cumsum(decay_blk, axis=1)
        ending = within[:, -1, :]
        memory_next = jnp.exp(ending)[:, :, None] * memory + jnp.einsum('hjd,hje->hde', key_blk * jnp.exp(ending[:, None, :] - within), value_blk, precision=lax.Precision.HIGHEST)
        result = jnp.einsum('hid,hde->hie', query_blk * jnp.exp(within), memory, precision=lax.Precision.HIGHEST)
        spread = jnp.exp(jnp.where(lower_mask, within[:, :, None, :] - within[:, None, :, :], -jnp.inf))
        scores = jnp.einsum('hid,hjd,hijd->hij', query_blk, key_blk, spread, precision=lax.Precision.HIGHEST)
        result = result + jnp.einsum('hij,hje->hie', scores, value_blk, precision=lax.Precision.HIGHEST)
        reached = query_blk * jnp.exp(within + offset[:, None, :])
        return ((memory_next, offset + ending), (result, reached))
    start_memory = jnp.zeros((head_count, key_dim, values_in.shape[-1]), jnp.float32)
    start_offset = jnp.zeros((head_count, key_dim), jnp.float32)
    (memory, decay_total), (outputs, reached) = lax.scan(advance, (start_memory, start_offset), (blocks(key_in), blocks(values_in), blocks(log_decay), blocks(query_in)))

    def unblock(tensor):
        return jnp.transpose(tensor, (0, 2, 1, 3)).reshape(sequence_length, head_count, tensor.shape[-1])
    return (unblock(outputs), unblock(reached), memory, decay_total)

def head_mix(combined, head_norm_gain, output_gate_preact):
    sequence_length, head_count, width = combined.shape
    inverse = lax.rsqrt(lax.optimization_barrier(jnp.mean(combined * combined, axis=-1, keepdims=True)) + norm_epsilon)
    gate_act = jax.nn.silu(output_gate_preact.astype(jnp.float32).reshape(sequence_length, head_count, width))
    weighted = combined * inverse * head_norm_gain.reshape(head_count, width) * gate_act
    return weighted.reshape(sequence_length, head_count * width).astype(jnp.bfloat16)

def row_norm(mid_rows, prenorm_gain):
    wide = mid_rows.astype(jnp.float32)
    inverse = lax.rsqrt(lax.optimization_barrier(jnp.mean(wide * wide, axis=-1, keepdims=True)) + norm_epsilon)
    return (wide * inverse * prenorm_gain).astype(jnp.bfloat16)

def reference(queries, key_projected, values, output_gate_preact, forward_decay_logits, backward_decay_logits, decay_logit_shift, decay_spike_values, residual, head_norm_gain, output_projection, prenorm_gain, gate_projection, up_projection, down_projection):
    sequence_length = queries.shape[0]
    query_f = queries.astype(jnp.float32).reshape(sequence_length, HEAD_TOTAL, KEY_CHANNELS) * KEY_CHANNELS ** (-0.5)
    keys_f = key_projected.astype(jnp.float32).reshape(sequence_length, HEAD_TOTAL, KEY_CHANNELS)
    values_f = values.astype(jnp.float32).reshape(sequence_length, HEAD_TOTAL, HEAD_V)
    decay_spikes = jnp.transpose(decay_spike_values)[:, :, None]
    logit_shifts = decay_logit_shift.reshape(2, HEAD_TOTAL, KEY_CHANNELS)
    forward_decay = jax.nn.log_sigmoid(forward_decay_logits.astype(jnp.float32).reshape(sequence_length, HEAD_TOTAL, KEY_CHANNELS) + logit_shifts[0]) / gate_denominator + decay_spikes
    backward_decay = jax.nn.log_sigmoid(backward_decay_logits.astype(jnp.float32).reshape(sequence_length, HEAD_TOTAL, KEY_CHANNELS) + logit_shifts[1]) / gate_denominator + decay_spikes
    fwd_out = block_sweep(query_f, keys_f, values_f, forward_decay, BLOCK)[0]
    bwd_out = block_sweep(query_f[::-1], keys_f[::-1], values_f[::-1], backward_decay[::-1], BLOCK)[0][::-1]
    attended = head_mix(fwd_out + bwd_out, head_norm_gain, output_gate_preact)
    projected = jnp.dot(attended, output_projection, preferred_element_type=jnp.float32)
    mid_rows = (residual.astype(jnp.float32) + projected).astype(jnp.bfloat16)
    normed = row_norm(mid_rows, prenorm_gain)
    gate_part = jnp.dot(normed, gate_projection, preferred_element_type=jnp.float32)
    up_part = jnp.dot(normed, up_projection, preferred_element_type=jnp.float32)
    hidden = (jax.nn.silu(gate_part) * up_part).astype(jnp.bfloat16)
    group_width = FF // N_TP
    summed = jnp.zeros((sequence_length, D), jnp.float32)
    for group_index in range(N_TP):
        low = group_index * group_width
        partial_value = jnp.dot(hidden[:, low:low + group_width], down_projection[low:low + group_width], preferred_element_type=jnp.float32).astype(jnp.bfloat16)
        summed = summed + lax.optimization_barrier(partial_value).astype(jnp.float32)
    return (mid_rows.astype(jnp.float32) + 0.5 * summed).astype(jnp.bfloat16)
```

```python
import functools

import jax
import jax.numpy as jnp
from jax import lax
from jax.experimental import pallas as pl
from jax.experimental.pallas import tpu as pltpu
from jax.sharding import PartitionSpec as P


KEY_CHANNELS = 64
HEAD_V = 128
BLOCK = 64
GATE_DENOMINATOR = 16.0
EPSILON = 1e-06
F32, BF16 = jnp.float32, jnp.bfloat16


def nt(a, b):
    return lax.dot_general(a, b, (((1,), (1,)), ((), ())), preferred_element_type=F32)


def tn(a, b):
    return lax.dot_general(a, b, (((0,), (0,)), ((), ())), preferred_element_type=F32)


def first_head(shape):
    return lax.broadcasted_iota(jnp.int32, shape, 1) < KEY_CHANNELS


VMEM = pl.BlockSpec(memory_space=pltpu.VMEM)


def cost(flops, size):
    return pl.CostEstimate(flops=flops, bytes_accessed=size, transcendentals=0)


def entering(value, axis, join, neutral, backward):
    count = lax.axis_size(axis)
    place = lax.axis_index(axis)
    ahead = count - 1 - place if backward else place
    gathered = jax.tree.map(
        lambda a, kind: lax.all_gather(a.astype(kind), axis), value, (jnp.bfloat16, jnp.bfloat16)
    )
    state = jax.tree.map(lambda a, e: jnp.zeros_like(a) + jnp.asarray(e, a.dtype), value, neutral)

    def one(lap, state):
        source = count - 1 - lap if backward else lap
        return join(
            state,
            jax.tree.map(
                lambda a, own: lax.dynamic_index_in_dim(a, source, 0, False).astype(own.dtype),
                gathered,
                value,
            ),
        )

    return lax.fori_loop(0, ahead, one, state)


def block_sweep(query_in, key_in, values_in, log_decay, span):
    sequence_length, head_count, key_dim = key_in.shape
    block_count = sequence_length // span

    def blocks(tensor):
        return jnp.transpose(
            tensor.reshape(block_count, span, head_count, tensor.shape[-1]), (0, 2, 1, 3)
        )

    lower_mask = jnp.tril(jnp.ones((span, span), dtype=bool))[:, :, None]

    def advance(carried, inputs):
        memory, offset = carried
        key_blk, value_blk, decay_blk, query_blk = inputs
        within = jnp.cumsum(decay_blk, axis=1)
        ending = within[:, -1, :]
        memory_next = jnp.exp(ending)[:, :, None] * memory + jnp.einsum(
            "hjd,hje->hde",
            key_blk * jnp.exp(ending[:, None, :] - within),
            value_blk,
            precision=lax.Precision.HIGHEST,
        )
        result = jnp.einsum(
            "hid,hde->hie", query_blk * jnp.exp(within), memory, precision=lax.Precision.HIGHEST
        )
        spread = jnp.exp(
            jnp.where(lower_mask, within[:, :, None, :] - within[:, None, :, :], -jnp.inf)
        )
        scores = jnp.einsum(
            "hid,hjd,hijd->hij", query_blk, key_blk, spread, precision=lax.Precision.HIGHEST
        )
        result = result + jnp.einsum(
            "hij,hje->hie", scores, value_blk, precision=lax.Precision.HIGHEST
        )
        reached = query_blk * jnp.exp(within + offset[:, None, :])
        return ((memory_next, offset + ending), (result, reached))

    start_memory = jnp.zeros((head_count, key_dim, values_in.shape[-1]), jnp.float32)
    start_offset = jnp.zeros((head_count, key_dim), jnp.float32)
    (memory, decay_total), (outputs, reached) = lax.scan(
        advance,
        (start_memory, start_offset),
        (blocks(key_in), blocks(values_in), blocks(log_decay), blocks(query_in)),
    )

    def unblock(tensor):
        return jnp.transpose(tensor, (0, 2, 1, 3)).reshape(
            sequence_length, head_count, tensor.shape[-1]
        )

    return (unblock(outputs), unblock(reached), memory, decay_total)


def head_mix(combined, head_norm_gain, output_gate_preact):
    sequence_length, head_count, width = combined.shape
    inverse = lax.rsqrt(jnp.mean(combined * combined, axis=-1, keepdims=True) + EPSILON)
    gate_act = jax.nn.silu(
        output_gate_preact.astype(jnp.float32).reshape(sequence_length, head_count, width)
    )
    weighted = combined * inverse * head_norm_gain.reshape(head_count, width) * gate_act
    return weighted.reshape(sequence_length, head_count * width).astype(jnp.bfloat16)


def row_norm(mid_rows, prenorm_gain):
    wide = mid_rows.astype(jnp.float32)
    inverse = lax.rsqrt(jnp.mean(wide * wide, axis=-1, keepdims=True) + EPSILON)
    return (wide * inverse * prenorm_gain).astype(jnp.bfloat16)


def combine_states(earlier, later):
    decay_early, memory_early = earlier
    decay_late, memory_late = later
    return (decay_early * decay_late, decay_late[:, :, None] * memory_early + memory_late)


def body(
    queries,
    key_projected,
    values,
    output_gate_preact,
    forward_decay_logits,
    backward_decay_logits,
    decay_logit_shift,
    decay_spike_values,
    residual,
    head_norm_gain,
    output_projection,
    prenorm_gain,
    gate_projection,
    up_projection,
    down_projection,
):
    sequence_length = queries.shape[0]
    local_heads = queries.shape[1] // KEY_CHANNELS
    query_f = queries.astype(jnp.float32).reshape(
        sequence_length, local_heads, KEY_CHANNELS
    ) * KEY_CHANNELS ** (-0.5)
    keys_f = key_projected.astype(jnp.float32).reshape(sequence_length, local_heads, KEY_CHANNELS)
    values_f = values.astype(jnp.float32).reshape(sequence_length, local_heads, HEAD_V)
    decay_spikes = jnp.transpose(decay_spike_values)[:, :, None]
    logit_shifts = decay_logit_shift.reshape(2, local_heads, KEY_CHANNELS)
    forward_decay = (
        jax.nn.log_sigmoid(
            forward_decay_logits.astype(jnp.float32).reshape(
                sequence_length, local_heads, KEY_CHANNELS
            )
            + logit_shifts[0]
        )
        / GATE_DENOMINATOR
        + decay_spikes
    )
    backward_decay = (
        jax.nn.log_sigmoid(
            backward_decay_logits.astype(jnp.float32).reshape(
                sequence_length, local_heads, KEY_CHANNELS
            )
            + logit_shifts[1]
        )
        / GATE_DENOMINATOR
        + decay_spikes
    )
    fwd_out, fwd_reach, fwd_memory, fwd_total = block_sweep(
        query_f, keys_f, values_f, forward_decay, BLOCK
    )
    bwd_out, bwd_reach, bwd_memory, bwd_total = block_sweep(
        query_f[::-1], keys_f[::-1], values_f[::-1], backward_decay[::-1], BLOCK
    )
    identity = (jnp.ones_like(fwd_total), jnp.zeros_like(fwd_memory))
    fwd_incoming = entering(
        (jnp.exp(fwd_total), fwd_memory), "sp", combine_states, identity, False
    )[1]
    bwd_incoming = entering((jnp.exp(bwd_total), bwd_memory), "sp", combine_states, identity, True)[
        1
    ]
    fwd_full = fwd_out + jnp.einsum(
        "lhd,hde->lhe", fwd_reach, fwd_incoming, precision=lax.Precision.HIGHEST
    )
    bwd_full = bwd_out + jnp.einsum(
        "lhd,hde->lhe", bwd_reach, bwd_incoming, precision=lax.Precision.HIGHEST
    )
    attended = head_mix(fwd_full + bwd_full[::-1], head_norm_gain, output_gate_preact)
    token_rows = lax.all_to_all(attended, "tp", split_axis=0, concat_axis=1, tiled=True)
    whole_out = lax.all_gather(output_projection, "tp", axis=0, tiled=True)
    projected = jnp.dot(token_rows, whole_out, preferred_element_type=jnp.float32)
    mid_rows = (residual.astype(jnp.float32) + projected).astype(jnp.bfloat16)
    normed = row_norm(mid_rows, prenorm_gain)
    fetched = (
        lax.all_gather(gate_projection, "sp", axis=0, tiled=True),
        lax.all_gather(up_projection, "sp", axis=0, tiled=True),
        lax.all_gather(down_projection, "sp", axis=1, tiled=True),
    )
    gate_full, up_full, down_full = fetched
    piece = lax.all_gather(normed, "tp", axis=0, tiled=True)
    gate_part = jnp.dot(piece, gate_full, preferred_element_type=jnp.float32)
    up_part = jnp.dot(piece, up_full, preferred_element_type=jnp.float32)
    hidden = (jax.nn.silu(gate_part) * up_part).astype(jnp.bfloat16)
    summed = lax.psum_scatter(
        jnp.dot(hidden, down_full, preferred_element_type=jnp.float32).astype(jnp.bfloat16),
        "tp",
        scatter_dimension=0,
        tiled=True,
    ).astype(jnp.float32)
    return (mid_rows.astype(jnp.float32) + 0.5 * summed).astype(jnp.bfloat16)


MESH = pl.DeviceIdType.MESH
PIECES = 5


def log_decay(logits, shift, spike):
    x = logits.astype(F32) + shift
    soft = jnp.minimum(x, 0.0) - jnp.log1p(jnp.exp(-jnp.abs(x)))
    return soft / GATE_DENOMINATOR + spike


def own_states(k_ref, v_ref, fd_ref, bd_ref, shift_ref, spike_ref, within_ref, kd_ref, fwd_ref, bwd_ref):
    tokens, lanes = k_ref.shape
    blocks = tokens // BLOCK
    row = lax.broadcasted_iota(jnp.int32, (2 * BLOCK, 2 * BLOCK), 0)
    col = lax.broadcasted_iota(jnp.int32, (2 * BLOCK, 2 * BLOCK), 1)
    r, c = row % BLOCK, col % BLOCK
    ahead = jnp.where(row < BLOCK, r - c, c - r)
    tri = jnp.where(ahead >= 0, 1.0, 0.0).astype(BF16)
    half = first_head((BLOCK, lanes))
    ends = []
    for b in range(blocks):
        at = slice(b * BLOCK, (b + 1) * BLOCK)
        spike = jnp.where(half, spike_ref[at, 0:1], spike_ref[at, 1:2])
        parts = [log_decay(ref[at, :], shift_ref[n : n + 1, :], spike) for n, ref in enumerate((fd_ref, bd_ref))]
        d = jnp.concatenate(parts, axis=1)
        hi = d.astype(BF16)
        lo = (d - hi.astype(F32)).astype(BF16)
        both = jnp.dot(tri, jnp.concatenate([hi, lo], axis=0), preferred_element_type=F32)
        fwd, bwd = both[:BLOCK, :lanes], both[BLOCK:, lanes:]
        within_ref[at, :lanes] = fwd
        within_ref[at, lanes:] = bwd
        ends.append((fwd[BLOCK - 1 :, :], bwd[:1, :]))
    zero = jnp.zeros((1, lanes), F32)
    after, before = [zero] * blocks, [zero] * blocks
    for b in range(1, blocks):
        before[b] = before[b - 1] + ends[b - 1][1]
        after[blocks - 1 - b] = after[blocks - b] + ends[blocks - b][0]
    totals = after[0] + ends[0][0], before[-1] + ends[-1][1]
    for b in range(blocks):
        at = slice(b * BLOCK, (b + 1) * BLOCK)
        key = k_ref[at, :].astype(F32)
        kd_ref[at, :lanes] = (key * jnp.exp((ends[b][0] + after[b]) - within_ref[at, :lanes])).astype(BF16)
        kd_ref[at, lanes:] = (key * jnp.exp((ends[b][1] + before[b]) - within_ref[at, lanes:])).astype(BF16)
    full = tn(v_ref[...], kd_ref[...])
    mine = first_head((HEAD_V, lanes))
    for n, ref in enumerate((fwd_ref, bwd_ref)):
        u = full[:, n * lanes : (n + 1) * lanes]
        ref[:HEAD_V, :] = jnp.where(mine, u[:HEAD_V], u[HEAD_V:]).astype(BF16)
        ref[HEAD_V:, :] = jnp.broadcast_to(jnp.exp(totals[n]), (16, lanes)).astype(BF16)


def spread(state):
    mine = first_head(state.shape)
    return jnp.concatenate([jnp.where(mine, state, 0.0), jnp.where(mine, 0.0, state)], axis=0).astype(BF16)


def pack(u):
    top = u[:HEAD_V]
    return jnp.where(first_head(top.shape), top, u[HEAD_V:])


def backward_states(k_ref, v_ref, within_ref, state, held_ref):
    tokens, lanes = k_ref.shape
    for b in reversed(range(tokens // BLOCK)):
        at = slice(b * BLOCK, (b + 1) * BLOCK)
        held_ref[b] = spread(state)
        within = within_ref[at, lanes:]
        end = within[:1, :]
        kd = (k_ref[at, :].astype(F32) * jnp.exp(end - within)).astype(BF16)
        state = state * jnp.exp(end) + pack(tn(v_ref[at, :], kd))


def attend(q_ref, k_ref, v_ref, within_ref, gate_ref, gain_ref, fwd_state, held_ref, out_ref):
    tokens, lanes = k_ref.shape
    row = lax.broadcasted_iota(jnp.int32, (2 * BLOCK, BLOCK), 0) % BLOCK
    col = lax.broadcasted_iota(jnp.int32, (2 * BLOCK, BLOCK), 1)
    half = first_head((BLOCK, lanes))
    for b in range(tokens // BLOCK):
        at = slice(b * BLOCK, (b + 1) * BLOCK)
        query = q_ref[at, :].astype(F32) * KEY_CHANNELS ** (-0.5)
        key = k_ref[at, :].astype(F32)
        value = v_ref[at, :]
        scores, reach = [], []
        for n in range(2):
            within = within_ref[at, n * lanes : (n + 1) * lanes]
            pivot = within[BLOCK // 2 - 1 + n : BLOCK // 2 + n, :]
            near = (query * jnp.exp(within - pivot)).astype(BF16)
            far = (key * jnp.exp(pivot - within)).astype(BF16)
            zero = jnp.zeros_like(near)
            pair = jnp.concatenate([jnp.where(half, near, zero), jnp.where(half, zero, near)], axis=0)
            scores.append(nt(pair, far))
            reach.append((query * jnp.exp(within)).astype(BF16))
        score = (jnp.where(col <= row, scores[0], 0.0) + jnp.where(col >= row, scores[1], 0.0)).astype(BF16)
        states = jnp.concatenate([spread(fwd_state), held_ref[b]], axis=1)
        result = nt(jnp.concatenate(reach, axis=1), states)
        for h in range(2):
            lane = slice(h * HEAD_V, (h + 1) * HEAD_V)
            x = result[:, lane] + jnp.dot(
                score[h * BLOCK : (h + 1) * BLOCK], value[:, lane], preferred_element_type=F32
            )
            inverse = lax.rsqrt(jnp.mean(x * x, axis=-1, keepdims=True) + EPSILON)
            g = gate_ref[at, lane].astype(F32)
            out_ref[at, lane] = (x * inverse * gain_ref[:, lane] * (g * jax.nn.sigmoid(g))).astype(BF16)
        within = within_ref[at, :lanes]
        end = within[BLOCK - 1 :, :]
        kd = (key * jnp.exp(end - within)).astype(BF16)
        fwd_state = fwd_state * jnp.exp(end) + pack(tn(value, kd))


def pick(i, table):
    value = table[0]
    for n, item in enumerate(table[1:], 1):
        value = jnp.where(i == n, item, value)
    return value


def ds(first, size):
    return pl.ds(pl.multiple_of(first, size if size % 128 == 0 else 16), size)


def layer_kernel(
    k_ref, v_ref, fd_ref, bd_ref, shift_ref, spike_ref, q_ref, gate_ref, gain_ref, norm_ref,
    res_hbm, out_hbm, g_hbm, u_hbm, d_hbm,
    out_ref,
    within, kd, fown, bown, fgot, bgot, fstate, bstate, held, attended, rows, outw, res, mid, acts,
    wg, wu, wd, hid, part, got, xsend, xgot, esend, egot, erelay,
    loc, st_s, st_r, a2a_s, a2a_r, ow_s, ow_r, ag_s, ag_r, ea_s, gs, gr, dsd, drv, cr_s, cr_r, xo_s, xo_r,
    eo_s, eo_r, er_s, er_r,
):
    count = lax.axis_size("sp")
    side, place, me = lax.axis_index("grp"), lax.axis_index("sp"), lax.axis_index("tp")
    chip, core = me // 2, me % 2
    tc, tx, td = 2 * chip + 1 - core, 2 * (1 - chip) + core, 2 * (1 - chip) + 1 - core
    upper = place // 2
    e, m, o, oe = 3 * upper, 1 + upper, 2 - upper, 3 - 3 * upper
    middle = place * (count - 1 - place) > 0
    own = res.shape[0]
    width = attended.shape[1]
    model = mid.shape[1]
    depth, hidden = g_hbm.shape
    tile = hidden // PIECES
    hr = depth // 2
    dr = hidden // 4
    dw = d_hbm.shape[1]
    orow = width // 4
    nrow = own // 2

    def remote(src, dst, send, recv, **dev):
        return pltpu.make_async_remote_copy(
            src_ref=src, dst_ref=dst, send_sem=send, recv_sem=recv, device_id=dev, device_id_type=MESH
        )

    def gu(n, source, half, p, local=False, **dev):
        dst = (wg, wu)[n].at[p, ds(source * depth + half * hr, hr), :]
        src = (g_hbm, u_hbm)[n].at[ds(half * hr, hr), ds(p * tile, tile)] if local else dst
        return remote(src, dst, gs.at[n, source, half, p], gr.at[n, source, half, p], **(dev or dict(sp=o)))

    def dn(source, half, p, local=False, **dev):
        at = ds(half * 2 * dr + p * dr, dr)
        dst = wd.at[source, at, :]
        src = d_hbm.at[at, :] if local else dst
        return remote(src, dst, dsd.at[source, half, p], drv.at[source, half, p], **(dev or dict(sp=o)))

    def send_gu(source, half, p, local=False, **dev):
        for n in range(2):
            gu(n, source, half, p, local, **dev).start()

    def take_gu(source, half, p):
        for n in range(2):
            gu(n, source, half, p).wait_recv()

    def relay_gu(source, p, **dev):
        take_gu(source, side, p)
        send_gu(source, side, p, **dev)

    def relay_dn(source, p, **dev):
        dn(source, side, p).wait_recv()
        dn(source, side, p, **dev).start()

    def ow(kind, block, i, dev, local=False):
        dst = outw.at[ds(block * width + i * orow, orow), :]
        src = out_hbm.at[i * orow : (i + 1) * orow, :] if local else dst
        return remote(src, dst, ow_s.at[kind, i], ow_r.at[block, i], tp=dev)

    def relay_ow(i):
        ow(2, tx, i, tc).wait_recv()
        ow(2, tx, i, tc).start()

    def a2a(n, block, dev):
        return remote(
            attended.at[ds(dev * own, own), :], rows.at[:, ds(block * width, width)], a2a_s.at[n], a2a_r.at[block], tp=dev
        )

    def ag(q, kind, block, i, dev):
        at = acts.at[q, ds(block * own + i * nrow, nrow), :]
        return remote(at, at, ag_s.at[q, kind, i], ag_r.at[q, block, i], tp=dev)

    def to_host(i):
        at = ds(me * own + i * nrow, nrow)
        return remote(acts.at[0, at, :], acts.at[1, at, :], ea_s.at[i], ag_r.at[1, me, i], sp=m)

    def state_copy(n, k, dev):
        src, dst = ((fown, fgot), (bown, bgot))[n]
        return remote(src, dst.at[k - 1], st_s.at[n, k - 1], st_r.at[n, k - 1], sp=dev)

    def cr(q, i, j):
        block = 2 * j + 1 - core
        return remote(part.at[q, i, ds(block * own, own), :], got.at[q, i, j], cr_s.at[q, i, j], cr_r.at[q, i, j], tp=tc)

    def xo(i):
        return remote(xsend.at[i], xgot.at[i], xo_s.at[i], xo_r.at[i], tp=tx)

    def eo(i, n):
        dst = egot.at[0, i] if n == 0 else erelay.at[i]
        return remote(esend.at[i, n], dst, eo_s.at[i, n], eo_r.at[i, n], sp=e)

    def er(i):
        return remote(erelay.at[i], egot.at[1, i], er_s.at[i], er_r.at[i], tp=tx)

    own_copies = []
    for p in range(PIECES):
        for n in range(2):
            own_copies.append(
                pltpu.make_async_copy(
                    (g_hbm, u_hbm)[n].at[:, p * tile : (p + 1) * tile],
                    (wg, wu)[n].at[p, ds(place * depth, depth), :],
                    loc.at[n * PIECES + p],
                )
            )
    own_copies.append(pltpu.make_async_copy(d_hbm, wd.at[place], loc.at[2 * PIECES]))
    own_out = pltpu.make_async_copy(out_hbm, outw.at[ds(me * width, width), :], loc.at[2 * PIECES + 1])
    own_res = pltpu.make_async_copy(res_hbm, res, loc.at[2 * PIECES + 2])

    barrier = pltpu.get_barrier_semaphore()
    friends = [dict(sp=lax.rem(place + k, count)) for k in range(1, count)]
    friends += [dict(grp=1 - side)] + [dict(tp=t) for t in (tc, tx, td)]
    for friend in friends:
        pl.semaphore_signal(barrier, inc=1, device_id=friend, device_id_type=MESH)
    pl.semaphore_wait(barrier, len(friends))

    @pl.when(middle)
    def _():
        send_gu(place, side, 0, True, sp=o)

    @pl.when(jnp.logical_not(middle))
    def _():
        send_gu(place, side, 0, True, sp=m)

    for i in range(4):
        ow(0, me, i, tx, True).start()
    for i in range(4):
        ow(1, me, i, tc, True).start()
    own_out.start()
    own_res.start()

    own_states(k_ref, v_ref, fd_ref, bd_ref, shift_ref, spike_ref, within, kd, fown, bown)
    for k in range(1, count):

        @pl.when(place + k < count)
        def _(k=k):
            state_copy(0, k, place + k).start()

        @pl.when(place >= k)
        def _(k=k):
            state_copy(1, k, place - k).start()

    @pl.when(middle)
    def _():
        for copy in own_copies:
            copy.start()
        for p in range(1, PIECES):
            send_gu(place, side, p, True, sp=o)
        relay_gu(o, 0, grp=1 - side)

    @pl.when(jnp.logical_not(middle))
    def _():
        for p in range(1, PIECES):
            send_gu(place, side, p, True, sp=m)

    fstate[...] = jnp.zeros_like(fstate)
    bstate[...] = jnp.zeros_like(bstate)
    for k in reversed(range(1, count)):

        @pl.when(place >= k)
        def _(k=k):
            state_copy(0, k, place).wait_recv()
            decay = fgot[k - 1, HEAD_V : HEAD_V + 1, :].astype(F32)
            fstate[...] = fstate[...] * decay + fgot[k - 1, :HEAD_V, :].astype(F32)

        @pl.when(place + k < count)
        def _(k=k):
            state_copy(1, k, place).wait_recv()
            decay = bgot[k - 1, HEAD_V : HEAD_V + 1, :].astype(F32)
            bstate[...] = bstate[...] * decay + bgot[k - 1, :HEAD_V, :].astype(F32)

    relay_ow(0)
    backward_states(k_ref, v_ref, within, bstate[...], held)

    @pl.when(middle)
    def _():
        relay_gu(o, 1, grp=1 - side)

    relay_ow(1)
    attend(q_ref, k_ref, v_ref, within, gate_ref, gain_ref, fstate[...], held, attended)
    others = (tx, td, tc)
    for n, t in enumerate(others):
        a2a(n, me, t).start()
    rows[:, ds(me * width, width)] = attended[ds(me * own, own), :]

    @pl.when(middle)
    def _():
        relay_gu(e, 0, sp=o)
        relay_gu(e, 1, sp=o)
        relay_gu(o, 2, grp=1 - side)

    relay_ow(2)

    @pl.when(middle)
    def _():
        relay_gu(e, 2, sp=o)
        relay_gu(o, 3, grp=1 - side)
        relay_gu(e, 3, sp=o)

    relay_ow(3)
    for t in others:
        a2a(0, t, t).wait_recv()
    for t in (tc, td):
        for i in range(4):
            ow(0, t, i, tc).wait_recv()
    own_out.wait()
    own_res.wait()

    total = jnp.zeros((own, 1), F32)
    wide = 512
    for n in range(model // wide):
        at = slice(n * wide, (n + 1) * wide)
        projected = jnp.dot(rows[...], outw[:, at], preferred_element_type=F32)
        mixed = (res[:, at].astype(F32) + projected).astype(BF16)
        mid[:, at] = mixed
        mixed = mixed.astype(F32)
        total += jnp.sum(mixed * mixed, axis=-1, keepdims=True)
    inverse = lax.rsqrt(total / model + EPSILON)
    for n in range(model // wide):
        at = slice(n * wide, (n + 1) * wide)
        acts[0, ds(me * own, own), at] = (mid[:, at].astype(F32) * inverse * norm_ref[:, at]).astype(BF16)

    def target(i):
        return pick(i, (m, o, oe, e))

    @pl.when(middle)
    def _():
        for i in range(2):
            ag(0, 0, me, i, tx).start()
            ag(0, 1, me, i, tc).start()
        relay_gu(o, 4, grp=1 - side)
        relay_gu(e, 4, sp=o)
        for p in range(2):
            dn(place, side, p, True, sp=o).start()
        for copy in own_copies:
            copy.wait()

        def relay_own(i):
            ag(0, 2, tx, i, tc).wait_recv()
            ag(0, 2, tx, i, tc).start()

        def relay_hosted(i):
            ag(1, 0, me, i, tx).wait_recv()
            ag(1, 0, me, i, tx).start()
            ag(1, 1, me, i, tc).start()

        relay_gu(oe, 0, grp=1 - side)
        relay_own(0)
        relay_gu(oe, 1, grp=1 - side)
        relay_hosted(0)
        relay_gu(oe, 2, grp=1 - side)
        relay_own(1)
        relay_hosted(1)
        relay_gu(oe, 3, grp=1 - side)

        order = [(0, 0), (0, 1), (0, 2), (1, 0), (0, 3), (1, 1), (0, 4), (1, 2), (1, 3), (1, 4)]

        def first(i, carry):
            q, j = pick(i, [a for a, _ in order]), pick(i, [b for _, b in order])

            @pl.when(i == 0)
            def _():
                for t in (tc, td):
                    for n in range(2):
                        ag(0, 0, t, n, tc).wait_recv()

            @pl.when(i == 1)
            def _():
                relay_gu(oe, 4, grp=1 - side)

            for n in range(2):

                @pl.when(i == 2 + n)
                def _(n=n):
                    ag(1, 2, tx, n, tc).wait_recv()
                    ag(1, 2, tx, n, tc).start()

            @pl.when(i == 3)
            def _():
                for t in (tc, td):
                    for n in range(2):
                        ag(1, 0, t, n, tc).wait_recv()

            for n in range(2):

                @pl.when(i == 5 + n)
                def _(n=n):
                    relay_dn(o, n, grp=1 - side)

            @pl.when(q == 0)
            def _():
                for source in (o, oe, e):
                    take_gu(source, 1 - side, j)

            g = jnp.dot(acts[q], wg[j], preferred_element_type=F32)
            u = jnp.dot(acts[q], wu[j], preferred_element_type=F32)
            hid[q, :, ds(j * tile, tile)] = (g * jax.nn.sigmoid(g) * u).astype(BF16)
            return carry

        lax.fori_loop(0, len(order), first, 0)

        def fold(i, q):
            for j in range(2):
                cr(q, i, j).wait_recv()

            def both(block, j):
                return part[q, i, ds(block * own, own), :].astype(F32) + got[q, i, j].astype(F32)

            @pl.when(q == 0)
            def _():
                xsend[i] = both(tx, 1 - chip).astype(BF16)
                xo(i).start()

            @pl.when(q == 1)
            def _():
                esend[i, 0] = both(me, chip).astype(BF16)
                eo(i, 0).start()
                esend[i, 1] = both(tx, 1 - chip).astype(BF16)
                eo(i, 1).start()

        def second(s, carry):
            i, q = s // 2, s % 2

            @pl.when(s == 2)
            def _():
                relay_dn(e, 0, sp=o)
                for p in range(2):
                    dn(o, 1 - side, p).wait_recv()

            @pl.when(s == 3)
            def _():
                relay_dn(e, 1, sp=o)
                relay_dn(oe, 0, grp=1 - side)

            @pl.when(s == 4)
            def _():
                relay_dn(oe, 1, grp=1 - side)
                for p in range(2):
                    dn(oe, 1 - side, p).wait_recv()

            @pl.when(s == 6)
            def _():
                for p in range(2):
                    dn(e, 1 - side, p).wait_recv()

            part[q, i] = jnp.dot(hid[q], wd[target(i)], preferred_element_type=F32).astype(BF16)
            for j in range(2):
                cr(q, i, j).start()

            @pl.when(s > 0)
            def _():
                fold((s - 1) // 2, (s + 1) % 2)

            return carry

        lax.fori_loop(0, 2 * count, second, 0)
        fold(count - 1, 1)

        for i in range(count):
            xo(i).wait_recv()
            at = ds(target(i) * dw, dw)
            total = part[0, i, ds(me * own, own), :].astype(F32) + got[0, i, chip].astype(F32) + xgot[i].astype(F32)
            out_ref[:, at] = (mid[:, at].astype(F32) + 0.5 * total).astype(BF16)

        for p in range(PIECES):
            for n in range(2):
                gu(n, place, side, p, True).wait_send()
                for source in (e, o, oe):
                    gu(n, source, side, p).wait_send()
        for p in range(2):
            dn(place, side, p, True).wait_send()
            for source in (e, o, oe):
                dn(source, side, p).wait_send()
        for q in range(2):
            for kind in range(3):
                for i in range(2):
                    ag(q, kind, me, i, tc).wait_send()
            for i in range(count):
                for j in range(2):
                    cr(q, i, j).wait_send()
        for i in range(count):
            xo(i).wait_send()
            for n in range(2):
                eo(i, n).wait_send()

    @pl.when(jnp.logical_not(middle))
    def _():
        for i in range(2):
            to_host(i).start()
        for p in range(PIECES):
            send_gu(place, 1 - side, p, True, sp=m)
        for half in (side, 1 - side):
            for p in range(2):
                dn(place, half, p, True, sp=m).start()
        for i in range(count):
            eo(i, 1).wait_recv()
            er(i).start()
        for i in range(count):
            eo(i, 0).wait_recv()
            er(i).wait_recv()
            at = ds(target(i) * dw, dw)
            total = egot[0, i].astype(F32) + egot[1, i].astype(F32)
            out_ref[:, at] = (mid[:, at].astype(F32) + 0.5 * total).astype(BF16)
        for i in range(2):
            to_host(i).wait_send()
        for half in (side, 1 - side):
            for p in range(PIECES):
                for n in range(2):
                    gu(n, place, half, p, True).wait_send()
            for p in range(2):
                dn(place, half, p, True).wait_send()
        for i in range(count):
            er(i).wait_send()

    for k in range(1, count):

        @pl.when(place + k < count)
        def _(k=k):
            state_copy(0, k, place).wait_send()

        @pl.when(place >= k)
        def _(k=k):
            state_copy(1, k, place).wait_send()

    for n, t in enumerate(others):
        a2a(n, me, t).wait_send()
    for kind in range(3):
        for i in range(4):
            ow(kind, me, i, tc).wait_send()


def fast_body(
    queries,
    key_projected,
    values,
    output_gate_preact,
    forward_decay_logits,
    backward_decay_logits,
    decay_logit_shift,
    decay_spike_values,
    residual,
    head_norm_gain,
    output_projection,
    prenorm_gain,
    gate_projection,
    up_projection,
    down_projection,
):
    count = lax.axis_size("sp")
    tokens, lanes = queries.shape
    width = values.shape[1]
    own, model = residual.shape
    depth, hidden = gate_projection.shape
    dw = down_projection.shape[1]
    tps = tokens // own
    blocks = tokens // BLOCK
    dma = lambda *shape: pltpu.SemaphoreType.DMA(shape)
    state = (HEAD_V + 16, lanes)
    V = pltpu.VMEM
    scratch = [
        V((tokens, 2 * lanes), F32),
        V((tokens, 2 * lanes), BF16),
        V(state, BF16),
        V(state, BF16),
        V((count - 1,) + state, BF16),
        V((count - 1,) + state, BF16),
        V((HEAD_V, lanes), F32),
        V((HEAD_V, lanes), F32),
        V((blocks, 2 * HEAD_V, lanes), BF16),
        V((tokens, width), BF16),
        V((own, tps * width), BF16),
        V((tps * width, model), BF16),
        V((own, model), BF16),
        V((own, model), BF16),
        V((2, tokens, model), BF16),
        V((PIECES, model, hidden // PIECES), BF16),
        V((PIECES, model, hidden // PIECES), BF16),
        V((count, hidden, dw), BF16),
        V((2, tokens, hidden), BF16),
        V((2, count, tokens, dw), BF16),
        V((2, count, 2, own, dw), BF16),
        V((count, own, dw), BF16),
        V((count, own, dw), BF16),
        V((count, 2, own, dw), BF16),
        V((2, count, own, dw), BF16),
        V((count, own, dw), BF16),
        dma(2 * PIECES + 3),
        dma(2, count - 1),
        dma(2, count - 1),
        dma(3),
        dma(tps),
        dma(3, 4),
        dma(tps, 4),
        dma(2, 3, 2),
        dma(2, tps, 2),
        dma(2),
        dma(2, count, 2, PIECES),
        dma(2, count, 2, PIECES),
        dma(count, 2, 2),
        dma(count, 2, 2),
        dma(2, count, 2),
        dma(2, count, 2),
        dma(count),
        dma(count),
        dma(count, 2),
        dma(count, 2),
        dma(count),
        dma(count),
    ]
    anywhere = pl.BlockSpec(memory_space=pl.ANY)
    return pl.pallas_call(
        layer_kernel,
        out_shape=jax.ShapeDtypeStruct((own, model), BF16),
        in_specs=[VMEM] * 10 + [anywhere] * 5,
        out_specs=VMEM,
        scratch_shapes=scratch,
        compiler_params=pltpu.CompilerParams(
            collective_id=0, has_side_effects=True, vmem_limit_bytes=67043328
        ),
        cost_estimate=cost(3 * 10**10, 3 * 10**7),
        name="layer",
    )(
        key_projected,
        values,
        forward_decay_logits,
        backward_decay_logits,
        decay_logit_shift,
        jnp.transpose(decay_spike_values),
        queries,
        output_gate_preact,
        head_norm_gain[None, :],
        prenorm_gain[None, :],
        residual,
        output_projection,
        gate_projection,
        up_projection,
        down_projection,
    )


def solution(mesh):
    in_specs = (
        P(("grp", "sp"), "tp"),
        P(("grp", "sp"), "tp"),
        P(("grp", "sp"), "tp"),
        P(("grp", "sp"), "tp"),
        P(("grp", "sp"), "tp"),
        P(("grp", "sp"), "tp"),
        P(None, "tp"),
        P("tp", ("grp", "sp")),
        P(("grp", "sp", "tp"), None),
        P("tp"),
        P("tp", None),
        P(),
        P("sp", "tp"),
        P("sp", "tp"),
        P("tp", "sp"),
    )
    out_specs = P(("grp", "sp", "tp"), None)

    def run(*args):
        lanes = args[0].shape[1]
        sizes = (mesh.shape["grp"], mesh.shape["sp"], mesh.shape["tp"])
        fits = lanes == 2 * KEY_CHANNELS and sizes == (2, 4, 4)
        return fast_body(*args) if fits else body(*args)

    return jax.shard_map(run, mesh=mesh, in_specs=in_specs, out_specs=out_specs, check_vma=False)
```

```python
import functools

import jax
import jax.numpy as jnp
from jax import lax
from jax.experimental import pallas as pl
from jax.experimental.pallas import tpu as pltpu
from jax.sharding import PartitionSpec as P


KEY_CHANNELS = 64
HEAD_V = 128
BLOCK = 64
GATE_DENOMINATOR = 16.0
EPSILON = 1e-06
F32, BF16 = jnp.float32, jnp.bfloat16


def nt(a, b):
    return lax.dot_general(a, b, (((1,), (1,)), ((), ())), preferred_element_type=F32)


def tn(a, b):
    return lax.dot_general(a, b, (((0,), (0,)), ((), ())), preferred_element_type=F32)


def first_head(shape):
    return lax.broadcasted_iota(jnp.int32, shape, 1) < KEY_CHANNELS


VMEM = pl.BlockSpec(memory_space=pltpu.VMEM)


def cost(flops, size):
    return pl.CostEstimate(flops=flops, bytes_accessed=size, transcendentals=0)


def entering(value, axis, join, neutral, backward):
    count = lax.axis_size(axis)
    place = lax.axis_index(axis)
    ahead = count - 1 - place if backward else place
    gathered = jax.tree.map(
        lambda a, kind: lax.all_gather(a.astype(kind), axis), value, (jnp.bfloat16, jnp.bfloat16)
    )
    state = jax.tree.map(lambda a, e: jnp.zeros_like(a) + jnp.asarray(e, a.dtype), value, neutral)

    def one(lap, state):
        source = count - 1 - lap if backward else lap
        return join(
            state,
            jax.tree.map(
                lambda a, own: lax.dynamic_index_in_dim(a, source, 0, False).astype(own.dtype),
                gathered,
                value,
            ),
        )

    return lax.fori_loop(0, ahead, one, state)


def block_sweep(query_in, key_in, values_in, log_decay, span):
    sequence_length, head_count, key_dim = key_in.shape
    block_count = sequence_length // span

    def blocks(tensor):
        return jnp.transpose(
            tensor.reshape(block_count, span, head_count, tensor.shape[-1]), (0, 2, 1, 3)
        )

    lower_mask = jnp.tril(jnp.ones((span, span), dtype=bool))[:, :, None]

    def advance(carried, inputs):
        memory, offset = carried
        key_blk, value_blk, decay_blk, query_blk = inputs
        within = jnp.cumsum(decay_blk, axis=1)
        ending = within[:, -1, :]
        memory_next = jnp.exp(ending)[:, :, None] * memory + jnp.einsum(
            "hjd,hje->hde",
            key_blk * jnp.exp(ending[:, None, :] - within),
            value_blk,
            precision=lax.Precision.HIGHEST,
        )
        result = jnp.einsum(
            "hid,hde->hie", query_blk * jnp.exp(within), memory, precision=lax.Precision.HIGHEST
        )
        spread = jnp.exp(
            jnp.where(lower_mask, within[:, :, None, :] - within[:, None, :, :], -jnp.inf)
        )
        scores = jnp.einsum(
            "hid,hjd,hijd->hij", query_blk, key_blk, spread, precision=lax.Precision.HIGHEST
        )
        result = result + jnp.einsum(
            "hij,hje->hie", scores, value_blk, precision=lax.Precision.HIGHEST
        )
        reached = query_blk * jnp.exp(within + offset[:, None, :])
        return ((memory_next, offset + ending), (result, reached))

    start_memory = jnp.zeros((head_count, key_dim, values_in.shape[-1]), jnp.float32)
    start_offset = jnp.zeros((head_count, key_dim), jnp.float32)
    (memory, decay_total), (outputs, reached) = lax.scan(
        advance,
        (start_memory, start_offset),
        (blocks(key_in), blocks(values_in), blocks(log_decay), blocks(query_in)),
    )

    def unblock(tensor):
        return jnp.transpose(tensor, (0, 2, 1, 3)).reshape(
            sequence_length, head_count, tensor.shape[-1]
        )

    return (unblock(outputs), unblock(reached), memory, decay_total)


def head_mix(combined, head_norm_gain, output_gate_preact):
    sequence_length, head_count, width = combined.shape
    inverse = lax.rsqrt(jnp.mean(combined * combined, axis=-1, keepdims=True) + EPSILON)
    gate_act = jax.nn.silu(
        output_gate_preact.astype(jnp.float32).reshape(sequence_length, head_count, width)
    )
    weighted = combined * inverse * head_norm_gain.reshape(head_count, width) * gate_act
    return weighted.reshape(sequence_length, head_count * width).astype(jnp.bfloat16)


def row_norm(mid_rows, prenorm_gain):
    wide = mid_rows.astype(jnp.float32)
    inverse = lax.rsqrt(jnp.mean(wide * wide, axis=-1, keepdims=True) + EPSILON)
    return (wide * inverse * prenorm_gain).astype(jnp.bfloat16)


def combine_states(earlier, later):
    decay_early, memory_early = earlier
    decay_late, memory_late = later
    return (decay_early * decay_late, decay_late[:, :, None] * memory_early + memory_late)


def body(
    queries,
    key_projected,
    values,
    output_gate_preact,
    forward_decay_logits,
    backward_decay_logits,
    decay_logit_shift,
    decay_spike_values,
    residual,
    head_norm_gain,
    output_projection,
    prenorm_gain,
    gate_projection,
    up_projection,
    down_projection,
):
    sequence_length = queries.shape[0]
    local_heads = queries.shape[1] // KEY_CHANNELS
    query_f = queries.astype(jnp.float32).reshape(
        sequence_length, local_heads, KEY_CHANNELS
    ) * KEY_CHANNELS ** (-0.5)
    keys_f = key_projected.astype(jnp.float32).reshape(sequence_length, local_heads, KEY_CHANNELS)
    values_f = values.astype(jnp.float32).reshape(sequence_length, local_heads, HEAD_V)
    decay_spikes = jnp.transpose(decay_spike_values)[:, :, None]
    logit_shifts = decay_logit_shift.reshape(2, local_heads, KEY_CHANNELS)
    forward_decay = (
        jax.nn.log_sigmoid(
            forward_decay_logits.astype(jnp.float32).reshape(
                sequence_length, local_heads, KEY_CHANNELS
            )
            + logit_shifts[0]
        )
        / GATE_DENOMINATOR
        + decay_spikes
    )
    backward_decay = (
        jax.nn.log_sigmoid(
            backward_decay_logits.astype(jnp.float32).reshape(
                sequence_length, local_heads, KEY_CHANNELS
            )
            + logit_shifts[1]
        )
        / GATE_DENOMINATOR
        + decay_spikes
    )
    fwd_out, fwd_reach, fwd_memory, fwd_total = block_sweep(
        query_f, keys_f, values_f, forward_decay, BLOCK
    )
    bwd_out, bwd_reach, bwd_memory, bwd_total = block_sweep(
        query_f[::-1], keys_f[::-1], values_f[::-1], backward_decay[::-1], BLOCK
    )
    identity = (jnp.ones_like(fwd_total), jnp.zeros_like(fwd_memory))
    fwd_incoming = entering(
        (jnp.exp(fwd_total), fwd_memory), "sp", combine_states, identity, False
    )[1]
    bwd_incoming = entering((jnp.exp(bwd_total), bwd_memory), "sp", combine_states, identity, True)[
        1
    ]
    fwd_full = fwd_out + jnp.einsum(
        "lhd,hde->lhe", fwd_reach, fwd_incoming, precision=lax.Precision.HIGHEST
    )
    bwd_full = bwd_out + jnp.einsum(
        "lhd,hde->lhe", bwd_reach, bwd_incoming, precision=lax.Precision.HIGHEST
    )
    attended = head_mix(fwd_full + bwd_full[::-1], head_norm_gain, output_gate_preact)
    token_rows = lax.all_to_all(attended, "tp", split_axis=0, concat_axis=1, tiled=True)
    whole_out = lax.all_gather(output_projection, "tp", axis=0, tiled=True)
    projected = jnp.dot(token_rows, whole_out, preferred_element_type=jnp.float32)
    mid_rows = (residual.astype(jnp.float32) + projected).astype(jnp.bfloat16)
    normed = row_norm(mid_rows, prenorm_gain)
    fetched = (
        lax.all_gather(gate_projection, "sp", axis=0, tiled=True),
        lax.all_gather(up_projection, "sp", axis=0, tiled=True),
        lax.all_gather(down_projection, "sp", axis=1, tiled=True),
    )
    gate_full, up_full, down_full = fetched
    piece = lax.all_gather(normed, "tp", axis=0, tiled=True)
    gate_part = jnp.dot(piece, gate_full, preferred_element_type=jnp.float32)
    up_part = jnp.dot(piece, up_full, preferred_element_type=jnp.float32)
    hidden = (jax.nn.silu(gate_part) * up_part).astype(jnp.bfloat16)
    summed = lax.psum_scatter(
        jnp.dot(hidden, down_full, preferred_element_type=jnp.float32).astype(jnp.bfloat16),
        "tp",
        scatter_dimension=0,
        tiled=True,
    ).astype(jnp.float32)
    return (mid_rows.astype(jnp.float32) + 0.5 * summed).astype(jnp.bfloat16)


MESH = pl.DeviceIdType.MESH
PIECES = 5


def log_decay(logits, shift, spike):
    x = logits.astype(F32) + shift
    soft = jnp.minimum(x, 0.0) - jnp.log1p(jnp.exp(-jnp.abs(x)))
    return soft / GATE_DENOMINATOR + spike


def own_states(k_ref, v_ref, fd_ref, bd_ref, shift_ref, spike_ref, within_ref, kd_ref, fwd_ref, bwd_ref):
    tokens, lanes = k_ref.shape
    blocks = tokens // BLOCK
    row = lax.broadcasted_iota(jnp.int32, (2 * BLOCK, 2 * BLOCK), 0)
    col = lax.broadcasted_iota(jnp.int32, (2 * BLOCK, 2 * BLOCK), 1)
    r, c = row % BLOCK, col % BLOCK
    ahead = jnp.where(row < BLOCK, r - c, c - r)
    tri = jnp.where(ahead >= 0, 1.0, 0.0).astype(BF16)
    half = first_head((BLOCK, lanes))
    spikes = jnp.transpose(jnp.concatenate([spike_ref[...]] * 4, axis=0))
    ends = []
    for b in range(blocks):
        at = slice(b * BLOCK, (b + 1) * BLOCK)
        spike = jnp.where(half, spikes[at, 0:1], spikes[at, 1:2])
        parts = [log_decay(ref[at, :], shift_ref[n : n + 1, :], spike) for n, ref in enumerate((fd_ref, bd_ref))]
        d = jnp.concatenate(parts, axis=1)
        hi = d.astype(BF16)
        lo = (d - hi.astype(F32)).astype(BF16)
        both = jnp.dot(tri, jnp.concatenate([hi, lo], axis=0), preferred_element_type=F32)
        fwd, bwd = both[:BLOCK, :lanes], both[BLOCK:, lanes:]
        within_ref[at, :lanes] = fwd
        within_ref[at, lanes:] = bwd
        ends.append((fwd[BLOCK - 1 :, :], bwd[:1, :]))
    zero = jnp.zeros((1, lanes), F32)
    after, before = [zero] * blocks, [zero] * blocks
    for b in range(1, blocks):
        before[b] = before[b - 1] + ends[b - 1][1]
        after[blocks - 1 - b] = after[blocks - b] + ends[blocks - b][0]
    totals = after[0] + ends[0][0], before[-1] + ends[-1][1]
    for b in range(blocks):
        at = slice(b * BLOCK, (b + 1) * BLOCK)
        key = k_ref[at, :].astype(F32)
        kd_ref[at, :lanes] = (key * jnp.exp((ends[b][0] + after[b]) - within_ref[at, :lanes])).astype(BF16)
        kd_ref[at, lanes:] = (key * jnp.exp((ends[b][1] + before[b]) - within_ref[at, lanes:])).astype(BF16)
    full = tn(v_ref[...], kd_ref[...])
    mine = first_head((HEAD_V, lanes))
    for n, ref in enumerate((fwd_ref, bwd_ref)):
        u = full[:, n * lanes : (n + 1) * lanes]
        ref[:HEAD_V, :] = jnp.where(mine, u[:HEAD_V], u[HEAD_V:]).astype(BF16)
        ref[HEAD_V:, :] = jnp.broadcast_to(jnp.exp(totals[n]), (16, lanes)).astype(BF16)


def spread(state):
    mine = first_head(state.shape)
    return jnp.concatenate([jnp.where(mine, state, 0.0), jnp.where(mine, 0.0, state)], axis=0).astype(BF16)


def pack(u):
    top = u[:HEAD_V]
    return jnp.where(first_head(top.shape), top, u[HEAD_V:])


def backward_states(k_ref, v_ref, within_ref, state, held_ref):
    tokens, lanes = k_ref.shape
    for b in reversed(range(tokens // BLOCK)):
        at = slice(b * BLOCK, (b + 1) * BLOCK)
        held_ref[b] = spread(state)
        within = within_ref[at, lanes:]
        end = within[:1, :]
        kd = (k_ref[at, :].astype(F32) * jnp.exp(end - within)).astype(BF16)
        state = state * jnp.exp(end) + pack(tn(v_ref[at, :], kd))


def attend(q_ref, k_ref, v_ref, within_ref, gate_ref, gain_ref, fwd_state, held_ref, out_ref):
    tokens, lanes = k_ref.shape
    row = lax.broadcasted_iota(jnp.int32, (2 * BLOCK, BLOCK), 0) % BLOCK
    col = lax.broadcasted_iota(jnp.int32, (2 * BLOCK, BLOCK), 1)
    half = first_head((BLOCK, lanes))
    for b in range(tokens // BLOCK):
        at = slice(b * BLOCK, (b + 1) * BLOCK)
        query = q_ref[at, :].astype(F32) * KEY_CHANNELS ** (-0.5)
        key = k_ref[at, :].astype(F32)
        value = v_ref[at, :]
        scores, reach = [], []
        for n in range(2):
            within = within_ref[at, n * lanes : (n + 1) * lanes]
            pivot = within[BLOCK // 2 - 1 + n : BLOCK // 2 + n, :]
            near = (query * jnp.exp(within - pivot)).astype(BF16)
            far = (key * jnp.exp(pivot - within)).astype(BF16)
            zero = jnp.zeros_like(near)
            pair = jnp.concatenate([jnp.where(half, near, zero), jnp.where(half, zero, near)], axis=0)
            scores.append(nt(pair, far))
            reach.append((query * jnp.exp(within)).astype(BF16))
        score = (jnp.where(col <= row, scores[0], 0.0) + jnp.where(col >= row, scores[1], 0.0)).astype(BF16)
        states = jnp.concatenate([spread(fwd_state), held_ref[b]], axis=1)
        result = nt(jnp.concatenate(reach, axis=1), states)
        for h in range(2):
            lane = slice(h * HEAD_V, (h + 1) * HEAD_V)
            x = result[:, lane] + jnp.dot(
                score[h * BLOCK : (h + 1) * BLOCK], value[:, lane], preferred_element_type=F32
            )
            inverse = lax.rsqrt(jnp.mean(x * x, axis=-1, keepdims=True) + EPSILON)
            g = gate_ref[at, lane].astype(F32)
            out_ref[at, lane] = (x * inverse * gain_ref[:, lane] * (g * jax.nn.sigmoid(g))).astype(BF16)
        within = within_ref[at, :lanes]
        end = within[BLOCK - 1 :, :]
        kd = (key * jnp.exp(end - within)).astype(BF16)
        fwd_state = fwd_state * jnp.exp(end) + pack(tn(value, kd))


def pick(i, table):
    value = table[0]
    for n, item in enumerate(table[1:], 1):
        value = jnp.where(i == n, item, value)
    return value


def ds(first, size):
    return pl.ds(pl.multiple_of(first, size if size % 128 == 0 else 16), size)


def layer_kernel(
    k_ref, v_ref, fd_ref, bd_ref, shift_ref, spike_ref, q_ref, gate_ref, gain_ref, norm_ref,
    res_hbm, out_hbm, g_hbm, u_hbm, d_hbm,
    out_ref,
    within, kd, fown, bown, fgot, bgot, fstate, bstate, held, attended, rows, outw, res, mid, acts,
    wg, wu, wd, hid, part, got, xsend, xgot, esend, egot, erelay,
    loc, st_s, st_r, a2a_s, a2a_r, ow_s, ow_r, ag_s, ag_r, ea_s, gs, gr, dsd, drv, cr_s, cr_r, xo_s, xo_r,
    eo_s, eo_r, er_s, er_r,
):
    count = lax.axis_size("sp")
    side, place, me = lax.axis_index("grp"), lax.axis_index("sp"), lax.axis_index("tp")
    chip, core = me // 2, me % 2
    tc, tx, td = 2 * chip + 1 - core, 2 * (1 - chip) + core, 2 * (1 - chip) + 1 - core
    upper = place // 2
    e, m, o, oe = 3 * upper, 1 + upper, 2 - upper, 3 - 3 * upper
    middle = place * (count - 1 - place) > 0
    outer = jnp.logical_not(middle)
    own = res.shape[0]
    width = attended.shape[1]
    model = mid.shape[1]
    depth, hidden = g_hbm.shape
    tile = hidden // PIECES
    hr = depth // 2
    dr = hidden // 2
    dw = wd.shape[3]
    chunks = part.shape[1]
    orow = width // 4
    nrow = own // 2

    def remote(src, dst, send, recv, **dev):
        return pltpu.make_async_remote_copy(
            src_ref=src, dst_ref=dst, send_sem=send, recv_sem=recv, device_id=dev, device_id_type=MESH
        )

    def gu(n, source, half, p, local=False, again=False, **dev):
        dst = (wg, wu)[n].at[p, ds(source * depth + half * hr, hr), :]
        src = (g_hbm, u_hbm)[n].at[ds(half * hr, hr), ds(p * tile, tile)] if local else dst
        send = gs.at[n, source, 1 - half if again else half, p]
        return remote(src, dst, send, gr.at[n, source, half, p], **(dev or dict(sp=o)))

    def dn(source, half, p, local=False, **dev):
        dst = wd.at[source, p, ds(half * dr, dr), :]
        src = d_hbm.at[ds(half * dr, dr), p * dw : (p + 1) * dw] if local else dst
        return remote(src, dst, dsd.at[source, half, p], drv.at[source, half, p], **(dev or dict(sp=o)))

    def send_gu(source, half, p, local=False, again=False, **dev):
        for n in range(2):
            gu(n, source, half, p, local, again, **dev).start()

    def take_gu(source, half, p):
        for n in range(2):
            gu(n, source, half, p).wait_recv()

    def relay_gu(source, p, **dev):
        take_gu(source, side, p)
        send_gu(source, side, p, **dev)

    def take_dn(source, half, p):
        dn(source, half, p).wait_recv()

    def relay_dn(source, p, **dev):
        take_dn(source, side, p)
        dn(source, side, p, **dev).start()

    def ow(kind, block, i, dev, local=False):
        dst = outw.at[ds(block * width + i * orow, orow), :]
        src = out_hbm.at[i * orow : (i + 1) * orow, :] if local else dst
        return remote(src, dst, ow_s.at[kind, i], ow_r.at[block, i], tp=dev)

    def relay_ow(i):
        ow(2, tx, i, tc).wait_recv()
        ow(2, tx, i, tc).start()

    def a2a(n, block, dev):
        return remote(
            attended.at[ds(dev * own, own), :], rows.at[:, ds(block * width, width)], a2a_s.at[n], a2a_r.at[block], tp=dev
        )

    def ag(q, kind, block, i, dev):
        at = acts.at[q, ds(block * own + i * nrow, nrow), :]
        return remote(at, at, ag_s.at[q, kind, i], ag_r.at[q, block, i], tp=dev)

    def to_host(i):
        at = ds(me * own + i * nrow, nrow)
        return remote(acts.at[0, at, :], acts.at[1, at, :], ea_s.at[i], ag_r.at[1, me, i], sp=m)

    def state_copy(n, k, dev):
        src, dst = ((fown, fgot), (bown, bgot))[n]
        return remote(src, dst.at[k - 1], st_s.at[n, k - 1], st_r.at[n, k - 1], sp=dev)

    def cr(q, i, j):
        block = 2 * j + 1 - core
        return remote(part.at[q, i, ds(block * own, own), :], got.at[q, i, j], cr_s.at[q, i, j], cr_r.at[q, i, j], tp=tc)

    def xo(q, i):
        return remote(xsend.at[q, i], xgot.at[q, i], xo_s.at[q, i], xo_r.at[q, i], tp=tx)

    def eo(i, n):
        dst = egot.at[0, i] if n == 0 else erelay.at[i]
        return remote(esend.at[i, n], dst, eo_s.at[i, n], eo_r.at[i, n], sp=e)

    def er(i):
        return remote(erelay.at[i], egot.at[1, i], er_s.at[i], er_r.at[i], tp=tx)

    own_copies = []
    for p in range(PIECES):
        for n in range(2):
            own_copies.append(
                pltpu.make_async_copy(
                    (g_hbm, u_hbm)[n].at[:, p * tile : (p + 1) * tile],
                    (wg, wu)[n].at[p, ds(place * depth, depth), :],
                    loc.at[n * PIECES + p],
                )
            )
    for p in range(2):
        own_copies.append(
            pltpu.make_async_copy(d_hbm.at[:, p * dw : (p + 1) * dw], wd.at[place, p], loc.at[2 * PIECES + p])
        )
    own_out = pltpu.make_async_copy(out_hbm, outw.at[ds(me * width, width), :], loc.at[2 * PIECES + 2])
    own_res = pltpu.make_async_copy(res_hbm, res, loc.at[2 * PIECES + 3])

    barrier = pltpu.get_barrier_semaphore()
    friends = [dict(sp=lax.rem(place + k, count)) for k in range(1, count)]
    friends += [dict(grp=1 - side)] + [dict(tp=t) for t in (tc, tx, td)]
    for friend in friends:
        pl.semaphore_signal(barrier, inc=1, device_id=friend, device_id_type=MESH)
    own_states(k_ref, v_ref, fd_ref, bd_ref, shift_ref, spike_ref, within, kd, fown, bown)
    pl.semaphore_wait(barrier, len(friends))

    for k in range(1, count):

        @pl.when(place + k < count)
        def _(k=k):
            state_copy(0, k, place + k).start()

        @pl.when(place >= k)
        def _(k=k):
            state_copy(1, k, place - k).start()

    @pl.when(middle)
    def _():
        for p in range(PIECES):
            send_gu(place, side, p, True, sp=o)

    @pl.when(outer)
    def _():
        for p in range(PIECES):
            send_gu(place, side, p, True, sp=m)
        send_gu(place, 1 - side, 0, True, sp=m)

    for i in range(4):
        ow(0, me, i, tx, True).start()
    for i in range(4):
        ow(1, me, i, tc, True).start()
    own_out.start()
    own_res.start()

    @pl.when(middle)
    def _():
        for copy in own_copies:
            copy.start()

    fstate[...] = jnp.zeros_like(fstate)
    bstate[...] = jnp.zeros_like(bstate)
    for k in reversed(range(1, count)):

        @pl.when(place >= k)
        def _(k=k):
            state_copy(0, k, place).wait_recv()
            decay = fgot[k - 1, HEAD_V : HEAD_V + 1, :].astype(F32)
            fstate[...] = fstate[...] * decay + fgot[k - 1, :HEAD_V, :].astype(F32)

        @pl.when(place + k < count)
        def _(k=k):
            state_copy(1, k, place).wait_recv()
            decay = bgot[k - 1, HEAD_V : HEAD_V + 1, :].astype(F32)
            bstate[...] = bstate[...] * decay + bgot[k - 1, :HEAD_V, :].astype(F32)

    backward_states(k_ref, v_ref, within, bstate[...], held)
    attend(q_ref, k_ref, v_ref, within, gate_ref, gain_ref, fstate[...], held, attended)
    others = (tx, td, tc)
    for n, t in enumerate(others):
        a2a(n, me, t).start()
    rows[:, ds(me * width, width)] = attended[ds(me * own, own), :]

    for p in range(4):
        relay_ow(p)

        @pl.when(middle)
        def _(p=p):
            relay_gu(o, p, grp=1 - side)
            relay_gu(e, p, sp=o)

    for t in others:
        a2a(0, t, t).wait_recv()
    for t in (tc, td):
        for i in range(4):
            ow(0, t, i, tc).wait_recv()
    own_out.wait()
    own_res.wait()

    total = jnp.zeros((own, 1), F32)
    wide = 512
    for n in range(model // wide):
        at = slice(n * wide, (n + 1) * wide)
        projected = jnp.dot(rows[...], outw[:, at], preferred_element_type=F32)
        mixed = (res[:, at].astype(F32) + projected).astype(BF16)
        mid[:, at] = mixed
        mixed = mixed.astype(F32)
        total += jnp.sum(mixed * mixed, axis=-1, keepdims=True)
    inverse = lax.rsqrt(total / model + EPSILON)
    for n in range(model // wide):
        at = slice(n * wide, (n + 1) * wide)
        acts[0, ds(me * own, own), at] = (mid[:, at].astype(F32) * inverse * norm_ref[:, at]).astype(BF16)

    sources = (m, m, o, o, e, oe, e, oe)

    @pl.when(middle)
    def _():
        for i in range(2):
            ag(0, 0, me, i, tx).start()
            ag(0, 1, me, i, tc).start()
        relay_gu(o, 4, grp=1 - side)
        relay_gu(e, 4, sp=o)
        for p in range(2):
            dn(place, side, p, True, sp=o).start()
        for copy in own_copies:
            copy.wait()

        def relay_own(i):
            ag(0, 2, tx, i, tc).wait_recv()
            ag(0, 2, tx, i, tc).start()

        def relay_hosted(i):
            ag(1, 0, me, i, tx).wait_recv()
            ag(1, 0, me, i, tx).start()
            ag(1, 1, me, i, tc).start()

        def pass_hosted(i):
            ag(1, 2, tx, i, tc).wait_recv()
            ag(1, 2, tx, i, tc).start()

        relay_gu(oe, 0, grp=1 - side)
        relay_own(0)
        relay_gu(oe, 1, grp=1 - side)
        relay_hosted(0)
        relay_gu(oe, 2, grp=1 - side)
        relay_own(1)

        order = [(0, 0), (0, 1), (0, 2), (1, 0), (1, 1), (1, 2), (0, 3), (0, 4), (1, 3), (1, 4)]

        def first(i, carry):
            q, j = pick(i, [a for a, _ in order]), pick(i, [b for _, b in order])

            @pl.when(i == 0)
            def _():
                for t in (tc, td):
                    for n in range(2):
                        ag(0, 0, t, n, tc).wait_recv()

            @pl.when(i == 1)
            def _():
                relay_hosted(1)
                relay_gu(oe, 3, grp=1 - side)
                pass_hosted(0)
                relay_gu(oe, 4, grp=1 - side)
                send_gu(e, side, 4, again=True, grp=1 - side)

            @pl.when(i == 3)
            def _():
                pass_hosted(1)
                relay_dn(o, 0, grp=1 - side)
                for t in (tc, td):
                    for n in range(2):
                        ag(1, 0, t, n, tc).wait_recv()

            @pl.when(i == 6)
            def _():
                relay_dn(o, 1, grp=1 - side)

            @pl.when(i == 8)
            def _():
                relay_dn(e, 0, sp=o)

            @pl.when(q == 0)
            def _():
                for source in (o, oe, e):
                    take_gu(source, 1 - side, j)

            g = jnp.dot(acts[q], wg[j], preferred_element_type=F32)
            u = jnp.dot(acts[q], wu[j], preferred_element_type=F32)
            hid[q, :, ds(j * tile, tile)] = (g * jax.nn.sigmoid(g) * u).astype(BF16)
            return carry

        lax.fori_loop(0, len(order), first, 0)

        def fold(i, q):
            for j in range(2):
                cr(q, i, j).wait_recv()

            def both(block, j):
                return part[q, i, ds(block * own, own), :].astype(F32) + got[q, i, j].astype(F32)

            @pl.when(q * (1 - i % 2) + 1 - q > 0)
            def _():
                xsend[q, i] = both(tx, 1 - chip).astype(BF16)
                xo(q, i).start()

            @pl.when(q * (i % 2) > 0)
            def _():
                esend[i, 1] = both(tx, 1 - chip).astype(BF16)
                eo(i, 1).start()
                esend[i, 0] = both(me, chip).astype(BF16)
                eo(i, 0).start()

        def push(i):
            xo(1, i).wait_recv()
            mixed = part[1, i, ds(me * own, own), :].astype(F32) + got[1, i, chip].astype(F32)
            esend[i, 0] = (mixed + xgot[1, i].astype(F32)).astype(BF16)
            eo(i, 0).start()

        def second(s, carry):
            i, q = s // 2, 1 - s % 2

            @pl.when((s == 6) | (s == 8) | (s == 10) | (s == 12) | (s == 14))
            def _():
                fold(i - 1, 0)

            @pl.when(s == 4)
            def _():
                take_dn(o, 1 - side, 0)

            @pl.when(s == 6)
            def _():
                relay_dn(e, 1, sp=o)
                take_dn(o, 1 - side, 1)

            @pl.when(s == 8)
            def _():
                relay_dn(oe, 0, grp=1 - side)
                take_dn(e, 1 - side, 0)

            @pl.when(s == 10)
            def _():
                relay_dn(oe, 1, grp=1 - side)
                take_dn(oe, 1 - side, 0)

            @pl.when(s == 12)
            def _():
                take_dn(e, 1 - side, 1)

            @pl.when(s == 14)
            def _():
                take_dn(oe, 1 - side, 1)

            weight = wd[pick(i, sources), pick(i, (0, 1, 0, 1, 0, 0, 1, 1))]
            part[q, i] = jnp.dot(hid[q], weight, preferred_element_type=F32).astype(BF16)
            for j in range(2):
                cr(q, i, j).start()

            @pl.when(q == 0)
            def _():
                fold(i, 1)

            @pl.when((s == 2) | (s == 4))
            def _():
                fold(i - 1, 0)

            @pl.when((s == 5) | (s == 9) | (s == 13))
            def _():
                push(i - 2)

            return carry

        lax.fori_loop(0, 2 * chunks, second, 0)
        fold(chunks - 1, 0)
        push(chunks - 2)

        for i in range(chunks):
            xo(0, i).wait_recv()
            at = ds((2 * sources[i] + (0, 1, 0, 1, 0, 0, 1, 1)[i]) * dw, dw)
            total = part[0, i, ds(me * own, own), :].astype(F32) + got[0, i, chip].astype(F32) + xgot[0, i].astype(F32)
            out_ref[:, at] = (mid[:, at].astype(F32) + 0.5 * total).astype(BF16)

        for p in range(PIECES):
            for n in range(2):
                gu(n, place, side, p, True).wait_send()
                for source in (e, o, oe):
                    gu(n, source, side, p).wait_send()
        for n in range(2):
            gu(n, e, side, 4, again=True).wait_send()
        for p in range(2):
            dn(place, side, p, True).wait_send()
            for source in (e, o, oe):
                dn(source, side, p).wait_send()
        for q in range(2):
            for kind in range(3):
                for i in range(2):
                    ag(q, kind, me, i, tc).wait_send()
            for i in range(chunks):
                for j in range(2):
                    cr(q, i, j).wait_send()
        for i in range(chunks):
            xo(0, i).wait_send()
            eo(i, 0).wait_send()
            (eo(i, 1) if i % 2 else xo(1, i)).wait_send()

    @pl.when(outer)
    def _():
        for i in range(2):
            to_host(i).start()
        for p in range(1, PIECES - 1):
            send_gu(place, 1 - side, p, True, sp=m)
        for half in (side, 1 - side):
            for p in range(2):
                dn(place, half, p, True, sp=m).start()

        def finish(i):
            eo(i, 0).wait_recv()
            total = egot[0, i].astype(F32)
            if i % 2:
                er(i).wait_recv()
                total += egot[1, i].astype(F32)
            at = ds((2 * sources[i] + (0, 1, 0, 1, 0, 0, 1, 1)[i]) * dw, dw)
            out_ref[:, at] = (mid[:, at].astype(F32) + 0.5 * total).astype(BF16)

        for i in range(1, chunks, 2):
            eo(i, 1).wait_recv()
            er(i).start()
            if i > 1:
                finish(i - 2)
                finish(i - 3)
        finish(chunks - 1)
        finish(chunks - 2)
        for i in range(2):
            to_host(i).wait_send()
        for half in (side, 1 - side):
            for p in range(PIECES):
                for n in range(2):
                    if p < PIECES - 1:
                        gu(n, place, half, p, True).wait_send()
            for p in range(2):
                dn(place, half, p, True).wait_send()
        for n in range(2):
            gu(n, place, side, PIECES - 1, True).wait_send()
        for i in range(1, chunks, 2):
            er(i).wait_send()

    for k in range(1, count):

        @pl.when(place + k < count)
        def _(k=k):
            state_copy(0, k, place).wait_send()

        @pl.when(place >= k)
        def _(k=k):
            state_copy(1, k, place).wait_send()

    for n, t in enumerate(others):
        a2a(n, me, t).wait_send()
    for kind in range(3):
        for i in range(4):
            ow(kind, me, i, tc).wait_send()


def fast_body(
    queries,
    key_projected,
    values,
    output_gate_preact,
    forward_decay_logits,
    backward_decay_logits,
    decay_logit_shift,
    decay_spike_values,
    residual,
    head_norm_gain,
    output_projection,
    prenorm_gain,
    gate_projection,
    up_projection,
    down_projection,
):
    count = lax.axis_size("sp")
    tokens, lanes = queries.shape
    width = values.shape[1]
    own, model = residual.shape
    depth, hidden = gate_projection.shape
    dw = down_projection.shape[1] // 2
    chunks = 2 * count
    tps = tokens // own
    blocks = tokens // BLOCK
    dma = lambda *shape: pltpu.SemaphoreType.DMA(shape)
    state = (HEAD_V + 16, lanes)
    V = pltpu.VMEM
    scratch = [
        V((tokens, 2 * lanes), F32),
        V((tokens, 2 * lanes), BF16),
        V(state, BF16),
        V(state, BF16),
        V((count - 1,) + state, BF16),
        V((count - 1,) + state, BF16),
        V((HEAD_V, lanes), F32),
        V((HEAD_V, lanes), F32),
        V((blocks, 2 * HEAD_V, lanes), BF16),
        V((tokens, width), BF16),
        V((own, tps * width), BF16),
        V((tps * width, model), BF16),
        V((own, model), BF16),
        V((own, model), BF16),
        V((2, tokens, model), BF16),
        V((PIECES, model, hidden // PIECES), BF16),
        V((PIECES, model, hidden // PIECES), BF16),
        V((count, 2, hidden, dw), BF16),
        V((2, tokens, hidden), BF16),
        V((2, chunks, tokens, dw), BF16),
        V((2, chunks, 2, own, dw), BF16),
        V((2, chunks, own, dw), BF16),
        V((2, chunks, own, dw), BF16),
        V((chunks, 2, own, dw), BF16),
        V((2, chunks, own, dw), BF16),
        V((chunks, own, dw), BF16),
        dma(2 * PIECES + 4),
        dma(2, count - 1),
        dma(2, count - 1),
        dma(3),
        dma(tps),
        dma(3, 4),
        dma(tps, 4),
        dma(2, 3, 2),
        dma(2, tps, 2),
        dma(2),
        dma(2, count, 2, PIECES),
        dma(2, count, 2, PIECES),
        dma(count, 2, 2),
        dma(count, 2, 2),
        dma(2, chunks, 2),
        dma(2, chunks, 2),
        dma(2, chunks),
        dma(2, chunks),
        dma(chunks, 2),
        dma(chunks, 2),
        dma(chunks),
        dma(chunks),
    ]
    anywhere = pl.BlockSpec(memory_space=pl.ANY)
    return pl.pallas_call(
        layer_kernel,
        out_shape=jax.ShapeDtypeStruct((own, model), BF16),
        in_specs=[VMEM] * 10 + [anywhere] * 5,
        out_specs=VMEM,
        scratch_shapes=scratch,
        compiler_params=pltpu.CompilerParams(
            collective_id=0, has_side_effects=True, vmem_limit_bytes=67043328
        ),
        cost_estimate=cost(3 * 10**10, 3 * 10**7),
        name="layer",
    )(
        key_projected,
        values,
        forward_decay_logits,
        backward_decay_logits,
        decay_logit_shift,
        decay_spike_values,
        queries,
        output_gate_preact,
        head_norm_gain[None, :],
        prenorm_gain[None, :],
        residual,
        output_projection,
        gate_projection,
        up_projection,
        down_projection,
    )


def solution(mesh):
    in_specs = (
        P(("grp", "sp"), "tp"),
        P(("grp", "sp"), "tp"),
        P(("grp", "sp"), "tp"),
        P(("grp", "sp"), "tp"),
        P(("grp", "sp"), "tp"),
        P(("grp", "sp"), "tp"),
        P(None, "tp"),
        P("tp", ("grp", "sp")),
        P(("grp", "sp", "tp"), None),
        P("tp"),
        P("tp", None),
        P(),
        P("sp", "tp"),
        P("sp", "tp"),
        P("tp", "sp"),
    )
    out_specs = P(("grp", "sp", "tp"), None)

    def run(*args):
        lanes = args[0].shape[1]
        sizes = (mesh.shape["grp"], mesh.shape["sp"], mesh.shape["tp"])
        fits = lanes == 2 * KEY_CHANNELS and sizes == (2, 4, 4)
        return fast_body(*args) if fits else body(*args)

    return jax.shard_map(run, mesh=mesh, in_specs=in_specs, out_specs=out_specs, check_vma=False)
```

```python
import functools

import jax
import jax.numpy as jnp
from jax import lax
from jax.experimental import pallas as pl
from jax.experimental.pallas import tpu as pltpu
from jax.sharding import PartitionSpec as P


KEY_CHANNELS = 64
HEAD_V = 128
BLOCK = 64
GATE_DENOMINATOR = 16.0
EPSILON = 1e-06
F32, BF16 = jnp.float32, jnp.bfloat16


def nt(a, b):
    return lax.dot_general(a, b, (((1,), (1,)), ((), ())), preferred_element_type=F32)


def tn(a, b):
    return lax.dot_general(a, b, (((0,), (0,)), ((), ())), preferred_element_type=F32)


def first_head(shape):
    return lax.broadcasted_iota(jnp.int32, shape, 1) < KEY_CHANNELS


VMEM = pl.BlockSpec(memory_space=pltpu.VMEM)


def cost(flops, size):
    return pl.CostEstimate(flops=flops, bytes_accessed=size, transcendentals=0)


def entering(value, axis, join, neutral, backward):
    count = lax.axis_size(axis)
    place = lax.axis_index(axis)
    ahead = count - 1 - place if backward else place
    gathered = jax.tree.map(
        lambda a, kind: lax.all_gather(a.astype(kind), axis), value, (jnp.bfloat16, jnp.bfloat16)
    )
    state = jax.tree.map(lambda a, e: jnp.zeros_like(a) + jnp.asarray(e, a.dtype), value, neutral)

    def one(lap, state):
        source = count - 1 - lap if backward else lap
        return join(
            state,
            jax.tree.map(
                lambda a, own: lax.dynamic_index_in_dim(a, source, 0, False).astype(own.dtype),
                gathered,
                value,
            ),
        )

    return lax.fori_loop(0, ahead, one, state)


def block_sweep(query_in, key_in, values_in, log_decay, span):
    sequence_length, head_count, key_dim = key_in.shape
    block_count = sequence_length // span

    def blocks(tensor):
        return jnp.transpose(
            tensor.reshape(block_count, span, head_count, tensor.shape[-1]), (0, 2, 1, 3)
        )

    lower_mask = jnp.tril(jnp.ones((span, span), dtype=bool))[:, :, None]

    def advance(carried, inputs):
        memory, offset = carried
        key_blk, value_blk, decay_blk, query_blk = inputs
        within = jnp.cumsum(decay_blk, axis=1)
        ending = within[:, -1, :]
        memory_next = jnp.exp(ending)[:, :, None] * memory + jnp.einsum(
            "hjd,hje->hde",
            key_blk * jnp.exp(ending[:, None, :] - within),
            value_blk,
            precision=lax.Precision.HIGHEST,
        )
        result = jnp.einsum(
            "hid,hde->hie", query_blk * jnp.exp(within), memory, precision=lax.Precision.HIGHEST
        )
        spread = jnp.exp(
            jnp.where(lower_mask, within[:, :, None, :] - within[:, None, :, :], -jnp.inf)
        )
        scores = jnp.einsum(
            "hid,hjd,hijd->hij", query_blk, key_blk, spread, precision=lax.Precision.HIGHEST
        )
        result = result + jnp.einsum(
            "hij,hje->hie", scores, value_blk, precision=lax.Precision.HIGHEST
        )
        reached = query_blk * jnp.exp(within + offset[:, None, :])
        return ((memory_next, offset + ending), (result, reached))

    start_memory = jnp.zeros((head_count, key_dim, values_in.shape[-1]), jnp.float32)
    start_offset = jnp.zeros((head_count, key_dim), jnp.float32)
    (memory, decay_total), (outputs, reached) = lax.scan(
        advance,
        (start_memory, start_offset),
        (blocks(key_in), blocks(values_in), blocks(log_decay), blocks(query_in)),
    )

    def unblock(tensor):
        return jnp.transpose(tensor, (0, 2, 1, 3)).reshape(
            sequence_length, head_count, tensor.shape[-1]
        )

    return (unblock(outputs), unblock(reached), memory, decay_total)


def head_mix(combined, head_norm_gain, output_gate_preact):
    sequence_length, head_count, width = combined.shape
    inverse = lax.rsqrt(jnp.mean(combined * combined, axis=-1, keepdims=True) + EPSILON)
    gate_act = jax.nn.silu(
        output_gate_preact.astype(jnp.float32).reshape(sequence_length, head_count, width)
    )
    weighted = combined * inverse * head_norm_gain.reshape(head_count, width) * gate_act
    return weighted.reshape(sequence_length, head_count * width).astype(jnp.bfloat16)


def row_norm(mid_rows, prenorm_gain):
    wide = mid_rows.astype(jnp.float32)
    inverse = lax.rsqrt(jnp.mean(wide * wide, axis=-1, keepdims=True) + EPSILON)
    return (wide * inverse * prenorm_gain).astype(jnp.bfloat16)


def combine_states(earlier, later):
    decay_early, memory_early = earlier
    decay_late, memory_late = later
    return (decay_early * decay_late, decay_late[:, :, None] * memory_early + memory_late)


def body(
    queries,
    key_projected,
    values,
    output_gate_preact,
    forward_decay_logits,
    backward_decay_logits,
    decay_logit_shift,
    decay_spike_values,
    residual,
    head_norm_gain,
    output_projection,
    prenorm_gain,
    gate_projection,
    up_projection,
    down_projection,
):
    sequence_length = queries.shape[0]
    local_heads = queries.shape[1] // KEY_CHANNELS
    query_f = queries.astype(jnp.float32).reshape(
        sequence_length, local_heads, KEY_CHANNELS
    ) * KEY_CHANNELS ** (-0.5)
    keys_f = key_projected.astype(jnp.float32).reshape(sequence_length, local_heads, KEY_CHANNELS)
    values_f = values.astype(jnp.float32).reshape(sequence_length, local_heads, HEAD_V)
    decay_spikes = jnp.transpose(decay_spike_values)[:, :, None]
    logit_shifts = decay_logit_shift.reshape(2, local_heads, KEY_CHANNELS)
    forward_decay = (
        jax.nn.log_sigmoid(
            forward_decay_logits.astype(jnp.float32).reshape(
                sequence_length, local_heads, KEY_CHANNELS
            )
            + logit_shifts[0]
        )
        / GATE_DENOMINATOR
        + decay_spikes
    )
    backward_decay = (
        jax.nn.log_sigmoid(
            backward_decay_logits.astype(jnp.float32).reshape(
                sequence_length, local_heads, KEY_CHANNELS
            )
            + logit_shifts[1]
        )
        / GATE_DENOMINATOR
        + decay_spikes
    )
    fwd_out, fwd_reach, fwd_memory, fwd_total = block_sweep(
        query_f, keys_f, values_f, forward_decay, BLOCK
    )
    bwd_out, bwd_reach, bwd_memory, bwd_total = block_sweep(
        query_f[::-1], keys_f[::-1], values_f[::-1], backward_decay[::-1], BLOCK
    )
    identity = (jnp.ones_like(fwd_total), jnp.zeros_like(fwd_memory))
    fwd_incoming = entering(
        (jnp.exp(fwd_total), fwd_memory), "sp", combine_states, identity, False
    )[1]
    bwd_incoming = entering((jnp.exp(bwd_total), bwd_memory), "sp", combine_states, identity, True)[
        1
    ]
    fwd_full = fwd_out + jnp.einsum(
        "lhd,hde->lhe", fwd_reach, fwd_incoming, precision=lax.Precision.HIGHEST
    )
    bwd_full = bwd_out + jnp.einsum(
        "lhd,hde->lhe", bwd_reach, bwd_incoming, precision=lax.Precision.HIGHEST
    )
    attended = head_mix(fwd_full + bwd_full[::-1], head_norm_gain, output_gate_preact)
    token_rows = lax.all_to_all(attended, "tp", split_axis=0, concat_axis=1, tiled=True)
    whole_out = lax.all_gather(output_projection, "tp", axis=0, tiled=True)
    projected = jnp.dot(token_rows, whole_out, preferred_element_type=jnp.float32)
    mid_rows = (residual.astype(jnp.float32) + projected).astype(jnp.bfloat16)
    normed = row_norm(mid_rows, prenorm_gain)
    fetched = (
        lax.all_gather(gate_projection, "sp", axis=0, tiled=True),
        lax.all_gather(up_projection, "sp", axis=0, tiled=True),
        lax.all_gather(down_projection, "sp", axis=1, tiled=True),
    )
    gate_full, up_full, down_full = fetched
    piece = lax.all_gather(normed, "tp", axis=0, tiled=True)
    gate_part = jnp.dot(piece, gate_full, preferred_element_type=jnp.float32)
    up_part = jnp.dot(piece, up_full, preferred_element_type=jnp.float32)
    hidden = (jax.nn.silu(gate_part) * up_part).astype(jnp.bfloat16)
    summed = lax.psum_scatter(
        jnp.dot(hidden, down_full, preferred_element_type=jnp.float32).astype(jnp.bfloat16),
        "tp",
        scatter_dimension=0,
        tiled=True,
    ).astype(jnp.float32)
    return (mid_rows.astype(jnp.float32) + 0.5 * summed).astype(jnp.bfloat16)


MESH = pl.DeviceIdType.MESH
PIECES = 5


def log_decay(logits, shift, spike):
    x = logits.astype(F32) + shift
    soft = jnp.minimum(x, 0.0) - jnp.log1p(jnp.exp(-jnp.abs(x)))
    return soft / GATE_DENOMINATOR + spike


def own_states(k_ref, v_ref, fd_ref, bd_ref, shift_ref, spike_ref, within_ref, kd_ref, fwd_ref, bwd_ref):
    tokens, lanes = k_ref.shape
    blocks = tokens // BLOCK
    row = lax.broadcasted_iota(jnp.int32, (2 * BLOCK, 2 * BLOCK), 0)
    col = lax.broadcasted_iota(jnp.int32, (2 * BLOCK, 2 * BLOCK), 1)
    r, c = row % BLOCK, col % BLOCK
    ahead = jnp.where(row < BLOCK, r - c, c - r)
    tri = jnp.where(ahead >= 0, 1.0, 0.0).astype(BF16)
    half = first_head((BLOCK, lanes))
    spikes = jnp.transpose(jnp.concatenate([spike_ref[...]] * 4, axis=0))
    ends = []
    for b in range(blocks):
        at = slice(b * BLOCK, (b + 1) * BLOCK)
        spike = jnp.where(half, spikes[at, 0:1], spikes[at, 1:2])
        parts = [log_decay(ref[at, :], shift_ref[n : n + 1, :], spike) for n, ref in enumerate((fd_ref, bd_ref))]
        d = jnp.concatenate(parts, axis=1)
        hi = d.astype(BF16)
        lo = (d - hi.astype(F32)).astype(BF16)
        both = jnp.dot(tri, jnp.concatenate([hi, lo], axis=0), preferred_element_type=F32)
        fwd, bwd = both[:BLOCK, :lanes], both[BLOCK:, lanes:]
        within_ref[at, :lanes] = fwd
        within_ref[at, lanes:] = bwd
        ends.append((fwd[BLOCK - 1 :, :], bwd[:1, :]))
    zero = jnp.zeros((1, lanes), F32)
    after, before = [zero] * blocks, [zero] * blocks
    for b in range(1, blocks):
        before[b] = before[b - 1] + ends[b - 1][1]
        after[blocks - 1 - b] = after[blocks - b] + ends[blocks - b][0]
    totals = after[0] + ends[0][0], before[-1] + ends[-1][1]
    for b in range(blocks):
        at = slice(b * BLOCK, (b + 1) * BLOCK)
        key = k_ref[at, :].astype(F32)
        kd_ref[at, :lanes] = (key * jnp.exp((ends[b][0] + after[b]) - within_ref[at, :lanes])).astype(BF16)
        kd_ref[at, lanes:] = (key * jnp.exp((ends[b][1] + before[b]) - within_ref[at, lanes:])).astype(BF16)
    full = tn(v_ref[...], kd_ref[...])
    mine = first_head((HEAD_V, lanes))
    for n, ref in enumerate((fwd_ref, bwd_ref)):
        u = full[:, n * lanes : (n + 1) * lanes]
        ref[:HEAD_V, :] = jnp.where(mine, u[:HEAD_V], u[HEAD_V:]).astype(BF16)
        ref[HEAD_V:, :] = jnp.broadcast_to(jnp.exp(totals[n]), (16, lanes)).astype(BF16)


def spread(state):
    mine = first_head(state.shape)
    return jnp.concatenate([jnp.where(mine, state, 0.0), jnp.where(mine, 0.0, state)], axis=0).astype(BF16)


def pack(u):
    top = u[:HEAD_V]
    return jnp.where(first_head(top.shape), top, u[HEAD_V:])


def backward_states(k_ref, v_ref, within_ref, state, held_ref):
    tokens, lanes = k_ref.shape
    for b in reversed(range(tokens // BLOCK)):
        at = slice(b * BLOCK, (b + 1) * BLOCK)
        held_ref[b] = spread(state)
        within = within_ref[at, lanes:]
        end = within[:1, :]
        kd = (k_ref[at, :].astype(F32) * jnp.exp(end - within)).astype(BF16)
        state = state * jnp.exp(end) + pack(tn(v_ref[at, :], kd))


def attend(q_ref, k_ref, v_ref, within_ref, gate_ref, gain_ref, fwd_state, held_ref, out_ref):
    tokens, lanes = k_ref.shape
    row = lax.broadcasted_iota(jnp.int32, (2 * BLOCK, BLOCK), 0) % BLOCK
    col = lax.broadcasted_iota(jnp.int32, (2 * BLOCK, BLOCK), 1)
    half = first_head((BLOCK, lanes))
    for b in range(tokens // BLOCK):
        at = slice(b * BLOCK, (b + 1) * BLOCK)
        query = q_ref[at, :].astype(F32) * KEY_CHANNELS ** (-0.5)
        key = k_ref[at, :].astype(F32)
        value = v_ref[at, :]
        scores, reach = [], []
        for n in range(2):
            within = within_ref[at, n * lanes : (n + 1) * lanes]
            pivot = within[BLOCK // 2 - 1 + n : BLOCK // 2 + n, :]
            near = (query * jnp.exp(within - pivot)).astype(BF16)
            far = (key * jnp.exp(pivot - within)).astype(BF16)
            zero = jnp.zeros_like(near)
            pair = jnp.concatenate([jnp.where(half, near, zero), jnp.where(half, zero, near)], axis=0)
            scores.append(nt(pair, far))
            reach.append((query * jnp.exp(within)).astype(BF16))
        score = (jnp.where(col <= row, scores[0], 0.0) + jnp.where(col >= row, scores[1], 0.0)).astype(BF16)
        states = jnp.concatenate([spread(fwd_state), held_ref[b]], axis=1)
        result = nt(jnp.concatenate(reach, axis=1), states)
        for h in range(2):
            lane = slice(h * HEAD_V, (h + 1) * HEAD_V)
            x = result[:, lane] + jnp.dot(
                score[h * BLOCK : (h + 1) * BLOCK], value[:, lane], preferred_element_type=F32
            )
            inverse = lax.rsqrt(jnp.mean(x * x, axis=-1, keepdims=True) + EPSILON)
            g = gate_ref[at, lane].astype(F32)
            out_ref[at, lane] = (x * inverse * gain_ref[:, lane] * (g * jax.nn.sigmoid(g))).astype(BF16)
        within = within_ref[at, :lanes]
        end = within[BLOCK - 1 :, :]
        kd = (key * jnp.exp(end - within)).astype(BF16)
        fwd_state = fwd_state * jnp.exp(end) + pack(tn(value, kd))


def pick(i, table):
    value = table[0]
    for n, item in enumerate(table[1:], 1):
        value = jnp.where(i == n, item, value)
    return value


def ds(first, size):
    return pl.ds(pl.multiple_of(first, size if size % 128 == 0 else 16), size)


def layer_kernel(
    k_ref, v_ref, fd_ref, bd_ref, shift_ref, spike_ref, q_ref, gate_ref, gain_ref, norm_ref,
    res_hbm, out_hbm, g_hbm, u_hbm, d_hbm,
    out_ref,
    within, kd, fown, bown, fgot, bgot, fstate, bstate, held, attended, rows, outw, res, mid, acts,
    wgu, wd, hid, part, got, xsend, xgot, esend, egot, erelay,
    loc, st_s, st_r, a2a_s, a2a_r, ow_s, ow_r, ag_s, ag_r, ea_s, ea_r, gs, gr, dsd, drv, cr_s, cr_r, xo_s, xo_r,
    eo_s, eo_r, er_s, er_r,
):
    count = lax.axis_size("sp")
    side, place, me = lax.axis_index("grp"), lax.axis_index("sp"), lax.axis_index("tp")
    chip, core = me // 2, me % 2
    tc, tx, td = 2 * chip + 1 - core, 2 * (1 - chip) + core, 2 * (1 - chip) + 1 - core
    upper = place // 2
    e, m, o, oe = 3 * upper, 1 + upper, 2 - upper, 3 - 3 * upper
    middle = place * (count - 1 - place) > 0
    outer = jnp.logical_not(middle)
    own = res.shape[0]
    width = attended.shape[1]
    model = mid.shape[1]
    depth, hidden = g_hbm.shape
    tile = hidden // PIECES
    hr = depth // 2
    dr = hidden // 2
    dw = wd.shape[3]
    chunks = part.shape[1]
    orow = width // 4
    nrow = own // 2

    def remote(src, dst, send, recv, **dev):
        return pltpu.make_async_remote_copy(
            src_ref=src, dst_ref=dst, send_sem=send, recv_sem=recv, device_id=dev, device_id_type=MESH
        )

    def gu(n, source, half, p, local=False, again=False, **dev):
        dst = wgu.at[n, p, ds(source * depth + half * hr, hr), :]
        src = (g_hbm, u_hbm)[n].at[ds(half * hr, hr), ds(p * tile, tile)] if local else dst
        send = gs.at[source, 1 - half if again else half]
        return remote(src, dst, send, gr.at[n, source, half, p], **(dev or dict(sp=o)))

    def dn(source, half, p, r, local=False, **dev):
        dst = wd.at[source, p, ds(half * dr + r * (dr // 2), dr // 2), :]
        src = d_hbm.at[ds(half * dr + r * (dr // 2), dr // 2), p * dw : (p + 1) * dw] if local else dst
        return remote(src, dst, dsd.at[source, half], drv.at[source, half, p, r], **(dev or dict(sp=o)))

    def send_gu(source, half, p, local=False, again=False, **dev):
        for n in range(2):
            gu(n, source, half, p, local, again, **dev).start()

    def take_gu(source, half, p):
        for n in range(2):
            gu(n, source, half, p).wait_recv()

    def relay_gu(source, p, **dev):
        for n in range(2):
            gu(n, source, side, p).wait_recv()
            gu(n, source, side, p, **dev).start()

    def send_dn(half, p, **dev):
        for r in range(2):
            dn(place, half, p, r, True, **dev).start()

    def take_dn(source, half, p):
        for r in range(2):
            dn(source, half, p, r).wait_recv()

    def relay_dn(source, p, r, **dev):
        dn(source, side, p, r).wait_recv()
        dn(source, side, p, r, **dev).start()

    def sent(ref, sem):
        remote(ref, ref, sem, sem, sp=o).wait_send()

    def sent_gu(source, half, low, high, again=False):
        at = ds(source * depth + half * hr, hr)
        sent(wgu.at[:, low:high, at, :], gs.at[source, 1 - half if again else half])

    def sent_dn(source, half, low, high):
        sent(wd.at[source, low:high, ds(half * dr, dr), :], dsd.at[source, half])

    def landed(ref, sem):
        remote(ref, ref, sem, sem, sp=o).wait_recv()

    def ow(kind, block, i, dev, local=False):
        dst = outw.at[ds(block * width + i * orow, orow), :]
        src = out_hbm.at[i * orow : (i + 1) * orow, :] if local else dst
        return remote(src, dst, ow_s.at[kind], ow_r.at[i if kind == 0 else 3 + kind], tp=dev)

    def relay_ow(i):
        ow(0, tx, i, tc).wait_recv()
        ow(2, tx, i, tc).start()

    def a2a(n, block, dev):
        return remote(
            attended.at[ds(dev * own, own), :], rows.at[:, ds(block * width, width)], a2a_s.at[n], a2a_r.at[block], tp=dev
        )

    def ag(q, kind, block, i, dev):
        at = acts.at[q, ds(block * own + i * nrow, nrow), :]
        return remote(at, at, ag_s.at[q, kind], ag_r.at[q, i if kind == 0 else 1 + kind], tp=dev)

    def to_host(i):
        at = ds(me * own + i * nrow, nrow)
        return remote(acts.at[0, at, :], acts.at[1, at, :], ea_s.at[0], ea_r.at[i], sp=m)

    def gathered(q):
        for kind, block in ((1, tc), (2, td)):
            landed(acts.at[q, ds(block * own, own), :], ag_r.at[q, 1 + kind])

    def state_copy(n, k, dev):
        src, dst = ((fown, fgot), (bown, bgot))[n]
        return remote(src, dst.at[k - 1], st_s.at[n, k - 1], st_r.at[n, k - 1], sp=dev)

    def cr(q, i, j):
        block = 2 * j + 1 - core
        return remote(part.at[q, i, ds(block * own, own), :], got.at[q, i, j], cr_s.at[q], cr_r.at[q, i], tp=tc)

    def xo(q, i):
        return remote(xsend.at[q, i], xgot.at[q, i], xo_s.at[q], xo_r.at[q, i], tp=tx)

    def eo(i, n):
        dst = egot.at[0, i] if n == 0 else erelay.at[i]
        return remote(esend.at[i, n], dst, eo_s.at[n], eo_r.at[i, n], sp=e)

    def er(i):
        return remote(erelay.at[i], egot.at[1, i], er_s.at[0], er_r.at[i], tp=tx)

    own_copies = []
    for p in range(PIECES):
        for n in range(2):
            own_copies.append(
                pltpu.make_async_copy(
                    (g_hbm, u_hbm)[n].at[:, p * tile : (p + 1) * tile],
                    wgu.at[n, p, ds(place * depth, depth), :],
                    loc.at[0],
                )
            )
    for p in range(2):
        own_copies.append(pltpu.make_async_copy(d_hbm.at[:, p * dw : (p + 1) * dw], wd.at[place, p], loc.at[1]))
    own_gu = wgu.at[:, :, ds(place * depth, depth), :]
    own_waits = [
        pltpu.make_async_copy(own_gu, own_gu, loc.at[0]),
        pltpu.make_async_copy(wd.at[place], wd.at[place], loc.at[1]),
    ]
    own_out = pltpu.make_async_copy(out_hbm, outw.at[ds(me * width, width), :], loc.at[2])
    own_res = pltpu.make_async_copy(res_hbm, res, loc.at[3])

    barrier = pltpu.get_barrier_semaphore()
    friends = [dict(sp=lax.rem(place + k, count)) for k in range(1, count)]
    friends += [dict(grp=1 - side)] + [dict(tp=t) for t in (tc, tx, td)]
    for friend in friends:
        pl.semaphore_signal(barrier, inc=1, device_id=friend, device_id_type=MESH)
    own_states(k_ref, v_ref, fd_ref, bd_ref, shift_ref, spike_ref, within, kd, fown, bown)
    pl.semaphore_wait(barrier, len(friends))

    for k in range(1, count):

        @pl.when(place + k < count)
        def _(k=k):
            state_copy(0, k, place + k).start()

        @pl.when(place >= k)
        def _(k=k):
            state_copy(1, k, place - k).start()

    @pl.when(middle)
    def _():
        for p in range(PIECES):
            send_gu(place, side, p, True, sp=o)

    @pl.when(outer)
    def _():
        for p in range(PIECES):
            send_gu(place, side, p, True, sp=m)
        send_gu(place, 1 - side, 0, True, sp=m)

    for i in range(4):
        ow(0, me, i, tx, True).start()
    for i in range(4):
        ow(1, me, i, tc, True).start()
    own_out.start()
    own_res.start()

    @pl.when(middle)
    def _():
        for copy in own_copies:
            copy.start()

    fstate[...] = jnp.zeros_like(fstate)
    bstate[...] = jnp.zeros_like(bstate)
    for k in reversed(range(1, count)):

        @pl.when(place >= k)
        def _(k=k):
            state_copy(0, k, place).wait_recv()
            decay = fgot[k - 1, HEAD_V : HEAD_V + 1, :].astype(F32)
            fstate[...] = fstate[...] * decay + fgot[k - 1, :HEAD_V, :].astype(F32)

        @pl.when(place + k < count)
        def _(k=k):
            state_copy(1, k, place).wait_recv()
            decay = bgot[k - 1, HEAD_V : HEAD_V + 1, :].astype(F32)
            bstate[...] = bstate[...] * decay + bgot[k - 1, :HEAD_V, :].astype(F32)

    backward_states(k_ref, v_ref, within, bstate[...], held)
    attend(q_ref, k_ref, v_ref, within, gate_ref, gain_ref, fstate[...], held, attended)
    others = (tx, td, tc)
    for n, t in enumerate(others):
        a2a(n, me, t).start()
    rows[:, ds(me * width, width)] = attended[ds(me * own, own), :]

    for p in range(4):
        relay_ow(p)

        @pl.when(middle)
        def _(p=p):
            relay_gu(o, p, grp=1 - side)
            relay_gu(e, p, sp=o)

    for t in others:
        a2a(0, t, t).wait_recv()
    for kind, t in ((1, tc), (2, td)):
        landed(outw.at[ds(t * width, width), :], ow_r.at[3 + kind])
    own_out.wait()
    own_res.wait()

    total = jnp.zeros((own, 1), F32)
    wide = 512
    for n in range(model // wide):
        at = slice(n * wide, (n + 1) * wide)
        projected = jnp.dot(rows[...], outw[:, at], preferred_element_type=F32)
        mixed = (res[:, at].astype(F32) + projected).astype(BF16)
        mid[:, at] = mixed
        mixed = mixed.astype(F32)
        total += jnp.sum(mixed * mixed, axis=-1, keepdims=True)
    inverse = lax.rsqrt(total / model + EPSILON)
    for n in range(model // wide):
        at = slice(n * wide, (n + 1) * wide)
        acts[0, ds(me * own, own), at] = (mid[:, at].astype(F32) * inverse * norm_ref[:, at]).astype(BF16)

    sources = (m, m, o, oe, e, o, oe, e)
    sides = (0, 1, 0, 0, 0, 1, 1, 1)

    @pl.when(middle)
    def _():
        for i in range(2):
            ag(0, 0, me, i, tx).start()
            ag(0, 1, me, i, tc).start()
        relay_gu(o, 4, grp=1 - side)
        relay_gu(e, 4, sp=o)
        for p in range(2):
            send_dn(side, p, sp=o)
        for copy in own_waits:
            copy.wait()

        def relay_own(i):
            ag(0, 0, tx, i, tc).wait_recv()
            ag(0, 2, tx, i, tc).start()

        def relay_hosted(i):
            to_host(i).wait_recv()
            ag(1, 0, me, i, tx).start()
            ag(1, 1, me, i, tc).start()

        def pass_hosted(i):
            ag(1, 0, tx, i, tc).wait_recv()
            ag(1, 2, tx, i, tc).start()

        relay_gu(oe, 0, grp=1 - side)
        relay_own(0)
        relay_gu(oe, 1, grp=1 - side)
        relay_hosted(0)
        relay_gu(oe, 2, grp=1 - side)
        relay_own(1)

        order = [(0, 0), (0, 1), (0, 2), (1, 0), (1, 1), (1, 2), (0, 3), (0, 4), (1, 3), (1, 4)]

        def first(i, carry):
            q, j = pick(i, [a for a, _ in order]), pick(i, [b for _, b in order])

            @pl.when(i == 0)
            def _():
                gathered(0)

            @pl.when(i == 1)
            def _():
                relay_hosted(1)
                relay_gu(oe, 3, grp=1 - side)
                pass_hosted(0)

            @pl.when(i == 2)
            def _():
                relay_gu(oe, 4, grp=1 - side)
                send_gu(e, side, 4, again=True, grp=1 - side)
                pass_hosted(1)

            @pl.when(i == 3)
            def _():
                for r in range(2):
                    relay_dn(o, 0, r, grp=1 - side)
                gathered(1)

            @pl.when(i == 8)
            def _():
                for r in range(2):
                    relay_dn(e, 0, r, sp=o)

            @pl.when(q == 0)
            def _():
                for source in (o, oe, e):
                    take_gu(source, 1 - side, j)

            g = jnp.dot(acts[q], wgu[0, j], preferred_element_type=F32)
            u = jnp.dot(acts[q], wgu[1, j], preferred_element_type=F32)
            hid[q, :, ds(j * tile, tile)] = (g * jax.nn.sigmoid(g) * u).astype(BF16)
            return carry

        lax.fori_loop(0, len(order), first, 0)

        def fold(i, q):
            landed(got.at[q, i], cr_r.at[q, i])

            def both(block, j):
                return part[q, i, ds(block * own, own), :].astype(F32) + got[q, i, j].astype(F32)

            @pl.when(q * (1 - i % 2) + 1 - q > 0)
            def _():
                xsend[q, i] = both(tx, 1 - chip).astype(BF16)
                xo(q, i).start()

            @pl.when(q * (i % 2) > 0)
            def _():
                esend[i, 1] = both(tx, 1 - chip).astype(BF16)
                eo(i, 1).start()
                esend[i, 0] = both(me, chip).astype(BF16)
                eo(i, 0).start()

        def push(i):
            xo(1, i).wait_recv()
            mixed = part[1, i, ds(me * own, own), :].astype(F32) + got[1, i, chip].astype(F32)
            esend[i, 0] = (mixed + xgot[1, i].astype(F32)).astype(BF16)
            eo(i, 0).start()

        def second(s, carry):
            i, q = s // 2, 1 - s % 2

            @pl.when((s == 6) | (s == 8) | (s == 10) | (s == 12) | (s == 14))
            def _():
                fold(i - 1, 0)

            @pl.when(s == 2)
            def _():
                relay_dn(e, 1, 0, sp=o)

            @pl.when(s == 4)
            def _():
                relay_dn(oe, 0, 0, grp=1 - side)
                relay_dn(e, 1, 1, sp=o)
                send_dn(1 - side, 1, sp=o)
                take_dn(o, 1 - side, 0)

            @pl.when(s == 6)
            def _():
                relay_dn(oe, 0, 1, grp=1 - side)
                relay_dn(oe, 1, 0, grp=1 - side)
                take_dn(oe, 1 - side, 0)

            @pl.when(s == 8)
            def _():
                relay_dn(oe, 1, 1, grp=1 - side)
                take_dn(e, 1 - side, 0)

            @pl.when(s == 10)
            def _():
                take_dn(o, side, 1)
                take_dn(o, 1 - side, 1)

            @pl.when(s == 12)
            def _():
                take_dn(oe, 1 - side, 1)

            @pl.when(s == 14)
            def _():
                take_dn(e, 1 - side, 1)

            weight = wd[pick(i, sources), pick(i, sides)]
            part[q, i] = jnp.dot(hid[q], weight, preferred_element_type=F32).astype(BF16)
            for j in range(2):
                cr(q, i, j).start()

            @pl.when(q == 0)
            def _():
                fold(i, 1)

            @pl.when((s == 2) | (s == 4))
            def _():
                fold(i - 1, 0)

            @pl.when((s == 5) | (s == 9) | (s == 13))
            def _():
                push(i - 2)

            return carry

        lax.fori_loop(0, 2 * chunks, second, 0)
        fold(chunks - 1, 0)
        push(chunks - 2)

        for i in range(chunks):
            xo(0, i).wait_recv()
            at = ds((2 * sources[i] + sides[i]) * dw, dw)
            total = part[0, i, ds(me * own, own), :].astype(F32) + got[0, i, chip].astype(F32) + xgot[0, i].astype(F32)
            out_ref[:, at] = (mid[:, at].astype(F32) + 0.5 * total).astype(BF16)

        for source in (place, e, o, oe):
            sent_gu(source, side, 0, PIECES)
        sent_gu(e, side, 4, 5, again=True)
        for source in (place, e, oe):
            sent_dn(source, side, 0, 2)
        sent_dn(o, side, 0, 1)
        sent_dn(place, 1 - side, 1, 2)
        for q in range(2):
            for kind in range(3):
                sent(acts.at[q, ds(me * own, own), :], ag_s.at[q, kind])
            sent(got.at[q], cr_s.at[q])
        sent(xsend.at[0], xo_s.at[0])
        sent(xsend.at[1, : chunks // 2], xo_s.at[1])
        sent(esend.at[:, 0], eo_s.at[0])
        sent(esend.at[: chunks // 2, 1], eo_s.at[1])

    @pl.when(outer)
    def _():
        for i in range(2):
            to_host(i).start()
        for p in range(1, PIECES - 1):
            send_gu(place, 1 - side, p, True, sp=m)
        for half in (side, 1 - side):
            for p in range(2):
                send_dn(half, p, sp=m)

        def finish(i):
            eo(i, 0).wait_recv()
            total = egot[0, i].astype(F32)
            if i % 2:
                er(i).wait_recv()
                total += egot[1, i].astype(F32)
            at = ds((2 * sources[i] + sides[i]) * dw, dw)
            out_ref[:, at] = (mid[:, at].astype(F32) + 0.5 * total).astype(BF16)

        for i in range(1, chunks, 2):
            eo(i, 1).wait_recv()
            er(i).start()
            if i > 1:
                finish(i - 2)
                finish(i - 3)
        finish(chunks - 1)
        finish(chunks - 2)
        sent(acts.at[0, ds(me * own, own), :], ea_s.at[0])
        sent_gu(place, side, 0, PIECES)
        sent_gu(place, 1 - side, 0, PIECES - 1)
        for half in (side, 1 - side):
            sent_dn(place, half, 0, 2)
        sent(erelay.at[: chunks // 2], er_s.at[0])

    for k in range(1, count):

        @pl.when(place + k < count)
        def _(k=k):
            state_copy(0, k, place).wait_send()

        @pl.when(place >= k)
        def _(k=k):
            state_copy(1, k, place).wait_send()

    for n, t in enumerate(others):
        a2a(n, me, t).wait_send()
    for kind in range(3):
        sent(outw.at[ds(me * width, width), :], ow_s.at[kind])


def fast_body(
    queries,
    key_projected,
    values,
    output_gate_preact,
    forward_decay_logits,
    backward_decay_logits,
    decay_logit_shift,
    decay_spike_values,
    residual,
    head_norm_gain,
    output_projection,
    prenorm_gain,
    gate_projection,
    up_projection,
    down_projection,
):
    count = lax.axis_size("sp")
    tokens, lanes = queries.shape
    width = values.shape[1]
    own, model = residual.shape
    depth, hidden = gate_projection.shape
    dw = down_projection.shape[1] // 2
    chunks = 2 * count
    tps = tokens // own
    blocks = tokens // BLOCK
    dma = lambda *shape: pltpu.SemaphoreType.DMA(shape)
    state = (HEAD_V + 16, lanes)
    V = pltpu.VMEM
    scratch = [
        V((tokens, 2 * lanes), F32),
        V((tokens, 2 * lanes), BF16),
        V(state, BF16),
        V(state, BF16),
        V((count - 1,) + state, BF16),
        V((count - 1,) + state, BF16),
        V((HEAD_V, lanes), F32),
        V((HEAD_V, lanes), F32),
        V((blocks, 2 * HEAD_V, lanes), BF16),
        V((tokens, width), BF16),
        V((own, tps * width), BF16),
        V((tps * width, model), BF16),
        V((own, model), BF16),
        V((own, model), BF16),
        V((2, tokens, model), BF16),
        V((2, PIECES, model, hidden // PIECES), BF16),
        V((count, 2, hidden, dw), BF16),
        V((2, tokens, hidden), BF16),
        V((2, chunks, tokens, dw), BF16),
        V((2, chunks, 2, own, dw), BF16),
        V((2, chunks, own, dw), BF16),
        V((2, chunks, own, dw), BF16),
        V((chunks, 2, own, dw), BF16),
        V((2, chunks, own, dw), BF16),
        V((chunks, own, dw), BF16),
        dma(4),
        dma(2, count - 1),
        dma(2, count - 1),
        dma(3),
        dma(tps),
        dma(3),
        dma(6),
        dma(2, 3),
        dma(2, 4),
        dma(1),
        dma(2),
        dma(count, 2),
        dma(2, count, 2, PIECES),
        dma(count, 2),
        dma(count, 2, 2, 2),
        dma(2),
        dma(2, chunks),
        dma(2),
        dma(2, chunks),
        dma(2),
        dma(chunks, 2),
        dma(1),
        dma(chunks),
    ]
    anywhere = pl.BlockSpec(memory_space=pl.ANY)
    return pl.pallas_call(
        layer_kernel,
        out_shape=jax.ShapeDtypeStruct((own, model), BF16),
        in_specs=[VMEM] * 10 + [anywhere] * 5,
        out_specs=VMEM,
        scratch_shapes=scratch,
        compiler_params=pltpu.CompilerParams(
            collective_id=0, has_side_effects=True, vmem_limit_bytes=67043328
        ),
        cost_estimate=cost(3 * 10**10, 3 * 10**7),
        name="layer",
    )(
        key_projected,
        values,
        forward_decay_logits,
        backward_decay_logits,
        decay_logit_shift,
        decay_spike_values,
        queries,
        output_gate_preact,
        head_norm_gain[None, :],
        prenorm_gain[None, :],
        residual,
        output_projection,
        gate_projection,
        up_projection,
        down_projection,
    )


def solution(mesh):
    in_specs = (
        P(("grp", "sp"), "tp"),
        P(("grp", "sp"), "tp"),
        P(("grp", "sp"), "tp"),
        P(("grp", "sp"), "tp"),
        P(("grp", "sp"), "tp"),
        P(("grp", "sp"), "tp"),
        P(None, "tp"),
        P("tp", ("grp", "sp")),
        P(("grp", "sp", "tp"), None),
        P("tp"),
        P("tp", None),
        P(),
        P("sp", "tp"),
        P("sp", "tp"),
        P("tp", "sp"),
    )
    out_specs = P(("grp", "sp", "tp"), None)

    def run(*args):
        lanes = args[0].shape[1]
        sizes = (mesh.shape["grp"], mesh.shape["sp"], mesh.shape["tp"])
        fits = lanes == 2 * KEY_CHANNELS and sizes == (2, 4, 4)
        return fast_body(*args) if fits else body(*args)

    return jax.shard_map(run, mesh=mesh, in_specs=in_specs, out_specs=out_specs, check_vma=False)
```

```python
import functools

import jax
import jax.numpy as jnp
from jax import lax
from jax.experimental import pallas as pl
from jax.experimental.pallas import tpu as pltpu
from jax.sharding import PartitionSpec as P


KEY_CHANNELS = 64
HEAD_V = 128
BLOCK = 64
GATE_DENOMINATOR = 16.0
EPSILON = 1e-06
F32, BF16 = jnp.float32, jnp.bfloat16


def nt(a, b):
    return lax.dot_general(a, b, (((1,), (1,)), ((), ())), preferred_element_type=F32)


def tn(a, b):
    return lax.dot_general(a, b, (((0,), (0,)), ((), ())), preferred_element_type=F32)


def first_head(shape):
    return lax.broadcasted_iota(jnp.int32, shape, 1) < KEY_CHANNELS


VMEM = pl.BlockSpec(memory_space=pltpu.VMEM)


def cost(flops, size):
    return pl.CostEstimate(flops=flops, bytes_accessed=size, transcendentals=0)


def entering(value, axis, join, neutral, backward):
    count = lax.axis_size(axis)
    place = lax.axis_index(axis)
    ahead = count - 1 - place if backward else place
    gathered = jax.tree.map(
        lambda a, kind: lax.all_gather(a.astype(kind), axis), value, (jnp.bfloat16, jnp.bfloat16)
    )
    state = jax.tree.map(lambda a, e: jnp.zeros_like(a) + jnp.asarray(e, a.dtype), value, neutral)

    def one(lap, state):
        source = count - 1 - lap if backward else lap
        return join(
            state,
            jax.tree.map(
                lambda a, own: lax.dynamic_index_in_dim(a, source, 0, False).astype(own.dtype),
                gathered,
                value,
            ),
        )

    return lax.fori_loop(0, ahead, one, state)


def block_sweep(query_in, key_in, values_in, log_decay, span):
    sequence_length, head_count, key_dim = key_in.shape
    block_count = sequence_length // span

    def blocks(tensor):
        return jnp.transpose(
            tensor.reshape(block_count, span, head_count, tensor.shape[-1]), (0, 2, 1, 3)
        )

    lower_mask = jnp.tril(jnp.ones((span, span), dtype=bool))[:, :, None]

    def advance(carried, inputs):
        memory, offset = carried
        key_blk, value_blk, decay_blk, query_blk = inputs
        within = jnp.cumsum(decay_blk, axis=1)
        ending = within[:, -1, :]
        memory_next = jnp.exp(ending)[:, :, None] * memory + jnp.einsum(
            "hjd,hje->hde",
            key_blk * jnp.exp(ending[:, None, :] - within),
            value_blk,
            precision=lax.Precision.HIGHEST,
        )
        result = jnp.einsum(
            "hid,hde->hie", query_blk * jnp.exp(within), memory, precision=lax.Precision.HIGHEST
        )
        spread = jnp.exp(
            jnp.where(lower_mask, within[:, :, None, :] - within[:, None, :, :], -jnp.inf)
        )
        scores = jnp.einsum(
            "hid,hjd,hijd->hij", query_blk, key_blk, spread, precision=lax.Precision.HIGHEST
        )
        result = result + jnp.einsum(
            "hij,hje->hie", scores, value_blk, precision=lax.Precision.HIGHEST
        )
        reached = query_blk * jnp.exp(within + offset[:, None, :])
        return ((memory_next, offset + ending), (result, reached))

    start_memory = jnp.zeros((head_count, key_dim, values_in.shape[-1]), jnp.float32)
    start_offset = jnp.zeros((head_count, key_dim), jnp.float32)
    (memory, decay_total), (outputs, reached) = lax.scan(
        advance,
        (start_memory, start_offset),
        (blocks(key_in), blocks(values_in), blocks(log_decay), blocks(query_in)),
    )

    def unblock(tensor):
        return jnp.transpose(tensor, (0, 2, 1, 3)).reshape(
            sequence_length, head_count, tensor.shape[-1]
        )

    return (unblock(outputs), unblock(reached), memory, decay_total)


def head_mix(combined, head_norm_gain, output_gate_preact):
    sequence_length, head_count, width = combined.shape
    inverse = lax.rsqrt(jnp.mean(combined * combined, axis=-1, keepdims=True) + EPSILON)
    gate_act = jax.nn.silu(
        output_gate_preact.astype(jnp.float32).reshape(sequence_length, head_count, width)
    )
    weighted = combined * inverse * head_norm_gain.reshape(head_count, width) * gate_act
    return weighted.reshape(sequence_length, head_count * width).astype(jnp.bfloat16)


def row_norm(mid_rows, prenorm_gain):
    wide = mid_rows.astype(jnp.float32)
    inverse = lax.rsqrt(jnp.mean(wide * wide, axis=-1, keepdims=True) + EPSILON)
    return (wide * inverse * prenorm_gain).astype(jnp.bfloat16)


def combine_states(earlier, later):
    decay_early, memory_early = earlier
    decay_late, memory_late = later
    return (decay_early * decay_late, decay_late[:, :, None] * memory_early + memory_late)


def body(
    queries,
    key_projected,
    values,
    output_gate_preact,
    forward_decay_logits,
    backward_decay_logits,
    decay_logit_shift,
    decay_spike_values,
    residual,
    head_norm_gain,
    output_projection,
    prenorm_gain,
    gate_projection,
    up_projection,
    down_projection,
):
    sequence_length = queries.shape[0]
    local_heads = queries.shape[1] // KEY_CHANNELS
    query_f = queries.astype(jnp.float32).reshape(
        sequence_length, local_heads, KEY_CHANNELS
    ) * KEY_CHANNELS ** (-0.5)
    keys_f = key_projected.astype(jnp.float32).reshape(sequence_length, local_heads, KEY_CHANNELS)
    values_f = values.astype(jnp.float32).reshape(sequence_length, local_heads, HEAD_V)
    decay_spikes = jnp.transpose(decay_spike_values)[:, :, None]
    logit_shifts = decay_logit_shift.reshape(2, local_heads, KEY_CHANNELS)
    forward_decay = (
        jax.nn.log_sigmoid(
            forward_decay_logits.astype(jnp.float32).reshape(
                sequence_length, local_heads, KEY_CHANNELS
            )
            + logit_shifts[0]
        )
        / GATE_DENOMINATOR
        + decay_spikes
    )
    backward_decay = (
        jax.nn.log_sigmoid(
            backward_decay_logits.astype(jnp.float32).reshape(
                sequence_length, local_heads, KEY_CHANNELS
            )
            + logit_shifts[1]
        )
        / GATE_DENOMINATOR
        + decay_spikes
    )
    fwd_out, fwd_reach, fwd_memory, fwd_total = block_sweep(
        query_f, keys_f, values_f, forward_decay, BLOCK
    )
    bwd_out, bwd_reach, bwd_memory, bwd_total = block_sweep(
        query_f[::-1], keys_f[::-1], values_f[::-1], backward_decay[::-1], BLOCK
    )
    identity = (jnp.ones_like(fwd_total), jnp.zeros_like(fwd_memory))
    fwd_incoming = entering(
        (jnp.exp(fwd_total), fwd_memory), "sp", combine_states, identity, False
    )[1]
    bwd_incoming = entering((jnp.exp(bwd_total), bwd_memory), "sp", combine_states, identity, True)[
        1
    ]
    fwd_full = fwd_out + jnp.einsum(
        "lhd,hde->lhe", fwd_reach, fwd_incoming, precision=lax.Precision.HIGHEST
    )
    bwd_full = bwd_out + jnp.einsum(
        "lhd,hde->lhe", bwd_reach, bwd_incoming, precision=lax.Precision.HIGHEST
    )
    attended = head_mix(fwd_full + bwd_full[::-1], head_norm_gain, output_gate_preact)
    token_rows = lax.all_to_all(attended, "tp", split_axis=0, concat_axis=1, tiled=True)
    whole_out = lax.all_gather(output_projection, "tp", axis=0, tiled=True)
    projected = jnp.dot(token_rows, whole_out, preferred_element_type=jnp.float32)
    mid_rows = (residual.astype(jnp.float32) + projected).astype(jnp.bfloat16)
    normed = row_norm(mid_rows, prenorm_gain)
    fetched = (
        lax.all_gather(gate_projection, "sp", axis=0, tiled=True),
        lax.all_gather(up_projection, "sp", axis=0, tiled=True),
        lax.all_gather(down_projection, "sp", axis=1, tiled=True),
    )
    gate_full, up_full, down_full = fetched
    piece = lax.all_gather(normed, "tp", axis=0, tiled=True)
    gate_part = jnp.dot(piece, gate_full, preferred_element_type=jnp.float32)
    up_part = jnp.dot(piece, up_full, preferred_element_type=jnp.float32)
    hidden = (jax.nn.silu(gate_part) * up_part).astype(jnp.bfloat16)
    summed = lax.psum_scatter(
        jnp.dot(hidden, down_full, preferred_element_type=jnp.float32).astype(jnp.bfloat16),
        "tp",
        scatter_dimension=0,
        tiled=True,
    ).astype(jnp.float32)
    return (mid_rows.astype(jnp.float32) + 0.5 * summed).astype(jnp.bfloat16)


MESH = pl.DeviceIdType.MESH
PIECES = 5


def log_decay(logits, shift, spike):
    x = logits.astype(F32) + shift
    soft = jnp.minimum(x, 0.0) - jnp.log1p(jnp.exp(-jnp.abs(x)))
    return soft / GATE_DENOMINATOR + spike


def own_states(k_ref, v_ref, fd_ref, bd_ref, shift_ref, spike_ref, within_ref, kd_ref, fwd_ref, bwd_ref):
    tokens, lanes = k_ref.shape
    blocks = tokens // BLOCK
    row = lax.broadcasted_iota(jnp.int32, (2 * BLOCK, 2 * BLOCK), 0)
    col = lax.broadcasted_iota(jnp.int32, (2 * BLOCK, 2 * BLOCK), 1)
    r, c = row % BLOCK, col % BLOCK
    ahead = jnp.where(row < BLOCK, r - c, c - r)
    tri = jnp.where(ahead >= 0, 1.0, 0.0).astype(BF16)
    half = first_head((BLOCK, lanes))
    spikes = jnp.transpose(jnp.concatenate([spike_ref[...]] * 4, axis=0))
    ends = []
    for b in range(blocks):
        at = slice(b * BLOCK, (b + 1) * BLOCK)
        spike = jnp.where(half, spikes[at, 0:1], spikes[at, 1:2])
        parts = [log_decay(ref[at, :], shift_ref[n : n + 1, :], spike) for n, ref in enumerate((fd_ref, bd_ref))]
        d = jnp.concatenate(parts, axis=1)
        hi = d.astype(BF16)
        lo = (d - hi.astype(F32)).astype(BF16)
        both = jnp.dot(tri, jnp.concatenate([hi, lo], axis=0), preferred_element_type=F32)
        fwd, bwd = both[:BLOCK, :lanes], both[BLOCK:, lanes:]
        within_ref[at, :lanes] = fwd
        within_ref[at, lanes:] = bwd
        ends.append((fwd[BLOCK - 1 :, :], bwd[:1, :]))
    zero = jnp.zeros((1, lanes), F32)
    after, before = [zero] * blocks, [zero] * blocks
    for b in range(1, blocks):
        before[b] = before[b - 1] + ends[b - 1][1]
        after[blocks - 1 - b] = after[blocks - b] + ends[blocks - b][0]
    totals = after[0] + ends[0][0], before[-1] + ends[-1][1]
    for b in range(blocks):
        at = slice(b * BLOCK, (b + 1) * BLOCK)
        key = k_ref[at, :].astype(F32)
        kd_ref[at, :lanes] = (key * jnp.exp((ends[b][0] + after[b]) - within_ref[at, :lanes])).astype(BF16)
        kd_ref[at, lanes:] = (key * jnp.exp((ends[b][1] + before[b]) - within_ref[at, lanes:])).astype(BF16)
    full = tn(v_ref[...], kd_ref[...])
    mine = first_head((HEAD_V, lanes))
    for n, ref in enumerate((fwd_ref, bwd_ref)):
        u = full[:, n * lanes : (n + 1) * lanes]
        ref[:HEAD_V, :] = jnp.where(mine, u[:HEAD_V], u[HEAD_V:]).astype(BF16)
        ref[HEAD_V:, :] = jnp.broadcast_to(jnp.exp(totals[n]), (16, lanes)).astype(BF16)


def spread(state):
    mine = first_head(state.shape)
    return jnp.concatenate([jnp.where(mine, state, 0.0), jnp.where(mine, 0.0, state)], axis=0).astype(BF16)


def pack(u):
    top = u[:HEAD_V]
    return jnp.where(first_head(top.shape), top, u[HEAD_V:])


def backward_states(k_ref, v_ref, within_ref, state, held_ref):
    tokens, lanes = k_ref.shape
    for b in reversed(range(tokens // BLOCK)):
        at = slice(b * BLOCK, (b + 1) * BLOCK)
        held_ref[b] = spread(state)
        within = within_ref[at, lanes:]
        end = within[:1, :]
        kd = (k_ref[at, :].astype(F32) * jnp.exp(end - within)).astype(BF16)
        state = state * jnp.exp(end) + pack(tn(v_ref[at, :], kd))


def attend(q_ref, k_ref, v_ref, within_ref, gate_ref, gain_ref, fwd_state, held_ref, out_ref):
    tokens, lanes = k_ref.shape
    row = lax.broadcasted_iota(jnp.int32, (2 * BLOCK, BLOCK), 0) % BLOCK
    col = lax.broadcasted_iota(jnp.int32, (2 * BLOCK, BLOCK), 1)
    half = first_head((BLOCK, lanes))
    for b in range(tokens // BLOCK):
        at = slice(b * BLOCK, (b + 1) * BLOCK)
        query = q_ref[at, :].astype(F32) * KEY_CHANNELS ** (-0.5)
        key = k_ref[at, :].astype(F32)
        value = v_ref[at, :]
        scores, reach = [], []
        for n in range(2):
            within = within_ref[at, n * lanes : (n + 1) * lanes]
            pivot = within[BLOCK // 2 - 1 + n : BLOCK // 2 + n, :]
            near = (query * jnp.exp(within - pivot)).astype(BF16)
            far = (key * jnp.exp(pivot - within)).astype(BF16)
            zero = jnp.zeros_like(near)
            pair = jnp.concatenate([jnp.where(half, near, zero), jnp.where(half, zero, near)], axis=0)
            scores.append(nt(pair, far))
            reach.append((query * jnp.exp(within)).astype(BF16))
        score = (jnp.where(col <= row, scores[0], 0.0) + jnp.where(col >= row, scores[1], 0.0)).astype(BF16)
        states = jnp.concatenate([spread(fwd_state), held_ref[b]], axis=1)
        result = nt(jnp.concatenate(reach, axis=1), states)
        for h in range(2):
            lane = slice(h * HEAD_V, (h + 1) * HEAD_V)
            x = result[:, lane] + jnp.dot(
                score[h * BLOCK : (h + 1) * BLOCK], value[:, lane], preferred_element_type=F32
            )
            inverse = lax.rsqrt(jnp.mean(x * x, axis=-1, keepdims=True) + EPSILON)
            g = gate_ref[at, lane].astype(F32)
            out_ref[at, lane] = (x * inverse * gain_ref[:, lane] * (g * jax.nn.sigmoid(g))).astype(BF16)
        within = within_ref[at, :lanes]
        end = within[BLOCK - 1 :, :]
        kd = (key * jnp.exp(end - within)).astype(BF16)
        fwd_state = fwd_state * jnp.exp(end) + pack(tn(value, kd))


def pick(i, table):
    value = table[0]
    for n, item in enumerate(table[1:], 1):
        value = jnp.where(i == n, item, value)
    return value


def ds(first, size):
    return pl.ds(pl.multiple_of(first, size if size % 128 == 0 else 16), size)


def layer_kernel(
    k_hbm, v_hbm, fd_hbm, bd_hbm, shift_hbm, spike_hbm, q_hbm, gate_hbm, gain_hbm, norm_hbm,
    res_hbm, out_hbm, g_hbm, u_hbm, d_hbm,
    out_ref,
    k_ref, v_ref, fd_ref, bd_ref, shift_ref, spike_ref, q_ref, gate_ref, gain_ref, norm_ref, in_s,
    within, kd, fown, bown, fgot, bgot, fstate, bstate, held, attended, rows, outw, res, mid, acts,
    wgu, wd, hid, part, got, xsend, xgot, esend, egot, erelay,
    loc, st_s, st_r, a2a_s, a2a_r, ow_s, ow_r, ag_s, ag_r, ea_s, ea_r, gs, gr, dsd, drv, cr_s, cr_r, xo_s, xo_r,
    eo_s, eo_r, er_s, er_r,
):
    count = lax.axis_size("sp")
    side, place, me = lax.axis_index("grp"), lax.axis_index("sp"), lax.axis_index("tp")
    chip, core = me // 2, me % 2
    tc, tx, td = 2 * chip + 1 - core, 2 * (1 - chip) + core, 2 * (1 - chip) + 1 - core
    upper = place // 2
    e, m, o, oe = 3 * upper, 1 + upper, 2 - upper, 3 - 3 * upper
    middle = place * (count - 1 - place) > 0
    outer = jnp.logical_not(middle)
    own = res.shape[0]
    width = attended.shape[1]
    model = mid.shape[1]
    depth, hidden = g_hbm.shape
    tile = hidden // PIECES
    hr = depth // 2
    dr = hidden // 2
    dw = wd.shape[3]
    chunks = part.shape[1]
    orow = width // 4
    nrow = own // 2

    def remote(src, dst, send, recv, **dev):
        return pltpu.make_async_remote_copy(
            src_ref=src, dst_ref=dst, send_sem=send, recv_sem=recv, device_id=dev, device_id_type=MESH
        )

    def gu(n, source, half, p, local=False, again=False, **dev):
        dst = wgu.at[n, p, ds(source * depth + half * hr, hr), :]
        src = (g_hbm, u_hbm)[n].at[ds(half * hr, hr), ds(p * tile, tile)] if local else dst
        send = gs.at[source, 1 - half if again else half]
        return remote(src, dst, send, gr.at[n, source, half, p], **(dev or dict(sp=o)))

    def dn(source, half, p, r, local=False, **dev):
        dst = wd.at[source, p, ds(half * dr + r * (dr // 2), dr // 2), :]
        src = d_hbm.at[ds(half * dr + r * (dr // 2), dr // 2), p * dw : (p + 1) * dw] if local else dst
        return remote(src, dst, dsd.at[source, half], drv.at[source, half, p, r], **(dev or dict(sp=o)))

    def send_gu(source, half, p, local=False, again=False, **dev):
        for n in range(2):
            gu(n, source, half, p, local, again, **dev).start()

    def take_gu(source, half, p):
        for n in range(2):
            gu(n, source, half, p).wait_recv()

    def relay_gu(source, p, **dev):
        for n in range(2):
            gu(n, source, side, p).wait_recv()
            gu(n, source, side, p, **dev).start()

    def send_dn(half, p, **dev):
        for r in range(2):
            dn(place, half, p, r, True, **dev).start()

    def take_dn(source, half, p):
        for r in range(2):
            dn(source, half, p, r).wait_recv()

    def relay_dn(source, p, r, **dev):
        dn(source, side, p, r).wait_recv()
        dn(source, side, p, r, **dev).start()

    def sent(ref, sem):
        remote(ref, ref, sem, sem, sp=o).wait_send()

    def sent_gu(source, half, low, high, again=False):
        at = ds(source * depth + half * hr, hr)
        sent(wgu.at[:, low:high, at, :], gs.at[source, 1 - half if again else half])

    def sent_dn(source, half, low, high):
        sent(wd.at[source, low:high, ds(half * dr, dr), :], dsd.at[source, half])

    def landed(ref, sem):
        remote(ref, ref, sem, sem, sp=o).wait_recv()

    def ow(kind, block, i, dev, local=False):
        dst = outw.at[ds(block * width + i * orow, orow), :]
        src = out_hbm.at[i * orow : (i + 1) * orow, :] if local else dst
        return remote(src, dst, ow_s.at[kind], ow_r.at[i if kind == 0 else 3 + kind], tp=dev)

    def relay_ow(i):
        ow(0, tx, i, tc).wait_recv()
        ow(2, tx, i, tc).start()

    def a2a(n, block, dev):
        return remote(
            attended.at[ds(dev * own, own), :], rows.at[:, ds(block * width, width)], a2a_s.at[n], a2a_r.at[block], tp=dev
        )

    def ag(q, kind, block, i, dev):
        at = acts.at[q, ds(block * own + i * nrow, nrow), :]
        return remote(at, at, ag_s.at[q, kind], ag_r.at[q, i if kind == 0 else 1 + kind], tp=dev)

    def to_host(i):
        at = ds(me * own + i * nrow, nrow)
        return remote(acts.at[0, at, :], acts.at[1, at, :], ea_s.at[0], ea_r.at[i], sp=m)

    def gathered(q):
        for kind, block in ((1, tc), (2, td)):
            landed(acts.at[q, ds(block * own, own), :], ag_r.at[q, 1 + kind])

    def state_copy(n, k, dev):
        src, dst = ((fown, fgot), (bown, bgot))[n]
        return remote(src, dst.at[k - 1], st_s.at[n, k - 1], st_r.at[n, k - 1], sp=dev)

    def cr(q, i, j):
        block = 2 * j + 1 - core
        return remote(part.at[q, i, ds(block * own, own), :], got.at[q, i, j], cr_s.at[q], cr_r.at[q, i], tp=tc)

    def xo(q, i):
        return remote(xsend.at[q, i], xgot.at[q, i], xo_s.at[q], xo_r.at[q, i], tp=tx)

    def eo(i, n):
        dst = egot.at[0, i] if n == 0 else erelay.at[i]
        return remote(esend.at[i, n], dst, eo_s.at[n], eo_r.at[i, n], sp=e)

    def er(i):
        return remote(erelay.at[i], egot.at[1, i], er_s.at[0], er_r.at[i], tp=tx)

    own_copies = []
    for p in range(PIECES):
        for n in range(2):
            own_copies.append(
                pltpu.make_async_copy(
                    (g_hbm, u_hbm)[n].at[:, p * tile : (p + 1) * tile],
                    wgu.at[n, p, ds(place * depth, depth), :],
                    loc.at[0],
                )
            )
    for p in range(2):
        own_copies.append(pltpu.make_async_copy(d_hbm.at[:, p * dw : (p + 1) * dw], wd.at[place, p], loc.at[1]))
    own_gu = wgu.at[:, :, ds(place * depth, depth), :]
    own_waits = [
        pltpu.make_async_copy(own_gu, own_gu, loc.at[0]),
        pltpu.make_async_copy(wd.at[place], wd.at[place], loc.at[1]),
    ]
    own_out = pltpu.make_async_copy(out_hbm, outw.at[ds(me * width, width), :], loc.at[2])
    own_res = pltpu.make_async_copy(res_hbm, res, loc.at[3])

    barrier = pltpu.get_barrier_semaphore()
    friends = [dict(sp=lax.rem(place + k, count)) for k in range(1, count)]
    friends += [dict(grp=1 - side)] + [dict(tp=t) for t in (tc, tx, td)]
    for friend in friends:
        pl.semaphore_signal(barrier, inc=1, device_id=friend, device_id_type=MESH)
    loads = [
        pltpu.make_async_copy(src, dst, in_s.at[n])
        for n, (src, dst) in enumerate(
            (
                (k_hbm, k_ref),
                (v_hbm, v_ref),
                (fd_hbm, fd_ref),
                (bd_hbm, bd_ref),
                (shift_hbm, shift_ref),
                (spike_hbm, spike_ref),
                (q_hbm, q_ref),
                (gate_hbm, gate_ref),
                (gain_hbm, gain_ref),
                (norm_hbm, norm_ref),
            )
        )
    ]
    for load in loads:
        load.start()
    pl.semaphore_wait(barrier, len(friends))

    @pl.when(middle)
    def _():
        gu(0, place, side, 0, True, sp=o).start()

    @pl.when(outer)
    def _():
        gu(0, place, side, 0, True, sp=m).start()

    for i in range(4):
        ow(0, me, i, tx, True).start()
    for i in range(4):
        ow(1, me, i, tc, True).start()
    for load in loads[:6]:
        load.wait()
    own_states(k_ref, v_ref, fd_ref, bd_ref, shift_ref, spike_ref, within, kd, fown, bown)

    for k in range(1, count):

        @pl.when(place + k < count)
        def _(k=k):
            state_copy(0, k, place + k).start()

        @pl.when(place >= k)
        def _(k=k):
            state_copy(1, k, place - k).start()

    @pl.when(middle)
    def _():
        gu(1, place, side, 0, True, sp=o).start()
        for p in range(1, PIECES):
            send_gu(place, side, p, True, sp=o)

    @pl.when(outer)
    def _():
        gu(1, place, side, 0, True, sp=m).start()
        for p in range(1, PIECES):
            send_gu(place, side, p, True, sp=m)
        send_gu(place, 1 - side, 0, True, sp=m)

    own_out.start()
    own_res.start()

    @pl.when(middle)
    def _():
        for copy in own_copies:
            copy.start()

    for load in loads[6:]:
        load.wait()
    fstate[...] = jnp.zeros_like(fstate)
    bstate[...] = jnp.zeros_like(bstate)
    for k in reversed(range(1, count)):

        @pl.when(place >= k)
        def _(k=k):
            state_copy(0, k, place).wait_recv()
            decay = fgot[k - 1, HEAD_V : HEAD_V + 1, :].astype(F32)
            fstate[...] = fstate[...] * decay + fgot[k - 1, :HEAD_V, :].astype(F32)

        @pl.when(place + k < count)
        def _(k=k):
            state_copy(1, k, place).wait_recv()
            decay = bgot[k - 1, HEAD_V : HEAD_V + 1, :].astype(F32)
            bstate[...] = bstate[...] * decay + bgot[k - 1, :HEAD_V, :].astype(F32)

    backward_states(k_ref, v_ref, within, bstate[...], held)
    attend(q_ref, k_ref, v_ref, within, gate_ref, gain_ref, fstate[...], held, attended)
    others = (tx, td, tc)
    for n, t in enumerate(others):
        a2a(n, me, t).start()
    rows[:, ds(me * width, width)] = attended[ds(me * own, own), :]

    for p in range(4):
        relay_ow(p)

        @pl.when(middle)
        def _(p=p):
            relay_gu(o, p, grp=1 - side)
            relay_gu(e, p, sp=o)

    for t in others:
        a2a(0, t, t).wait_recv()
    for kind, t in ((1, tc), (2, td)):
        landed(outw.at[ds(t * width, width), :], ow_r.at[3 + kind])
    own_out.wait()
    own_res.wait()

    total = jnp.zeros((own, 1), F32)
    wide = 512
    for n in range(model // wide):
        at = slice(n * wide, (n + 1) * wide)
        projected = jnp.dot(rows[...], outw[:, at], preferred_element_type=F32)
        mixed = (res[:, at].astype(F32) + projected).astype(BF16)
        mid[:, at] = mixed
        mixed = mixed.astype(F32)
        total += jnp.sum(mixed * mixed, axis=-1, keepdims=True)
    inverse = lax.rsqrt(total / model + EPSILON)
    for n in range(model // wide):
        at = slice(n * wide, (n + 1) * wide)
        acts[0, ds(me * own, own), at] = (mid[:, at].astype(F32) * inverse * norm_ref[:, at]).astype(BF16)

    sources = (m, m, o, e, oe, e, oe, o)
    sides = (0, 1, 0, 0, 0, 1, 1, 1)

    @pl.when(middle)
    def _():
        for i in range(2):
            ag(0, 0, me, i, tx).start()
            ag(0, 1, me, i, tc).start()
        relay_gu(o, 4, grp=1 - side)
        relay_gu(e, 4, sp=o)
        for p in (4, 3):
            send_gu(e, side, p, again=True, grp=1 - side)
        for p in range(2):
            send_dn(side, p, sp=o)
        for copy in own_waits:
            copy.wait()

        def relay_own(i):
            ag(0, 0, tx, i, tc).wait_recv()
            ag(0, 2, tx, i, tc).start()

        def relay_hosted(i):
            to_host(i).wait_recv()
            ag(1, 0, me, i, tx).start()
            ag(1, 1, me, i, tc).start()

        def pass_hosted(i):
            ag(1, 0, tx, i, tc).wait_recv()
            ag(1, 2, tx, i, tc).start()

        relay_gu(oe, 0, grp=1 - side)
        relay_own(0)
        relay_gu(oe, 1, grp=1 - side)
        relay_hosted(0)
        relay_gu(oe, 2, grp=1 - side)
        relay_own(1)

        order = [(0, 0), (0, 1), (0, 2), (1, 0), (1, 1), (1, 2), (0, 3), (0, 4), (1, 3), (1, 4)]

        def first(i, carry):
            q, j = pick(i, [a for a, _ in order]), pick(i, [b for _, b in order])

            @pl.when(i == 0)
            def _():
                gathered(0)

            @pl.when(i == 1)
            def _():
                relay_hosted(1)
                relay_gu(oe, 3, grp=1 - side)
                pass_hosted(0)

            @pl.when(i == 2)
            def _():
                relay_gu(oe, 4, grp=1 - side)

            @pl.when(i == 3)
            def _():
                pass_hosted(1)
                for r in range(2):
                    relay_dn(o, 0, r, grp=1 - side)
                gathered(1)

            @pl.when(i == 4)
            def _():
                relay_dn(e, 0, 0, sp=o)

            @pl.when(i == 5)
            def _():
                relay_dn(e, 0, 1, sp=o)

            @pl.when(i == 7)
            def _():
                relay_dn(e, 1, 0, sp=o)

            @pl.when(i == 8)
            def _():
                relay_dn(oe, 0, 0, grp=1 - side)
                relay_dn(e, 1, 1, sp=o)
                send_dn(1 - side, 1, sp=o)

            @pl.when(q == 0)
            def _():
                for source in (o, oe, e):
                    take_gu(source, 1 - side, j)

            g = jnp.dot(acts[q], wgu[0, j], preferred_element_type=F32)
            u = jnp.dot(acts[q], wgu[1, j], preferred_element_type=F32)
            hid[q, :, ds(j * tile, tile)] = (g * jax.nn.sigmoid(g) * u).astype(BF16)
            return carry

        lax.fori_loop(0, len(order), first, 0)

        def fold(i, q):
            landed(got.at[q, i], cr_r.at[q, i])

            def both(block, j):
                return part[q, i, ds(block * own, own), :].astype(F32) + got[q, i, j].astype(F32)

            @pl.when(q * (1 - i % 2) + 1 - q > 0)
            def _():
                xsend[q, i] = both(tx, 1 - chip).astype(BF16)
                xo(q, i).start()

            @pl.when(q * (i % 2) > 0)
            def _():
                esend[i, 1] = both(tx, 1 - chip).astype(BF16)
                eo(i, 1).start()
                esend[i, 0] = both(me, chip).astype(BF16)
                eo(i, 0).start()

        def push(i):
            xo(1, i).wait_recv()
            mixed = part[1, i, ds(me * own, own), :].astype(F32) + got[1, i, chip].astype(F32)
            esend[i, 0] = (mixed + xgot[1, i].astype(F32)).astype(BF16)
            eo(i, 0).start()

        def second(s, carry):
            i, q = s // 2, 1 - s % 2

            @pl.when(s == 0)
            def _():
                relay_dn(oe, 0, 1, grp=1 - side)

            @pl.when(s == 4)
            def _():
                take_dn(o, 1 - side, 0)

            @pl.when(s == 5)
            def _():
                relay_dn(oe, 1, 0, grp=1 - side)

            @pl.when(s == 6)
            def _():
                take_dn(e, 1 - side, 0)

            @pl.when(s == 8)
            def _():
                take_dn(oe, 1 - side, 0)

            @pl.when(s == 10)
            def _():
                relay_dn(oe, 1, 1, grp=1 - side)
                fold(4, 1)
                fold(4, 0)
                push(2)
                take_dn(e, 1 - side, 1)

            @pl.when(s == 12)
            def _():
                take_dn(oe, 1 - side, 1)

            @pl.when(s == 14)
            def _():
                take_dn(o, side, 1)
                take_dn(o, 1 - side, 1)

            weight = wd[pick(i, sources), pick(i, sides)]
            part[q, i] = jnp.dot(hid[q], weight, preferred_element_type=F32).astype(BF16)
            for j in range(2):
                cr(q, i, j).start()

            @pl.when(((s > 1) & (s < 10)) | (s > 11))
            def _():
                fold(i - 1, q)

            @pl.when((s == 9) | (s == 12))
            def _():
                push(pick(s - 9, (0, 4, 4, 4)))

            return carry

        lax.fori_loop(0, 2 * chunks, second, 0)
        for q in (1, 0):
            fold(chunks - 1, q)
        push(chunks - 2)

        for i in range(chunks):
            xo(0, i).wait_recv()
            at = ds((2 * sources[i] + sides[i]) * dw, dw)
            total = part[0, i, ds(me * own, own), :].astype(F32) + got[0, i, chip].astype(F32) + xgot[0, i].astype(F32)
            out_ref[:, at] = (mid[:, at].astype(F32) + 0.5 * total).astype(BF16)

        for source in (place, e, o, oe):
            sent_gu(source, side, 0, PIECES)
        sent_gu(e, side, PIECES - 2, PIECES, again=True)
        for source in (place, e, oe):
            sent_dn(source, side, 0, 2)
        sent_dn(o, side, 0, 1)
        sent_dn(place, 1 - side, 1, 2)
        for q in range(2):
            for kind in range(3):
                sent(acts.at[q, ds(me * own, own), :], ag_s.at[q, kind])
            sent(got.at[q], cr_s.at[q])
        sent(xsend.at[0], xo_s.at[0])
        sent(xsend.at[1, : chunks // 2], xo_s.at[1])
        sent(esend.at[:, 0], eo_s.at[0])
        sent(esend.at[: chunks // 2, 1], eo_s.at[1])

    @pl.when(outer)
    def _():
        for i in range(2):
            to_host(i).start()
        for p in range(1, PIECES - 2):
            send_gu(place, 1 - side, p, True, sp=m)
        for half in (side, 1 - side):
            for p in range(2):
                send_dn(half, p, sp=m)

        def finish(i):
            eo(i, 0).wait_recv()
            total = egot[0, i].astype(F32)
            if i % 2:
                er(i).wait_recv()
                total += egot[1, i].astype(F32)
            at = ds((2 * sources[i] + sides[i]) * dw, dw)
            out_ref[:, at] = (mid[:, at].astype(F32) + 0.5 * total).astype(BF16)

        for i in range(1, chunks, 2):
            eo(i, 1).wait_recv()
            er(i).start()
            if i > 1:
                finish(i - 2)
                finish(i - 3)
        finish(chunks - 1)
        finish(chunks - 2)
        sent(acts.at[0, ds(me * own, own), :], ea_s.at[0])
        sent_gu(place, side, 0, PIECES)
        sent_gu(place, 1 - side, 0, PIECES - 2)
        for half in (side, 1 - side):
            sent_dn(place, half, 0, 2)
        sent(erelay.at[: chunks // 2], er_s.at[0])

    for k in range(1, count):

        @pl.when(place + k < count)
        def _(k=k):
            state_copy(0, k, place).wait_send()

        @pl.when(place >= k)
        def _(k=k):
            state_copy(1, k, place).wait_send()

    for n, t in enumerate(others):
        a2a(n, me, t).wait_send()
    for kind in range(3):
        sent(outw.at[ds(me * width, width), :], ow_s.at[kind])


def fast_body(
    queries,
    key_projected,
    values,
    output_gate_preact,
    forward_decay_logits,
    backward_decay_logits,
    decay_logit_shift,
    decay_spike_values,
    residual,
    head_norm_gain,
    output_projection,
    prenorm_gain,
    gate_projection,
    up_projection,
    down_projection,
):
    count = lax.axis_size("sp")
    tokens, lanes = queries.shape
    width = values.shape[1]
    own, model = residual.shape
    depth, hidden = gate_projection.shape
    dw = down_projection.shape[1] // 2
    chunks = 2 * count
    tps = tokens // own
    blocks = tokens // BLOCK
    dma = lambda *shape: pltpu.SemaphoreType.DMA(shape)
    state = (HEAD_V + 16, lanes)
    V = pltpu.VMEM
    scratch = [
        V((tokens, lanes), BF16),
        V((tokens, width), BF16),
        V((tokens, lanes), BF16),
        V((tokens, lanes), BF16),
        V(decay_logit_shift.shape, F32),
        V(decay_spike_values.shape, F32),
        V((tokens, lanes), BF16),
        V((tokens, width), BF16),
        V((1, width), F32),
        V((1, model), F32),
        dma(10),
        V((tokens, 2 * lanes), F32),
        V((tokens, 2 * lanes), BF16),
        V(state, BF16),
        V(state, BF16),
        V((count - 1,) + state, BF16),
        V((count - 1,) + state, BF16),
        V((HEAD_V, lanes), F32),
        V((HEAD_V, lanes), F32),
        V((blocks, 2 * HEAD_V, lanes), BF16),
        V((tokens, width), BF16),
        V((own, tps * width), BF16),
        V((tps * width, model), BF16),
        V((own, model), BF16),
        V((own, model), BF16),
        V((2, tokens, model), BF16),
        V((2, PIECES, model, hidden // PIECES), BF16),
        V((count, 2, hidden, dw), BF16),
        V((2, tokens, hidden), BF16),
        V((2, chunks, tokens, dw), BF16),
        V((2, chunks, 2, own, dw), BF16),
        V((2, chunks, own, dw), BF16),
        V((2, chunks, own, dw), BF16),
        V((chunks, 2, own, dw), BF16),
        V((2, chunks, own, dw), BF16),
        V((chunks, own, dw), BF16),
        dma(4),
        dma(2, count - 1),
        dma(2, count - 1),
        dma(3),
        dma(tps),
        dma(3),
        dma(6),
        dma(2, 3),
        dma(2, 4),
        dma(1),
        dma(2),
        dma(count, 2),
        dma(2, count, 2, PIECES),
        dma(count, 2),
        dma(count, 2, 2, 2),
        dma(2),
        dma(2, chunks),
        dma(2),
        dma(2, chunks),
        dma(2),
        dma(chunks, 2),
        dma(1),
        dma(chunks),
    ]
    anywhere = pl.BlockSpec(memory_space=pl.ANY)
    return pl.pallas_call(
        layer_kernel,
        out_shape=pltpu.MemorySpace.VMEM((own, model), BF16),
        in_specs=[anywhere] * 15,
        out_specs=VMEM,
        scratch_shapes=scratch,
        compiler_params=pltpu.CompilerParams(
            collective_id=0, has_side_effects=True, vmem_limit_bytes=61000000
        ),
        cost_estimate=cost(3 * 10**10, 3 * 10**7),
        name="layer",
    )(
        key_projected,
        values,
        forward_decay_logits,
        backward_decay_logits,
        decay_logit_shift,
        decay_spike_values,
        queries,
        output_gate_preact,
        head_norm_gain[None, :],
        prenorm_gain[None, :],
        residual,
        output_projection,
        gate_projection,
        up_projection,
        down_projection,
    )


def solution(mesh):
    in_specs = (
        P(("grp", "sp"), "tp"),
        P(("grp", "sp"), "tp"),
        P(("grp", "sp"), "tp"),
        P(("grp", "sp"), "tp"),
        P(("grp", "sp"), "tp"),
        P(("grp", "sp"), "tp"),
        P(None, "tp"),
        P("tp", ("grp", "sp")),
        P(("grp", "sp", "tp"), None),
        P("tp"),
        P("tp", None),
        P(),
        P("sp", "tp"),
        P("sp", "tp"),
        P("tp", "sp"),
    )
    out_specs = P(("grp", "sp", "tp"), None)

    def run(*args):
        lanes = args[0].shape[1]
        sizes = (mesh.shape["grp"], mesh.shape["sp"], mesh.shape["tp"])
        fits = lanes == 2 * KEY_CHANNELS and sizes == (2, 4, 4)
        return fast_body(*args) if fits else body(*args)

    return jax.shard_map(run, mesh=mesh, in_specs=in_specs, out_specs=out_specs, check_vma=False)
```

```python
import functools

import jax
import jax.numpy as jnp
from jax import lax
from jax.experimental import pallas as pl
from jax.experimental.pallas import tpu as pltpu
from jax.sharding import PartitionSpec as P


KEY_CHANNELS = 64
HEAD_V = 128
BLOCK = 64
GATE_DENOMINATOR = 16.0
EPSILON = 1e-06
F32, BF16 = jnp.float32, jnp.bfloat16


def nt(a, b):
    return lax.dot_general(a, b, (((1,), (1,)), ((), ())), preferred_element_type=F32)


def tn(a, b):
    return lax.dot_general(a, b, (((0,), (0,)), ((), ())), preferred_element_type=F32)


def first_head(shape):
    return lax.broadcasted_iota(jnp.int32, shape, 1) < KEY_CHANNELS


VMEM = pl.BlockSpec(memory_space=pltpu.VMEM)


def cost(flops, size):
    return pl.CostEstimate(flops=flops, bytes_accessed=size, transcendentals=0)


def entering(value, axis, join, neutral, backward):
    count = lax.axis_size(axis)
    place = lax.axis_index(axis)
    ahead = count - 1 - place if backward else place
    gathered = jax.tree.map(
        lambda a, kind: lax.all_gather(a.astype(kind), axis), value, (jnp.bfloat16, jnp.bfloat16)
    )
    state = jax.tree.map(lambda a, e: jnp.zeros_like(a) + jnp.asarray(e, a.dtype), value, neutral)

    def one(lap, state):
        source = count - 1 - lap if backward else lap
        return join(
            state,
            jax.tree.map(
                lambda a, own: lax.dynamic_index_in_dim(a, source, 0, False).astype(own.dtype),
                gathered,
                value,
            ),
        )

    return lax.fori_loop(0, ahead, one, state)


def block_sweep(query_in, key_in, values_in, log_decay, span):
    sequence_length, head_count, key_dim = key_in.shape
    block_count = sequence_length // span

    def blocks(tensor):
        return jnp.transpose(
            tensor.reshape(block_count, span, head_count, tensor.shape[-1]), (0, 2, 1, 3)
        )

    lower_mask = jnp.tril(jnp.ones((span, span), dtype=bool))[:, :, None]

    def advance(carried, inputs):
        memory, offset = carried
        key_blk, value_blk, decay_blk, query_blk = inputs
        within = jnp.cumsum(decay_blk, axis=1)
        ending = within[:, -1, :]
        memory_next = jnp.exp(ending)[:, :, None] * memory + jnp.einsum(
            "hjd,hje->hde",
            key_blk * jnp.exp(ending[:, None, :] - within),
            value_blk,
            precision=lax.Precision.HIGHEST,
        )
        result = jnp.einsum(
            "hid,hde->hie", query_blk * jnp.exp(within), memory, precision=lax.Precision.HIGHEST
        )
        spread = jnp.exp(
            jnp.where(lower_mask, within[:, :, None, :] - within[:, None, :, :], -jnp.inf)
        )
        scores = jnp.einsum(
            "hid,hjd,hijd->hij", query_blk, key_blk, spread, precision=lax.Precision.HIGHEST
        )
        result = result + jnp.einsum(
            "hij,hje->hie", scores, value_blk, precision=lax.Precision.HIGHEST
        )
        reached = query_blk * jnp.exp(within + offset[:, None, :])
        return ((memory_next, offset + ending), (result, reached))

    start_memory = jnp.zeros((head_count, key_dim, values_in.shape[-1]), jnp.float32)
    start_offset = jnp.zeros((head_count, key_dim), jnp.float32)
    (memory, decay_total), (outputs, reached) = lax.scan(
        advance,
        (start_memory, start_offset),
        (blocks(key_in), blocks(values_in), blocks(log_decay), blocks(query_in)),
    )

    def unblock(tensor):
        return jnp.transpose(tensor, (0, 2, 1, 3)).reshape(
            sequence_length, head_count, tensor.shape[-1]
        )

    return (unblock(outputs), unblock(reached), memory, decay_total)


def head_mix(combined, head_norm_gain, output_gate_preact):
    sequence_length, head_count, width = combined.shape
    inverse = lax.rsqrt(jnp.mean(combined * combined, axis=-1, keepdims=True) + EPSILON)
    gate_act = jax.nn.silu(
        output_gate_preact.astype(jnp.float32).reshape(sequence_length, head_count, width)
    )
    weighted = combined * inverse * head_norm_gain.reshape(head_count, width) * gate_act
    return weighted.reshape(sequence_length, head_count * width).astype(jnp.bfloat16)


def row_norm(mid_rows, prenorm_gain):
    wide = mid_rows.astype(jnp.float32)
    inverse = lax.rsqrt(jnp.mean(wide * wide, axis=-1, keepdims=True) + EPSILON)
    return (wide * inverse * prenorm_gain).astype(jnp.bfloat16)


def combine_states(earlier, later):
    decay_early, memory_early = earlier
    decay_late, memory_late = later
    return (decay_early * decay_late, decay_late[:, :, None] * memory_early + memory_late)


def body(
    queries,
    key_projected,
    values,
    output_gate_preact,
    forward_decay_logits,
    backward_decay_logits,
    decay_logit_shift,
    decay_spike_values,
    residual,
    head_norm_gain,
    output_projection,
    prenorm_gain,
    gate_projection,
    up_projection,
    down_projection,
):
    sequence_length = queries.shape[0]
    local_heads = queries.shape[1] // KEY_CHANNELS
    query_f = queries.astype(jnp.float32).reshape(
        sequence_length, local_heads, KEY_CHANNELS
    ) * KEY_CHANNELS ** (-0.5)
    keys_f = key_projected.astype(jnp.float32).reshape(sequence_length, local_heads, KEY_CHANNELS)
    values_f = values.astype(jnp.float32).reshape(sequence_length, local_heads, HEAD_V)
    decay_spikes = jnp.transpose(decay_spike_values)[:, :, None]
    logit_shifts = decay_logit_shift.reshape(2, local_heads, KEY_CHANNELS)
    forward_decay = (
        jax.nn.log_sigmoid(
            forward_decay_logits.astype(jnp.float32).reshape(
                sequence_length, local_heads, KEY_CHANNELS
            )
            + logit_shifts[0]
        )
        / GATE_DENOMINATOR
        + decay_spikes
    )
    backward_decay = (
        jax.nn.log_sigmoid(
            backward_decay_logits.astype(jnp.float32).reshape(
                sequence_length, local_heads, KEY_CHANNELS
            )
            + logit_shifts[1]
        )
        / GATE_DENOMINATOR
        + decay_spikes
    )
    fwd_out, fwd_reach, fwd_memory, fwd_total = block_sweep(
        query_f, keys_f, values_f, forward_decay, BLOCK
    )
    bwd_out, bwd_reach, bwd_memory, bwd_total = block_sweep(
        query_f[::-1], keys_f[::-1], values_f[::-1], backward_decay[::-1], BLOCK
    )
    identity = (jnp.ones_like(fwd_total), jnp.zeros_like(fwd_memory))
    fwd_incoming = entering(
        (jnp.exp(fwd_total), fwd_memory), "sp", combine_states, identity, False
    )[1]
    bwd_incoming = entering((jnp.exp(bwd_total), bwd_memory), "sp", combine_states, identity, True)[
        1
    ]
    fwd_full = fwd_out + jnp.einsum(
        "lhd,hde->lhe", fwd_reach, fwd_incoming, precision=lax.Precision.HIGHEST
    )
    bwd_full = bwd_out + jnp.einsum(
        "lhd,hde->lhe", bwd_reach, bwd_incoming, precision=lax.Precision.HIGHEST
    )
    attended = head_mix(fwd_full + bwd_full[::-1], head_norm_gain, output_gate_preact)
    token_rows = lax.all_to_all(attended, "tp", split_axis=0, concat_axis=1, tiled=True)
    whole_out = lax.all_gather(output_projection, "tp", axis=0, tiled=True)
    projected = jnp.dot(token_rows, whole_out, preferred_element_type=jnp.float32)
    mid_rows = (residual.astype(jnp.float32) + projected).astype(jnp.bfloat16)
    normed = row_norm(mid_rows, prenorm_gain)
    fetched = (
        lax.all_gather(gate_projection, "sp", axis=0, tiled=True),
        lax.all_gather(up_projection, "sp", axis=0, tiled=True),
        lax.all_gather(down_projection, "sp", axis=1, tiled=True),
    )
    gate_full, up_full, down_full = fetched
    piece = lax.all_gather(normed, "tp", axis=0, tiled=True)
    gate_part = jnp.dot(piece, gate_full, preferred_element_type=jnp.float32)
    up_part = jnp.dot(piece, up_full, preferred_element_type=jnp.float32)
    hidden = (jax.nn.silu(gate_part) * up_part).astype(jnp.bfloat16)
    summed = lax.psum_scatter(
        jnp.dot(hidden, down_full, preferred_element_type=jnp.float32).astype(jnp.bfloat16),
        "tp",
        scatter_dimension=0,
        tiled=True,
    ).astype(jnp.float32)
    return (mid_rows.astype(jnp.float32) + 0.5 * summed).astype(jnp.bfloat16)


MESH = pl.DeviceIdType.MESH
PIECES = 5


def log_decay(logits, shift, spike):
    x = logits.astype(F32) + shift
    soft = jnp.minimum(x, 0.0) - jnp.log1p(jnp.exp(-jnp.abs(x)))
    return soft / GATE_DENOMINATOR + spike


def own_states(k_ref, v_ref, fd_ref, bd_ref, shift_ref, spike_ref, within_ref, kd_ref, fwd_ref, bwd_ref):
    tokens, lanes = k_ref.shape
    blocks = tokens // BLOCK
    row = lax.broadcasted_iota(jnp.int32, (2 * BLOCK, 2 * BLOCK), 0)
    col = lax.broadcasted_iota(jnp.int32, (2 * BLOCK, 2 * BLOCK), 1)
    r, c = row % BLOCK, col % BLOCK
    ahead = jnp.where(row < BLOCK, r - c, c - r)
    tri = jnp.where(ahead >= 0, 1.0, 0.0).astype(BF16)
    half = first_head((BLOCK, lanes))
    spikes = jnp.transpose(jnp.concatenate([spike_ref[...]] * 4, axis=0))
    ends = []
    for b in range(blocks):
        at = slice(b * BLOCK, (b + 1) * BLOCK)
        spike = jnp.where(half, spikes[at, 0:1], spikes[at, 1:2])
        parts = [log_decay(ref[at, :], shift_ref[n : n + 1, :], spike) for n, ref in enumerate((fd_ref, bd_ref))]
        d = jnp.concatenate(parts, axis=1)
        hi = d.astype(BF16)
        lo = (d - hi.astype(F32)).astype(BF16)
        both = jnp.dot(tri, jnp.concatenate([hi, lo], axis=0), preferred_element_type=F32)
        fwd, bwd = both[:BLOCK, :lanes], both[BLOCK:, lanes:]
        within_ref[at, :lanes] = fwd
        within_ref[at, lanes:] = bwd
        ends.append((fwd[BLOCK - 1 :, :], bwd[:1, :]))
    zero = jnp.zeros((1, lanes), F32)
    after, before = [zero] * blocks, [zero] * blocks
    for b in range(1, blocks):
        before[b] = before[b - 1] + ends[b - 1][1]
        after[blocks - 1 - b] = after[blocks - b] + ends[blocks - b][0]
    totals = after[0] + ends[0][0], before[-1] + ends[-1][1]
    for b in range(blocks):
        at = slice(b * BLOCK, (b + 1) * BLOCK)
        key = k_ref[at, :].astype(F32)
        kd_ref[at, :lanes] = (key * jnp.exp((ends[b][0] + after[b]) - within_ref[at, :lanes])).astype(BF16)
        kd_ref[at, lanes:] = (key * jnp.exp((ends[b][1] + before[b]) - within_ref[at, lanes:])).astype(BF16)
    full = tn(v_ref[...], kd_ref[...])
    mine = first_head((HEAD_V, lanes))
    for n, ref in enumerate((fwd_ref, bwd_ref)):
        u = full[:, n * lanes : (n + 1) * lanes]
        ref[:HEAD_V, :] = jnp.where(mine, u[:HEAD_V], u[HEAD_V:]).astype(BF16)
        ref[HEAD_V:, :] = jnp.broadcast_to(jnp.exp(totals[n]), (16, lanes)).astype(BF16)


def spread(state):
    mine = first_head(state.shape)
    return jnp.concatenate([jnp.where(mine, state, 0.0), jnp.where(mine, 0.0, state)], axis=0).astype(BF16)


def pack(u):
    top = u[:HEAD_V]
    return jnp.where(first_head(top.shape), top, u[HEAD_V:])


def backward_states(k_ref, v_ref, within_ref, state, held_ref):
    tokens, lanes = k_ref.shape
    for b in reversed(range(tokens // BLOCK)):
        at = slice(b * BLOCK, (b + 1) * BLOCK)
        held_ref[b] = spread(state)
        within = within_ref[at, lanes:]
        end = within[:1, :]
        kd = (k_ref[at, :].astype(F32) * jnp.exp(end - within)).astype(BF16)
        state = state * jnp.exp(end) + pack(tn(v_ref[at, :], kd))


def attend(q_ref, k_ref, v_ref, within_ref, gate_ref, gain_ref, fwd_state, held_ref, out_ref):
    tokens, lanes = k_ref.shape
    row = lax.broadcasted_iota(jnp.int32, (2 * BLOCK, BLOCK), 0) % BLOCK
    col = lax.broadcasted_iota(jnp.int32, (2 * BLOCK, BLOCK), 1)
    half = first_head((BLOCK, lanes))
    for b in range(tokens // BLOCK):
        at = slice(b * BLOCK, (b + 1) * BLOCK)
        query = q_ref[at, :].astype(F32) * KEY_CHANNELS ** (-0.5)
        key = k_ref[at, :].astype(F32)
        value = v_ref[at, :]
        scores, reach = [], []
        for n in range(2):
            within = within_ref[at, n * lanes : (n + 1) * lanes]
            pivot = within[BLOCK // 2 - 1 + n : BLOCK // 2 + n, :]
            near = (query * jnp.exp(within - pivot)).astype(BF16)
            far = (key * jnp.exp(pivot - within)).astype(BF16)
            zero = jnp.zeros_like(near)
            pair = jnp.concatenate([jnp.where(half, near, zero), jnp.where(half, zero, near)], axis=0)
            scores.append(nt(pair, far))
            reach.append((query * jnp.exp(within)).astype(BF16))
        score = (jnp.where(col <= row, scores[0], 0.0) + jnp.where(col >= row, scores[1], 0.0)).astype(BF16)
        states = jnp.concatenate([spread(fwd_state), held_ref[b]], axis=1)
        result = nt(jnp.concatenate(reach, axis=1), states)
        for h in range(2):
            lane = slice(h * HEAD_V, (h + 1) * HEAD_V)
            x = result[:, lane] + jnp.dot(
                score[h * BLOCK : (h + 1) * BLOCK], value[:, lane], preferred_element_type=F32
            )
            inverse = lax.rsqrt(jnp.mean(x * x, axis=-1, keepdims=True) + EPSILON)
            g = gate_ref[at, lane].astype(F32)
            out_ref[at, lane] = (x * inverse * gain_ref[:, lane] * (g * jax.nn.sigmoid(g))).astype(BF16)
        within = within_ref[at, :lanes]
        end = within[BLOCK - 1 :, :]
        kd = (key * jnp.exp(end - within)).astype(BF16)
        fwd_state = fwd_state * jnp.exp(end) + pack(tn(value, kd))


def pick(i, table):
    value = table[0]
    for n, item in enumerate(table[1:], 1):
        value = jnp.where(i == n, item, value)
    return value


def ds(first, size):
    return pl.ds(pl.multiple_of(first, size if size % 128 == 0 else 16), size)


def layer_kernel(
    k_hbm, v_hbm, fd_hbm, bd_hbm, shift_hbm, spike_hbm, q_hbm, gate_hbm, gain_hbm, norm_hbm,
    res_hbm, out_hbm, g_hbm, u_hbm, d_hbm,
    out_ref,
    k_ref, v_ref, fd_ref, bd_ref, shift_ref, spike_ref, q_ref, gate_ref, gain_ref, norm_ref, in_s,
    within, kd, fown, bown, fgot, bgot, fstate, bstate, held, attended, rows, outw, res, mid, acts,
    wgu, wd, hid, part, got, xsend, xgot, esend, egot, erelay,
    loc, st_s, st_r, a2a_s, a2a_r, ow_s, ow_r, ag_s, ag_r, ea_s, ea_r, gs, gr, dsd, drv, cr_s, cr_r, xo_s, xo_r,
    eo_s, eo_r, er_s, er_r,
):
    count = lax.axis_size("sp")
    side, place, me = lax.axis_index("grp"), lax.axis_index("sp"), lax.axis_index("tp")
    chip, core = me // 2, me % 2
    tc, tx, td = 2 * chip + 1 - core, 2 * (1 - chip) + core, 2 * (1 - chip) + 1 - core
    upper = place // 2
    e, m, o, oe = 3 * upper, 1 + upper, 2 - upper, 3 - 3 * upper
    middle = place * (count - 1 - place) > 0
    outer = jnp.logical_not(middle)
    own = res.shape[0]
    width = attended.shape[1]
    model = mid.shape[1]
    depth, hidden = g_hbm.shape
    tile = hidden // PIECES
    hr = depth // 2
    dr = hidden // 2
    dw = wd.shape[3]
    chunks = part.shape[1]
    orow = width // 4
    nrow = own // 2

    def remote(src, dst, send, recv, **dev):
        return pltpu.make_async_remote_copy(
            src_ref=src, dst_ref=dst, send_sem=send, recv_sem=recv, device_id=dev, device_id_type=MESH
        )

    def gu(n, source, half, p, local=False, again=False, **dev):
        dst = wgu.at[n, p, ds(source * depth + half * hr, hr), :]
        src = (g_hbm, u_hbm)[n].at[ds(half * hr, hr), ds(p * tile, tile)] if local else dst
        send = gs.at[source, 1 - half if again else half]
        return remote(src, dst, send, gr.at[n, source, half, p], **(dev or dict(sp=o)))

    def dn(source, half, p, r, local=False, **dev):
        dst = wd.at[source, p, ds(half * dr + r * (dr // 2), dr // 2), :]
        src = d_hbm.at[ds(half * dr + r * (dr // 2), dr // 2), p * dw : (p + 1) * dw] if local else dst
        return remote(src, dst, dsd.at[source, half], drv.at[source, half, p, r], **(dev or dict(sp=o)))

    def send_gu(source, half, p, local=False, again=False, **dev):
        for n in range(2):
            gu(n, source, half, p, local, again, **dev).start()

    def take_gu(source, half, p):
        for n in range(2):
            gu(n, source, half, p).wait_recv()

    def relay_gu(source, p, **dev):
        for n in range(2):
            gu(n, source, side, p).wait_recv()
            gu(n, source, side, p, **dev).start()

    def send_dn(half, p, **dev):
        for r in range(2):
            dn(place, half, p, r, True, **dev).start()

    def take_dn(source, half, p):
        for r in range(2):
            dn(source, half, p, r).wait_recv()

    def relay_dn(source, p, r, **dev):
        dn(source, side, p, r).wait_recv()
        dn(source, side, p, r, **dev).start()

    def sent(ref, sem):
        remote(ref, ref, sem, sem, sp=o).wait_send()

    def sent_gu(source, half, low, high, again=False):
        at = ds(source * depth + half * hr, hr)
        sent(wgu.at[:, low:high, at, :], gs.at[source, 1 - half if again else half])

    def sent_dn(source, half, low, high):
        sent(wd.at[source, low:high, ds(half * dr, dr), :], dsd.at[source, half])

    def landed(ref, sem):
        remote(ref, ref, sem, sem, sp=o).wait_recv()

    def ow(kind, block, i, dev, local=False):
        dst = outw.at[ds(block * width + i * orow, orow), :]
        src = out_hbm.at[i * orow : (i + 1) * orow, :] if local else dst
        return remote(src, dst, ow_s.at[kind], ow_r.at[i if kind == 0 else 3 + kind], tp=dev)

    def relay_ow(i):
        ow(0, tx, i, tc).wait_recv()
        ow(2, tx, i, tc).start()

    def a2a(n, block, dev):
        return remote(
            attended.at[ds(dev * own, own), :], rows.at[:, ds(block * width, width)], a2a_s.at[n], a2a_r.at[block], tp=dev
        )

    def ag(q, kind, block, i, dev):
        at = acts.at[q, ds(block * own + i * nrow, nrow), :]
        return remote(at, at, ag_s.at[q, kind], ag_r.at[q, i if kind == 0 else 1 + kind], tp=dev)

    def to_host(i):
        at = ds(me * own + i * nrow, nrow)
        return remote(acts.at[0, at, :], acts.at[1, at, :], ea_s.at[0], ea_r.at[i], sp=m)

    def gathered(q):
        for kind, block in ((1, tc), (2, td)):
            landed(acts.at[q, ds(block * own, own), :], ag_r.at[q, 1 + kind])

    def state_copy(n, k, dev):
        src, dst = ((fown, fgot), (bown, bgot))[n]
        return remote(src, dst.at[k - 1], st_s.at[n, k - 1], st_r.at[n, k - 1], sp=dev)

    def cr(q, i, j):
        block = 2 * j + 1 - core
        return remote(part.at[q, i, ds(block * own, own), :], got.at[q, i, j], cr_s.at[q], cr_r.at[q, i], tp=tc)

    def xo(q, i):
        return remote(xsend.at[q, i], xgot.at[q, i], xo_s.at[q], xo_r.at[q, i], tp=tx)

    def eo(i, n):
        dst = egot.at[0, i] if n == 0 else erelay.at[i]
        return remote(esend.at[i, n], dst, eo_s.at[n], eo_r.at[i, n], sp=e)

    def er(i):
        return remote(erelay.at[i], egot.at[1, i], er_s.at[0], er_r.at[i], tp=tx)

    own_copies = []
    for p in range(PIECES):
        for n in range(2):
            own_copies.append(
                pltpu.make_async_copy(
                    (g_hbm, u_hbm)[n].at[:, p * tile : (p + 1) * tile],
                    wgu.at[n, p, ds(place * depth, depth), :],
                    loc.at[0],
                )
            )
    for p in range(2):
        own_copies.append(pltpu.make_async_copy(d_hbm.at[:, p * dw : (p + 1) * dw], wd.at[place, p], loc.at[1]))
    own_gu = wgu.at[:, :, ds(place * depth, depth), :]
    own_waits = [
        pltpu.make_async_copy(own_gu, own_gu, loc.at[0]),
        pltpu.make_async_copy(wd.at[place], wd.at[place], loc.at[1]),
    ]
    own_out = pltpu.make_async_copy(out_hbm, outw.at[ds(me * width, width), :], loc.at[2])
    own_res = pltpu.make_async_copy(res_hbm, res, loc.at[3])

    barrier = pltpu.get_barrier_semaphore()
    friends = [dict(sp=lax.rem(place + k, count)) for k in range(1, count)]
    friends += [dict(grp=1 - side)] + [dict(tp=t) for t in (tc, tx, td)]
    for friend in friends:
        pl.semaphore_signal(barrier, inc=1, device_id=friend, device_id_type=MESH)
    loads = [
        pltpu.make_async_copy(src, dst, in_s.at[n])
        for n, (src, dst) in enumerate(
            (
                (k_hbm, k_ref),
                (v_hbm, v_ref),
                (fd_hbm, fd_ref),
                (bd_hbm, bd_ref),
                (shift_hbm, shift_ref),
                (spike_hbm, spike_ref),
                (q_hbm, q_ref),
                (gate_hbm, gate_ref),
                (gain_hbm, gain_ref),
                (norm_hbm, norm_ref),
            )
        )
    ]
    for load in loads:
        load.start()
    pl.semaphore_wait(barrier, len(friends))

    @pl.when(middle)
    def _():
        gu(0, place, side, 0, True, sp=o).start()

    @pl.when(outer)
    def _():
        gu(0, place, side, 0, True, sp=m).start()

    for i in range(4):
        ow(0, me, i, tx, True).start()
    for i in range(4):
        ow(1, me, i, tc, True).start()
    for load in loads[:6]:
        load.wait()
    own_states(k_ref, v_ref, fd_ref, bd_ref, shift_ref, spike_ref, within, kd, fown, bown)

    for k in range(1, count):

        @pl.when(place + k < count)
        def _(k=k):
            state_copy(0, k, place + k).start()

        @pl.when(place >= k)
        def _(k=k):
            state_copy(1, k, place - k).start()

    @pl.when(middle)
    def _():
        gu(1, place, side, 0, True, sp=o).start()
        for p in range(1, PIECES):
            send_gu(place, side, p, True, sp=o)

    @pl.when(outer)
    def _():
        gu(1, place, side, 0, True, sp=m).start()
        for p in range(1, PIECES):
            send_gu(place, side, p, True, sp=m)
        send_gu(place, 1 - side, 0, True, sp=m)

    own_out.start()
    own_res.start()

    @pl.when(middle)
    def _():
        for copy in own_copies:
            copy.start()

    for load in loads[6:]:
        load.wait()
    fstate[...] = jnp.zeros_like(fstate)
    bstate[...] = jnp.zeros_like(bstate)
    for k in reversed(range(1, count)):

        @pl.when(place >= k)
        def _(k=k):
            state_copy(0, k, place).wait_recv()
            decay = fgot[k - 1, HEAD_V : HEAD_V + 1, :].astype(F32)
            fstate[...] = fstate[...] * decay + fgot[k - 1, :HEAD_V, :].astype(F32)

        @pl.when(place + k < count)
        def _(k=k):
            state_copy(1, k, place).wait_recv()
            decay = bgot[k - 1, HEAD_V : HEAD_V + 1, :].astype(F32)
            bstate[...] = bstate[...] * decay + bgot[k - 1, :HEAD_V, :].astype(F32)

    backward_states(k_ref, v_ref, within, bstate[...], held)
    attend(q_ref, k_ref, v_ref, within, gate_ref, gain_ref, fstate[...], held, attended)
    others = (tx, td, tc)
    for n, t in enumerate(others):
        a2a(n, me, t).start()
    rows[:, ds(me * width, width)] = attended[ds(me * own, own), :]

    for p in range(4):
        relay_ow(p)

        @pl.when(middle)
        def _(p=p):
            relay_gu(o, p, grp=1 - side)
            relay_gu(e, p, sp=o)

    for t in others:
        a2a(0, t, t).wait_recv()
    for kind, t in ((1, tc), (2, td)):
        landed(outw.at[ds(t * width, width), :], ow_r.at[3 + kind])
    own_out.wait()
    own_res.wait()

    total = jnp.zeros((own, 1), F32)
    wide = 512
    for n in range(model // wide):
        at = slice(n * wide, (n + 1) * wide)
        projected = jnp.dot(rows[...], outw[:, at], preferred_element_type=F32)
        mixed = (res[:, at].astype(F32) + projected).astype(BF16)
        mid[:, at] = mixed
        mixed = mixed.astype(F32)
        total += jnp.sum(mixed * mixed, axis=-1, keepdims=True)
    inverse = lax.rsqrt(total / model + EPSILON)
    for n in range(model // wide):
        at = slice(n * wide, (n + 1) * wide)
        acts[0, ds(me * own, own), at] = (mid[:, at].astype(F32) * inverse * norm_ref[:, at]).astype(BF16)

    direct = (1, 1, 0, 0, 0, 1, 0, 1)
    whole = [i for i, d in enumerate(direct) if d]

    def straight(i):
        return direct[i] if isinstance(i, int) else pick(i, direct)

    sources = (m, m, o, e, oe, e, oe, o)
    sides = (0, 1, 0, 0, 0, 1, 1, 1)

    @pl.when(middle)
    def _():
        for i in range(2):
            ag(0, 0, me, i, tx).start()
            ag(0, 1, me, i, tc).start()
        relay_gu(o, 4, grp=1 - side)
        relay_gu(e, 4, sp=o)
        send_gu(e, side, PIECES - 1, again=True, grp=1 - side)
        for p in range(2):
            send_dn(side, p, sp=o)
        for copy in own_waits:
            copy.wait()

        def relay_own(i):
            ag(0, 0, tx, i, tc).wait_recv()
            ag(0, 2, tx, i, tc).start()

        def relay_hosted(i):
            to_host(i).wait_recv()
            ag(1, 0, me, i, tx).start()
            ag(1, 1, me, i, tc).start()

        def pass_hosted(i):
            ag(1, 0, tx, i, tc).wait_recv()
            ag(1, 2, tx, i, tc).start()

        relay_gu(oe, 0, grp=1 - side)
        relay_own(0)
        relay_gu(oe, 1, grp=1 - side)
        relay_hosted(0)
        relay_gu(oe, 2, grp=1 - side)
        relay_own(1)

        order = [(0, 0), (0, 1), (0, 2), (0, 4), (1, 0), (1, 1), (0, 3), (1, 2), (1, 3), (1, 4)]

        def fold(i, q):
            landed(got.at[q, i], cr_r.at[q, i])

            def both(block, j):
                return part[q, i, ds(block * own, own), :].astype(F32) + got[q, i, j].astype(F32)

            @pl.when(jnp.logical_or(q == 0, straight(i) == 0))
            def _():
                xsend[q, i] = both(tx, 1 - chip).astype(BF16)
                xo(q, i).start()

            @pl.when(jnp.logical_and(q == 1, straight(i) == 1))
            def _():
                esend[i, 1] = both(tx, 1 - chip).astype(BF16)
                eo(i, 1).start()
                esend[i, 0] = both(me, chip).astype(BF16)
                eo(i, 0).start()

        def push(i):
            xo(1, i).wait_recv()
            mixed = part[1, i, ds(me * own, own), :].astype(F32) + got[1, i, chip].astype(F32)
            esend[i, 0] = (mixed + xgot[1, i].astype(F32)).astype(BF16)
            eo(i, 0).start()

        def product(q, i):
            weight = wd[pick(i, sources), pick(i, sides)]
            part[q, i] = jnp.dot(hid[q], weight, preferred_element_type=F32).astype(BF16)
            for j in range(2):
                cr(q, i, j).start()

        def first(i, carry):
            q, j = pick(i, [a for a, _ in order]), pick(i, [b for _, b in order])

            @pl.when(i == 0)
            def _():
                gathered(0)

            @pl.when(i == 1)
            def _():
                relay_hosted(1)
                relay_gu(oe, 3, grp=1 - side)
                pass_hosted(0)

            @pl.when(i == 2)
            def _():
                relay_gu(oe, 4, grp=1 - side)
                send_gu(e, side, PIECES - 2, again=True, grp=1 - side)

            @pl.when(i == 4)
            def _():
                pass_hosted(1)
                for r in range(2):
                    relay_dn(o, 0, r, grp=1 - side)
                gathered(1)

            @pl.when(i == 5)
            def _():
                relay_dn(e, 0, 0, sp=o)

            @pl.when(i == 6)
            def _():
                relay_dn(e, 0, 1, sp=o)

            @pl.when(i == 7)
            def _():
                for c in range(2):
                    product(0, c)
                relay_dn(e, 1, 0, sp=o)

            @pl.when(i == 8)
            def _():
                relay_dn(oe, 0, 0, grp=1 - side)
                relay_dn(e, 1, 1, sp=o)
                send_dn(1 - side, 1, sp=o)
                for c in range(2):
                    fold(c, 0)

            @pl.when(i == 9)
            def _():
                relay_dn(oe, 0, 1, grp=1 - side)

            @pl.when(q == 0)
            def _():
                for source in (o, oe, e):
                    take_gu(source, 1 - side, j)

            g = jnp.dot(acts[q], wgu[0, j], preferred_element_type=F32)
            u = jnp.dot(acts[q], wgu[1, j], preferred_element_type=F32)
            hid[q, :, ds(j * tile, tile)] = (g * jax.nn.sigmoid(g) * u).astype(BF16)
            return carry

        lax.fori_loop(0, len(order), first, 0)

        steps = [(1, 0), (1, 1)] + [(q, c) for c in range(2, chunks) for q in (1, 0)]

        def step(s):
            return pick(s, [a for a, _ in steps]), pick(s, [b for _, b in steps])

        def second(s, carry):
            q, i = step(s)

            @pl.when(s == 2)
            def _():
                take_dn(o, 1 - side, 0)

            @pl.when(s == 4)
            def _():
                relay_dn(oe, 1, 0, grp=1 - side)
                take_dn(e, 1 - side, 0)

            @pl.when(s == 6)
            def _():
                take_dn(oe, 1 - side, 0)

            @pl.when(s == 8)
            def _():
                relay_dn(oe, 1, 1, grp=1 - side)
                fold(4, 1)
                fold(4, 0)
                take_dn(e, 1 - side, 1)

            @pl.when(s == 10)
            def _():
                take_dn(oe, 1 - side, 1)

            @pl.when(s == 12)
            def _():
                take_dn(o, side, 1)
                take_dn(o, 1 - side, 1)

            product(q, i)

            @pl.when(((s > 1) & (s < 8)) | (s > 9))
            def _():
                fold(*reversed(step(s - 2)))

            @pl.when((s == 9) | (s == 10) | (s == 13))
            def _():
                push(pick(s - 9, (2, 3, 4, 4, 4)))

            return carry

        lax.fori_loop(0, len(steps), second, 0)
        for q in (1, 0):
            fold(chunks - 1, q)
        push(chunks - 2)

        for i in range(chunks):
            xo(0, i).wait_recv()
            at = ds((2 * sources[i] + sides[i]) * dw, dw)
            total = part[0, i, ds(me * own, own), :].astype(F32) + got[0, i, chip].astype(F32) + xgot[0, i].astype(F32)
            out_ref[:, at] = (mid[:, at].astype(F32) + 0.5 * total).astype(BF16)

        for source in (place, e, o, oe):
            sent_gu(source, side, 0, PIECES)
        sent_gu(e, side, PIECES - 2, PIECES, again=True)
        for source in (place, e, oe):
            sent_dn(source, side, 0, 2)
        sent_dn(o, side, 0, 1)
        sent_dn(place, 1 - side, 1, 2)
        for q in range(2):
            for kind in range(3):
                sent(acts.at[q, ds(me * own, own), :], ag_s.at[q, kind])
            sent(got.at[q], cr_s.at[q])
        sent(xsend.at[0], xo_s.at[0])
        sent(xsend.at[1, : chunks - len(whole)], xo_s.at[1])
        sent(esend.at[:, 0], eo_s.at[0])
        sent(esend.at[: len(whole), 1], eo_s.at[1])

    @pl.when(outer)
    def _():
        for i in range(2):
            to_host(i).start()
        for p in range(1, PIECES - 2):
            send_gu(place, 1 - side, p, True, sp=m)
        for half in (side, 1 - side):
            for p in range(2):
                send_dn(half, p, sp=m)

        def finish(i):
            eo(i, 0).wait_recv()
            total = egot[0, i].astype(F32)
            if direct[i]:
                er(i).wait_recv()
                total += egot[1, i].astype(F32)
            at = ds((2 * sources[i] + sides[i]) * dw, dw)
            out_ref[:, at] = (mid[:, at].astype(F32) + 0.5 * total).astype(BF16)

        for i in range(chunks):
            if direct[i]:
                eo(i, 1).wait_recv()
                er(i).start()
            if i > 1:
                finish(i - 2)
        finish(chunks - 2)
        finish(chunks - 1)
        sent(acts.at[0, ds(me * own, own), :], ea_s.at[0])
        sent_gu(place, side, 0, PIECES)
        sent_gu(place, 1 - side, 0, PIECES - 2)
        for half in (side, 1 - side):
            sent_dn(place, half, 0, 2)
        sent(erelay.at[: len(whole)], er_s.at[0])

    for k in range(1, count):

        @pl.when(place + k < count)
        def _(k=k):
            state_copy(0, k, place).wait_send()

        @pl.when(place >= k)
        def _(k=k):
            state_copy(1, k, place).wait_send()

    for n, t in enumerate(others):
        a2a(n, me, t).wait_send()
    for kind in range(3):
        sent(outw.at[ds(me * width, width), :], ow_s.at[kind])


def fast_body(
    queries,
    key_projected,
    values,
    output_gate_preact,
    forward_decay_logits,
    backward_decay_logits,
    decay_logit_shift,
    decay_spike_values,
    residual,
    head_norm_gain,
    output_projection,
    prenorm_gain,
    gate_projection,
    up_projection,
    down_projection,
):
    count = lax.axis_size("sp")
    tokens, lanes = queries.shape
    width = values.shape[1]
    own, model = residual.shape
    depth, hidden = gate_projection.shape
    dw = down_projection.shape[1] // 2
    chunks = 2 * count
    tps = tokens // own
    blocks = tokens // BLOCK
    dma = lambda *shape: pltpu.SemaphoreType.DMA(shape)
    state = (HEAD_V + 16, lanes)
    V = pltpu.VMEM
    scratch = [
        V((tokens, lanes), BF16),
        V((tokens, width), BF16),
        V((tokens, lanes), BF16),
        V((tokens, lanes), BF16),
        V(decay_logit_shift.shape, F32),
        V(decay_spike_values.shape, F32),
        V((tokens, lanes), BF16),
        V((tokens, width), BF16),
        V((1, width), F32),
        V((1, model), F32),
        dma(10),
        V((tokens, 2 * lanes), F32),
        V((tokens, 2 * lanes), BF16),
        V(state, BF16),
        V(state, BF16),
        V((count - 1,) + state, BF16),
        V((count - 1,) + state, BF16),
        V((HEAD_V, lanes), F32),
        V((HEAD_V, lanes), F32),
        V((blocks, 2 * HEAD_V, lanes), BF16),
        V((tokens, width), BF16),
        V((own, tps * width), BF16),
        V((tps * width, model), BF16),
        V((own, model), BF16),
        V((own, model), BF16),
        V((2, tokens, model), BF16),
        V((2, PIECES, model, hidden // PIECES), BF16),
        V((count, 2, hidden, dw), BF16),
        V((2, tokens, hidden), BF16),
        V((2, chunks, tokens, dw), BF16),
        V((2, chunks, 2, own, dw), BF16),
        V((2, chunks, own, dw), BF16),
        V((2, chunks, own, dw), BF16),
        V((chunks, 2, own, dw), BF16),
        V((2, chunks, own, dw), BF16),
        V((chunks, own, dw), BF16),
        dma(4),
        dma(2, count - 1),
        dma(2, count - 1),
        dma(3),
        dma(tps),
        dma(3),
        dma(6),
        dma(2, 3),
        dma(2, 4),
        dma(1),
        dma(2),
        dma(count, 2),
        dma(2, count, 2, PIECES),
        dma(count, 2),
        dma(count, 2, 2, 2),
        dma(2),
        dma(2, chunks),
        dma(2),
        dma(2, chunks),
        dma(2),
        dma(chunks, 2),
        dma(1),
        dma(chunks),
    ]
    anywhere = pl.BlockSpec(memory_space=pl.ANY)
    return pl.pallas_call(
        layer_kernel,
        out_shape=pltpu.MemorySpace.VMEM((own, model), BF16),
        in_specs=[anywhere] * 15,
        out_specs=VMEM,
        scratch_shapes=scratch,
        compiler_params=pltpu.CompilerParams(
            collective_id=0, has_side_effects=True, vmem_limit_bytes=61000000
        ),
        cost_estimate=cost(3 * 10**10, 3 * 10**7),
        name="layer",
    )(
        key_projected,
        values,
        forward_decay_logits,
        backward_decay_logits,
        decay_logit_shift,
        decay_spike_values,
        queries,
        output_gate_preact,
        head_norm_gain[None, :],
        prenorm_gain[None, :],
        residual,
        output_projection,
        gate_projection,
        up_projection,
        down_projection,
    )


def solution(mesh):
    in_specs = (
        P(("grp", "sp"), "tp"),
        P(("grp", "sp"), "tp"),
        P(("grp", "sp"), "tp"),
        P(("grp", "sp"), "tp"),
        P(("grp", "sp"), "tp"),
        P(("grp", "sp"), "tp"),
        P(None, "tp"),
        P("tp", ("grp", "sp")),
        P(("grp", "sp", "tp"), None),
        P("tp"),
        P("tp", None),
        P(),
        P("sp", "tp"),
        P("sp", "tp"),
        P("tp", "sp"),
    )
    out_specs = P(("grp", "sp", "tp"), None)

    def run(*args):
        lanes = args[0].shape[1]
        sizes = (mesh.shape["grp"], mesh.shape["sp"], mesh.shape["tp"])
        fits = lanes == 2 * KEY_CHANNELS and sizes == (2, 4, 4)
        return fast_body(*args) if fits else body(*args)

    return jax.shard_map(run, mesh=mesh, in_specs=in_specs, out_specs=out_specs, check_vma=False)
```

```python
import functools

import jax
import jax.numpy as jnp
from jax import lax
from jax.experimental import pallas as pl
from jax.experimental.pallas import tpu as pltpu
from jax.sharding import PartitionSpec as P


KEY_CHANNELS = 64
HEAD_V = 128
BLOCK = 64
GATE_DENOMINATOR = 16.0
EPSILON = 1e-06
F32, BF16 = jnp.float32, jnp.bfloat16


def nt(a, b):
    return lax.dot_general(a, b, (((1,), (1,)), ((), ())), preferred_element_type=F32)


def tn(a, b):
    return lax.dot_general(a, b, (((0,), (0,)), ((), ())), preferred_element_type=F32)


def first_head(shape):
    return lax.broadcasted_iota(jnp.int32, shape, 1) < KEY_CHANNELS


VMEM = pl.BlockSpec(memory_space=pltpu.VMEM)


def cost(flops, size):
    return pl.CostEstimate(flops=flops, bytes_accessed=size, transcendentals=0)


def entering(value, axis, join, neutral, backward):
    count = lax.axis_size(axis)
    place = lax.axis_index(axis)
    ahead = count - 1 - place if backward else place
    gathered = jax.tree.map(
        lambda a, kind: lax.all_gather(a.astype(kind), axis), value, (jnp.bfloat16, jnp.bfloat16)
    )
    state = jax.tree.map(lambda a, e: jnp.zeros_like(a) + jnp.asarray(e, a.dtype), value, neutral)

    def one(lap, state):
        source = count - 1 - lap if backward else lap
        return join(
            state,
            jax.tree.map(
                lambda a, own: lax.dynamic_index_in_dim(a, source, 0, False).astype(own.dtype),
                gathered,
                value,
            ),
        )

    return lax.fori_loop(0, ahead, one, state)


def block_sweep(query_in, key_in, values_in, log_decay, span):
    sequence_length, head_count, key_dim = key_in.shape
    block_count = sequence_length // span

    def blocks(tensor):
        return jnp.transpose(
            tensor.reshape(block_count, span, head_count, tensor.shape[-1]), (0, 2, 1, 3)
        )

    lower_mask = jnp.tril(jnp.ones((span, span), dtype=bool))[:, :, None]

    def advance(carried, inputs):
        memory, offset = carried
        key_blk, value_blk, decay_blk, query_blk = inputs
        within = jnp.cumsum(decay_blk, axis=1)
        ending = within[:, -1, :]
        memory_next = jnp.exp(ending)[:, :, None] * memory + jnp.einsum(
            "hjd,hje->hde",
            key_blk * jnp.exp(ending[:, None, :] - within),
            value_blk,
            precision=lax.Precision.HIGHEST,
        )
        result = jnp.einsum(
            "hid,hde->hie", query_blk * jnp.exp(within), memory, precision=lax.Precision.HIGHEST
        )
        spread = jnp.exp(
            jnp.where(lower_mask, within[:, :, None, :] - within[:, None, :, :], -jnp.inf)
        )
        scores = jnp.einsum(
            "hid,hjd,hijd->hij", query_blk, key_blk, spread, precision=lax.Precision.HIGHEST
        )
        result = result + jnp.einsum(
            "hij,hje->hie", scores, value_blk, precision=lax.Precision.HIGHEST
        )
        reached = query_blk * jnp.exp(within + offset[:, None, :])
        return ((memory_next, offset + ending), (result, reached))

    start_memory = jnp.zeros((head_count, key_dim, values_in.shape[-1]), jnp.float32)
    start_offset = jnp.zeros((head_count, key_dim), jnp.float32)
    (memory, decay_total), (outputs, reached) = lax.scan(
        advance,
        (start_memory, start_offset),
        (blocks(key_in), blocks(values_in), blocks(log_decay), blocks(query_in)),
    )

    def unblock(tensor):
        return jnp.transpose(tensor, (0, 2, 1, 3)).reshape(
            sequence_length, head_count, tensor.shape[-1]
        )

    return (unblock(outputs), unblock(reached), memory, decay_total)


def head_mix(combined, head_norm_gain, output_gate_preact):
    sequence_length, head_count, width = combined.shape
    inverse = lax.rsqrt(jnp.mean(combined * combined, axis=-1, keepdims=True) + EPSILON)
    gate_act = jax.nn.silu(
        output_gate_preact.astype(jnp.float32).reshape(sequence_length, head_count, width)
    )
    weighted = combined * inverse * head_norm_gain.reshape(head_count, width) * gate_act
    return weighted.reshape(sequence_length, head_count * width).astype(jnp.bfloat16)


def row_norm(mid_rows, prenorm_gain):
    wide = mid_rows.astype(jnp.float32)
    inverse = lax.rsqrt(jnp.mean(wide * wide, axis=-1, keepdims=True) + EPSILON)
    return (wide * inverse * prenorm_gain).astype(jnp.bfloat16)


def combine_states(earlier, later):
    decay_early, memory_early = earlier
    decay_late, memory_late = later
    return (decay_early * decay_late, decay_late[:, :, None] * memory_early + memory_late)


def body(
    queries,
    key_projected,
    values,
    output_gate_preact,
    forward_decay_logits,
    backward_decay_logits,
    decay_logit_shift,
    decay_spike_values,
    residual,
    head_norm_gain,
    output_projection,
    prenorm_gain,
    gate_projection,
    up_projection,
    down_projection,
):
    sequence_length = queries.shape[0]
    local_heads = queries.shape[1] // KEY_CHANNELS
    query_f = queries.astype(jnp.float32).reshape(
        sequence_length, local_heads, KEY_CHANNELS
    ) * KEY_CHANNELS ** (-0.5)
    keys_f = key_projected.astype(jnp.float32).reshape(sequence_length, local_heads, KEY_CHANNELS)
    values_f = values.astype(jnp.float32).reshape(sequence_length, local_heads, HEAD_V)
    decay_spikes = jnp.transpose(decay_spike_values)[:, :, None]
    logit_shifts = decay_logit_shift.reshape(2, local_heads, KEY_CHANNELS)
    forward_decay = (
        jax.nn.log_sigmoid(
            forward_decay_logits.astype(jnp.float32).reshape(
                sequence_length, local_heads, KEY_CHANNELS
            )
            + logit_shifts[0]
        )
        / GATE_DENOMINATOR
        + decay_spikes
    )
    backward_decay = (
        jax.nn.log_sigmoid(
            backward_decay_logits.astype(jnp.float32).reshape(
                sequence_length, local_heads, KEY_CHANNELS
            )
            + logit_shifts[1]
        )
        / GATE_DENOMINATOR
        + decay_spikes
    )
    fwd_out, fwd_reach, fwd_memory, fwd_total = block_sweep(
        query_f, keys_f, values_f, forward_decay, BLOCK
    )
    bwd_out, bwd_reach, bwd_memory, bwd_total = block_sweep(
        query_f[::-1], keys_f[::-1], values_f[::-1], backward_decay[::-1], BLOCK
    )
    identity = (jnp.ones_like(fwd_total), jnp.zeros_like(fwd_memory))
    fwd_incoming = entering(
        (jnp.exp(fwd_total), fwd_memory), "sp", combine_states, identity, False
    )[1]
    bwd_incoming = entering((jnp.exp(bwd_total), bwd_memory), "sp", combine_states, identity, True)[
        1
    ]
    fwd_full = fwd_out + jnp.einsum(
        "lhd,hde->lhe", fwd_reach, fwd_incoming, precision=lax.Precision.HIGHEST
    )
    bwd_full = bwd_out + jnp.einsum(
        "lhd,hde->lhe", bwd_reach, bwd_incoming, precision=lax.Precision.HIGHEST
    )
    attended = head_mix(fwd_full + bwd_full[::-1], head_norm_gain, output_gate_preact)
    token_rows = lax.all_to_all(attended, "tp", split_axis=0, concat_axis=1, tiled=True)
    whole_out = lax.all_gather(output_projection, "tp", axis=0, tiled=True)
    projected = jnp.dot(token_rows, whole_out, preferred_element_type=jnp.float32)
    mid_rows = (residual.astype(jnp.float32) + projected).astype(jnp.bfloat16)
    normed = row_norm(mid_rows, prenorm_gain)
    fetched = (
        lax.all_gather(gate_projection, "sp", axis=0, tiled=True),
        lax.all_gather(up_projection, "sp", axis=0, tiled=True),
        lax.all_gather(down_projection, "sp", axis=1, tiled=True),
    )
    gate_full, up_full, down_full = fetched
    piece = lax.all_gather(normed, "tp", axis=0, tiled=True)
    gate_part = jnp.dot(piece, gate_full, preferred_element_type=jnp.float32)
    up_part = jnp.dot(piece, up_full, preferred_element_type=jnp.float32)
    hidden = (jax.nn.silu(gate_part) * up_part).astype(jnp.bfloat16)
    summed = lax.psum_scatter(
        jnp.dot(hidden, down_full, preferred_element_type=jnp.float32).astype(jnp.bfloat16),
        "tp",
        scatter_dimension=0,
        tiled=True,
    ).astype(jnp.float32)
    return (mid_rows.astype(jnp.float32) + 0.5 * summed).astype(jnp.bfloat16)


MESH = pl.DeviceIdType.MESH
PIECES = 5


def log_decay(logits, shift, spike):
    x = logits.astype(F32) + shift
    soft = jnp.minimum(x, 0.0) - jnp.log1p(jnp.exp(-jnp.abs(x)))
    return soft / GATE_DENOMINATOR + spike


def own_states(k_ref, v_ref, fd_ref, bd_ref, shift_ref, spike_ref, within_ref, kd_ref, fwd_ref, bwd_ref):
    tokens, lanes = k_ref.shape
    blocks = tokens // BLOCK
    row = lax.broadcasted_iota(jnp.int32, (2 * BLOCK, 2 * BLOCK), 0)
    col = lax.broadcasted_iota(jnp.int32, (2 * BLOCK, 2 * BLOCK), 1)
    r, c = row % BLOCK, col % BLOCK
    ahead = jnp.where(row < BLOCK, r - c, c - r)
    tri = jnp.where(ahead >= 0, 1.0, 0.0).astype(BF16)
    half = first_head((BLOCK, lanes))
    spikes = jnp.transpose(jnp.concatenate([spike_ref[...]] * 4, axis=0))
    ends = []
    for b in range(blocks):
        at = slice(b * BLOCK, (b + 1) * BLOCK)
        spike = jnp.where(half, spikes[at, 0:1], spikes[at, 1:2])
        parts = [log_decay(ref[at, :], shift_ref[n : n + 1, :], spike) for n, ref in enumerate((fd_ref, bd_ref))]
        d = jnp.concatenate(parts, axis=1)
        hi = d.astype(BF16)
        lo = (d - hi.astype(F32)).astype(BF16)
        both = jnp.dot(tri, jnp.concatenate([hi, lo], axis=0), preferred_element_type=F32)
        fwd, bwd = both[:BLOCK, :lanes], both[BLOCK:, lanes:]
        within_ref[at, :lanes] = fwd
        within_ref[at, lanes:] = bwd
        ends.append((fwd[BLOCK - 1 :, :], bwd[:1, :]))
    zero = jnp.zeros((1, lanes), F32)
    after, before = [zero] * blocks, [zero] * blocks
    for b in range(1, blocks):
        before[b] = before[b - 1] + ends[b - 1][1]
        after[blocks - 1 - b] = after[blocks - b] + ends[blocks - b][0]
    totals = after[0] + ends[0][0], before[-1] + ends[-1][1]
    for b in range(blocks):
        at = slice(b * BLOCK, (b + 1) * BLOCK)
        key = k_ref[at, :].astype(F32)
        kd_ref[at, :lanes] = (key * jnp.exp((ends[b][0] + after[b]) - within_ref[at, :lanes])).astype(BF16)
        kd_ref[at, lanes:] = (key * jnp.exp((ends[b][1] + before[b]) - within_ref[at, lanes:])).astype(BF16)
    full = tn(v_ref[...], kd_ref[...])
    mine = first_head((HEAD_V, lanes))
    for n, ref in enumerate((fwd_ref, bwd_ref)):
        u = full[:, n * lanes : (n + 1) * lanes]
        ref[:HEAD_V, :] = jnp.where(mine, u[:HEAD_V], u[HEAD_V:]).astype(BF16)
        ref[HEAD_V:, :] = jnp.broadcast_to(jnp.exp(totals[n]), (16, lanes)).astype(BF16)


def spread(state):
    mine = first_head(state.shape)
    return jnp.concatenate([jnp.where(mine, state, 0.0), jnp.where(mine, 0.0, state)], axis=0).astype(BF16)


def pack(u):
    top = u[:HEAD_V]
    return jnp.where(first_head(top.shape), top, u[HEAD_V:])


def backward_states(k_ref, v_ref, within_ref, state, held_ref):
    tokens, lanes = k_ref.shape
    for b in reversed(range(tokens // BLOCK)):
        at = slice(b * BLOCK, (b + 1) * BLOCK)
        held_ref[b] = spread(state)
        within = within_ref[at, lanes:]
        end = within[:1, :]
        kd = (k_ref[at, :].astype(F32) * jnp.exp(end - within)).astype(BF16)
        state = state * jnp.exp(end) + pack(tn(v_ref[at, :], kd))


def attend(q_ref, k_ref, v_ref, within_ref, gate_ref, gain_ref, fwd_state, held_ref, out_ref):
    tokens, lanes = k_ref.shape
    row = lax.broadcasted_iota(jnp.int32, (2 * BLOCK, BLOCK), 0) % BLOCK
    col = lax.broadcasted_iota(jnp.int32, (2 * BLOCK, BLOCK), 1)
    half = first_head((BLOCK, lanes))
    for b in range(tokens // BLOCK):
        at = slice(b * BLOCK, (b + 1) * BLOCK)
        query = q_ref[at, :].astype(F32) * KEY_CHANNELS ** (-0.5)
        key = k_ref[at, :].astype(F32)
        value = v_ref[at, :]
        scores, reach = [], []
        for n in range(2):
            within = within_ref[at, n * lanes : (n + 1) * lanes]
            pivot = within[BLOCK // 2 - 1 + n : BLOCK // 2 + n, :]
            near = (query * jnp.exp(within - pivot)).astype(BF16)
            far = (key * jnp.exp(pivot - within)).astype(BF16)
            zero = jnp.zeros_like(near)
            pair = jnp.concatenate([jnp.where(half, near, zero), jnp.where(half, zero, near)], axis=0)
            scores.append(nt(pair, far))
            reach.append((query * jnp.exp(within)).astype(BF16))
        score = (jnp.where(col <= row, scores[0], 0.0) + jnp.where(col >= row, scores[1], 0.0)).astype(BF16)
        states = jnp.concatenate([spread(fwd_state), held_ref[b]], axis=1)
        result = nt(jnp.concatenate(reach, axis=1), states)
        for h in range(2):
            lane = slice(h * HEAD_V, (h + 1) * HEAD_V)
            x = result[:, lane] + jnp.dot(
                score[h * BLOCK : (h + 1) * BLOCK], value[:, lane], preferred_element_type=F32
            )
            inverse = lax.rsqrt(jnp.mean(x * x, axis=-1, keepdims=True) + EPSILON)
            g = gate_ref[at, lane].astype(F32)
            out_ref[at, lane] = (x * inverse * gain_ref[:, lane] * (g * jax.nn.sigmoid(g))).astype(BF16)
        within = within_ref[at, :lanes]
        end = within[BLOCK - 1 :, :]
        kd = (key * jnp.exp(end - within)).astype(BF16)
        fwd_state = fwd_state * jnp.exp(end) + pack(tn(value, kd))


def pick(i, table):
    value = table[0]
    for n, item in enumerate(table[1:], 1):
        value = jnp.where(i == n, item, value)
    return value


def ds(first, size):
    return pl.ds(pl.multiple_of(first, size if size % 128 == 0 else 16), size)


def layer_kernel(
    k_hbm, v_hbm, fd_hbm, bd_hbm, shift_hbm, spike_hbm, q_hbm, gate_hbm, gain_hbm, norm_hbm,
    res_hbm, out_hbm, g_hbm, u_hbm, d_hbm,
    out_ref,
    k_ref, v_ref, fd_ref, bd_ref, shift_ref, spike_ref, q_ref, gate_ref, gain_ref, norm_ref, in_s,
    within, kd, fown, bown, fgot, bgot, fstate, bstate, held, attended, rows, outl, outh, pout, rgot, rxs, rxg, squares, res, mid, acts,
    wgu, wd, hid, part, got, xsend, xgot, esend, egot, erelay,
    loc, st_s, st_r, a2a_s, a2a_r, ow_s, ow_r, rs_s, rs_r, rx_s, rx_r, ag_s, ag_r, ea_s, ea_r, gs, gr, dsd, drv, cr_s, cr_r, xo_s, xo_r,
    eo_s, eo_r, er_s, er_r,
):
    count = lax.axis_size("sp")
    side, place, me = lax.axis_index("grp"), lax.axis_index("sp"), lax.axis_index("tp")
    chip, core = me // 2, me % 2
    tc, tx, td = 2 * chip + 1 - core, 2 * (1 - chip) + core, 2 * (1 - chip) + 1 - core
    upper = place // 2
    e, m, o, oe = 3 * upper, 1 + upper, 2 - upper, 3 - 3 * upper
    middle = place * (count - 1 - place) > 0
    outer = jnp.logical_not(middle)
    own = res.shape[0]
    width = attended.shape[1]
    model = mid.shape[1]
    depth, hidden = g_hbm.shape
    tile = hidden // PIECES
    hr = depth // 2
    dr = hidden // 2
    dw = wd.shape[3]
    chunks = part.shape[1]
    wide = pout.shape[2]
    parts = pout.shape[0]
    nrow = own // 2

    def remote(src, dst, send, recv, **dev):
        return pltpu.make_async_remote_copy(
            src_ref=src, dst_ref=dst, send_sem=send, recv_sem=recv, device_id=dev, device_id_type=MESH
        )

    def gu(n, source, half, p, local=False, again=False, **dev):
        dst = wgu.at[n, p, ds(source * depth + half * hr, hr), :]
        src = (g_hbm, u_hbm)[n].at[ds(half * hr, hr), ds(p * tile, tile)] if local else dst
        send = gs.at[source, 1 - half if again else half]
        return remote(src, dst, send, gr.at[n, source, half, p], **(dev or dict(sp=o)))

    def dn(source, half, p, r, local=False, again=False, **dev):
        dst = wd.at[source, p, ds(half * dr + r * (dr // 2), dr // 2), :]
        src = d_hbm.at[ds(half * dr + r * (dr // 2), dr // 2), p * dw : (p + 1) * dw] if local else dst
        send = dsd.at[source, 1 - half if again else half]
        return remote(src, dst, send, drv.at[source, half, p, r], **(dev or dict(sp=o)))

    def send_gu(source, half, p, local=False, again=False, **dev):
        for n in range(2):
            gu(n, source, half, p, local, again, **dev).start()

    def take_gu(source, half, p):
        for n in range(2):
            gu(n, source, half, p).wait_recv()

    def relay_gu(source, p, **dev):
        for n in range(2):
            gu(n, source, side, p).wait_recv()
            gu(n, source, side, p, **dev).start()

    def send_dn(half, p, **dev):
        for r in range(2):
            dn(place, half, p, r, True, **dev).start()

    def take_dn(source, half, p):
        for r in range(2):
            dn(source, half, p, r).wait_recv()

    def relay_dn(source, p, r, **dev):
        dn(source, side, p, r).wait_recv()
        dn(source, side, p, r, **dev).start()

    def sent(ref, sem):
        remote(ref, ref, sem, sem, sp=o).wait_send()

    def sent_gu(source, half, low, high, again=False):
        at = ds(source * depth + half * hr, hr)
        sent(wgu.at[:, low:high, at, :], gs.at[source, 1 - half if again else half])

    def sent_dn(source, half, low, high):
        sent(wd.at[source, low:high, ds(half * dr, dr), :], dsd.at[source, half])

    def landed(ref, sem):
        remote(ref, ref, sem, sem, sp=o).wait_recv()

    def ow(kind, block, i, dev, local=False):
        half = width // 2
        dst = outh.at[ds(block * width + i * half, half), :]
        src = out_hbm.at[i * half : (i + 1) * half, model // 2 :] if local else dst
        return remote(src, dst, ow_s.at[kind], ow_r.at[i if kind == 0 else 1 + kind], tp=dev)

    def relay_ow(i):
        ow(0, tx, i, tc).wait_recv()
        ow(2, tx, i, tc).start()

    def a2a(block, dev):
        src = attended.at[ds(dev * own, own), :]
        return remote(src, rows.at[:, ds(block * width, width)], a2a_s.at[0], a2a_r.at[block], tp=dev)

    def rs(c, j):
        block = 2 * j + 1 - core
        return remote(pout.at[c, ds(block * own, own), :], rgot.at[c, j], rs_s.at[0], rs_r.at[c], tp=tc)

    def rx(c):
        return remote(rxs.at[c], rxg.at[c], rx_s.at[0], rx_r.at[c], tp=tx)

    def ag(q, kind, block, i, dev):
        at = acts.at[q, ds(block * own + i * nrow, nrow), :]
        return remote(at, at, ag_s.at[q, kind], ag_r.at[q, i if kind == 0 else 1 + kind], tp=dev)

    def to_host(i):
        at = ds(me * own + i * nrow, nrow)
        return remote(acts.at[0, at, :], acts.at[1, at, :], ea_s.at[0], ea_r.at[i], sp=m)

    def gathered(q):
        for kind, block in ((1, tc), (2, td)):
            landed(acts.at[q, ds(block * own, own), :], ag_r.at[q, 1 + kind])

    def state_copy(n, k, dev):
        src, dst = ((fown, fgot), (bown, bgot))[n]
        return remote(src, dst.at[k - 1], st_s.at[n, k - 1], st_r.at[n, k - 1], sp=dev)

    def cr(q, i, j):
        block = 2 * j + 1 - core
        return remote(part.at[q, i, ds(block * own, own), :], got.at[q, i, j], cr_s.at[q], cr_r.at[q, i], tp=tc)

    def xo(q, i):
        return remote(xsend.at[q, i], xgot.at[q, i], xo_s.at[q], xo_r.at[q, i], tp=tx)

    def eo(i, n):
        dst = egot.at[0, i] if n == 0 else erelay.at[i]
        return remote(esend.at[i, n], dst, eo_s.at[n], eo_r.at[i, n], sp=e)

    def er(i):
        return remote(erelay.at[i], egot.at[1, i], er_s.at[0], er_r.at[i], tp=tx)

    own_copies = []
    for p in range(PIECES):
        for n in range(2):
            own_copies.append(
                pltpu.make_async_copy(
                    (g_hbm, u_hbm)[n].at[:, p * tile : (p + 1) * tile],
                    wgu.at[n, p, ds(place * depth, depth), :],
                    loc.at[0],
                )
            )
    for p in range(2):
        own_copies.append(pltpu.make_async_copy(d_hbm.at[:, p * dw : (p + 1) * dw], wd.at[place, p], loc.at[1]))
    own_gu = wgu.at[:, :, ds(place * depth, depth), :]
    own_waits = [
        pltpu.make_async_copy(own_gu, own_gu, loc.at[0]),
        pltpu.make_async_copy(wd.at[place], wd.at[place], loc.at[1]),
    ]
    own_low = pltpu.make_async_copy(out_hbm.at[:, : model // 2], outl, loc.at[2])
    own_high = pltpu.make_async_copy(out_hbm.at[:, model // 2 :], outh.at[ds(me * width, width), :], loc.at[4])
    own_res = pltpu.make_async_copy(res_hbm, res, loc.at[3])

    barrier = pltpu.get_barrier_semaphore()
    friends = [dict(sp=lax.rem(place + k, count)) for k in range(1, count)]
    friends += [dict(grp=1 - side)] + [dict(tp=t) for t in (tc, tx, td)]
    for friend in friends:
        pl.semaphore_signal(barrier, inc=1, device_id=friend, device_id_type=MESH)
    loads = [
        pltpu.make_async_copy(src, dst, in_s.at[n])
        for n, (src, dst) in enumerate(
            (
                (k_hbm, k_ref),
                (v_hbm, v_ref),
                (fd_hbm, fd_ref),
                (bd_hbm, bd_ref),
                (shift_hbm, shift_ref),
                (spike_hbm, spike_ref),
                (q_hbm, q_ref),
                (gate_hbm, gate_ref),
                (gain_hbm, gain_ref),
                (norm_hbm, norm_ref),
            )
        )
    ]
    for load in loads:
        load.start()
    own_low.start()
    own_high.start()
    own_res.start()
    for load in loads[:6]:
        load.wait()
    own_states(k_ref, v_ref, fd_ref, bd_ref, shift_ref, spike_ref, within, kd, fown, bown)
    pl.semaphore_wait(barrier, len(friends))

    for k in range(1, count):

        @pl.when(place + k < count)
        def _(k=k):
            state_copy(0, k, place + k).start()

        @pl.when(place >= k)
        def _(k=k):
            state_copy(1, k, place - k).start()

    @pl.when(middle)
    def _():
        for p in range(PIECES):
            send_gu(place, side, p, True, sp=o)

    @pl.when(outer)
    def _():
        for p in range(PIECES):
            send_gu(place, side, p, True, sp=m)

    for i in range(2):
        ow(0, me, i, tx, True).start()
        ow(1, me, i, tc, True).start()

    @pl.when(middle)
    def _():
        for copy in own_copies:
            copy.start()

    for load in loads[6:]:
        load.wait()
    fstate[...] = jnp.zeros_like(fstate)
    bstate[...] = jnp.zeros_like(bstate)
    for k in reversed(range(1, count)):

        @pl.when(place >= k)
        def _(k=k):
            state_copy(0, k, place).wait_recv()
            decay = fgot[k - 1, HEAD_V : HEAD_V + 1, :].astype(F32)
            fstate[...] = fstate[...] * decay + fgot[k - 1, :HEAD_V, :].astype(F32)

        @pl.when(place + k < count)
        def _(k=k):
            state_copy(1, k, place).wait_recv()
            decay = bgot[k - 1, HEAD_V : HEAD_V + 1, :].astype(F32)
            bstate[...] = bstate[...] * decay + bgot[k - 1, :HEAD_V, :].astype(F32)

    backward_states(k_ref, v_ref, within, bstate[...], held)
    attend(q_ref, k_ref, v_ref, within, gate_ref, gain_ref, fstate[...], held, attended)
    others = (tx, td, tc)
    for t in others:
        a2a(me, t).start()
    rows[:, ds(me * width, width)] = attended[ds(me * own, own), :]
    own_low.wait()
    for c in range(parts):
        at = slice(c * wide, (c + 1) * wide)
        pout[c] = jnp.dot(attended[...], outl[:, at], preferred_element_type=F32).astype(BF16)
        for j in range(2):
            rs(c, j).start()
    relay_ow(0)
    for c in range(parts):
        landed(rgot.at[c], rs_r.at[c])
        rxs[c] = (pout[c, ds(tx * own, own), :].astype(F32) + rgot[c, 1 - chip].astype(F32)).astype(BF16)
        rx(c).start()

    def mix(at, projected):
        mixed = (res[:, at].astype(F32) + projected).astype(BF16)
        mid[:, at] = mixed
        mixed = mixed.astype(F32)
        return jnp.sum(mixed * mixed, axis=-1, keepdims=True)

    @pl.when(middle)
    def _():
        relay_gu(o, 0, grp=1 - side)
        relay_gu(e, 0, sp=o)

    relay_ow(1)

    @pl.when(middle)
    def _():
        relay_gu(o, 1, grp=1 - side)
        relay_gu(e, 1, sp=o)

    for t in others:
        a2a(t, t).wait_recv()
    for kind, t in ((1, tc), (2, td)):
        landed(outh.at[ds(t * width, width), :], ow_r.at[1 + kind])
    own_high.wait()
    own_res.wait()
    total = jnp.zeros((own, 1), F32)
    for n in range(parts):
        high = slice(n * wide, (n + 1) * wide)
        projected = jnp.dot(rows[...], outh[:, high], preferred_element_type=F32)
        total += mix(slice(model // 2 + n * wide, model // 2 + (n + 1) * wide), projected)
    squares[...] = jnp.broadcast_to(total, squares.shape)

    @pl.when(middle)
    def _():
        relay_gu(o, 2, grp=1 - side)
        relay_gu(e, 2, sp=o)

    total = squares[:, :1]
    for n in range(parts):
        rx(n).wait_recv()
        projected = pout[n, ds(me * own, own), :].astype(F32) + rgot[n, chip].astype(F32) + rxg[n].astype(F32)
        total += mix(slice(n * wide, (n + 1) * wide), projected)
    inverse = lax.rsqrt(total / model + EPSILON)
    for n in range(2 * parts):
        at = slice(n * wide, (n + 1) * wide)
        acts[0, ds(me * own, own), at] = (mid[:, at].astype(F32) * inverse * norm_ref[:, at]).astype(BF16)

    direct = (1, 1, 1, 0, 0, 0, 0, 1)
    whole = [i for i, d in enumerate(direct) if d]

    def straight(i):
        return direct[i] if isinstance(i, int) else pick(i, direct)

    sources = (m, m, o, o, e, oe, e, oe)
    sides = (0, 1, 0, 1, 0, 0, 1, 1)

    @pl.when(middle)
    def _():
        for i in range(2):
            ag(0, 0, me, i, tx).start()
            ag(0, 1, me, i, tc).start()
        for p in range(3, PIECES):
            relay_gu(o, p, grp=1 - side)
            relay_gu(e, p, sp=o)
        send_gu(e, side, 1, again=True, grp=1 - side)
        for p in range(2):
            send_dn(side, p, sp=o)
        send_dn(1 - side, 1, sp=o)
        for copy in own_waits:
            copy.wait()

        def relay_own(i):
            ag(0, 0, tx, i, tc).wait_recv()
            ag(0, 2, tx, i, tc).start()

        def relay_hosted(i):
            to_host(i).wait_recv()
            ag(1, 0, me, i, tx).start()
            ag(1, 1, me, i, tc).start()

        def pass_hosted(i):
            ag(1, 0, tx, i, tc).wait_recv()
            ag(1, 2, tx, i, tc).start()

        relay_gu(oe, 0, grp=1 - side)
        relay_own(0)
        relay_hosted(0)
        relay_gu(oe, 1, grp=1 - side)
        relay_own(1)
        relay_gu(oe, 2, grp=1 - side)
        relay_hosted(1)

        order = [(0, 0), (0, 1), (0, 2), (1, 0), (1, 1), (0, 3), (1, 2), (1, 3), (0, 4), (1, 4)]

        def fold(i, q):
            landed(got.at[q, i], cr_r.at[q, i])

            def both(block, j):
                return part[q, i, ds(block * own, own), :].astype(F32) + got[q, i, j].astype(F32)

            @pl.when(jnp.logical_or(q == 0, straight(i) == 0))
            def _():
                xsend[q, i] = both(tx, 1 - chip).astype(BF16)
                xo(q, i).start()

            @pl.when(jnp.logical_and(q == 1, straight(i) == 1))
            def _():
                esend[i, 1] = both(tx, 1 - chip).astype(BF16)
                eo(i, 1).start()
                esend[i, 0] = both(me, chip).astype(BF16)
                eo(i, 0).start()

        def push(i):
            if direct[i]:
                return
            xo(1, i).wait_recv()
            mixed = part[1, i, ds(me * own, own), :].astype(F32) + got[1, i, chip].astype(F32)
            esend[i, 0] = (mixed + xgot[1, i].astype(F32)).astype(BF16)
            eo(i, 0).start()

        def product(q, i):
            weight = wd[pick(i, sources), pick(i, sides)]
            part[q, i] = jnp.dot(hid[q], weight, preferred_element_type=F32).astype(BF16)
            for j in range(2):
                cr(q, i, j).start()

        def first(i, carry):
            q, j = pick(i, [a for a, _ in order]), pick(i, [b for _, b in order])

            @pl.when(i == 0)
            def _():
                gathered(0)

            @pl.when(i == 1)
            def _():
                pass_hosted(0)
                relay_gu(oe, 3, grp=1 - side)

            @pl.when(i == 2)
            def _():
                relay_gu(oe, 4, grp=1 - side)
                pass_hosted(1)

            @pl.when(i == 3)
            def _():
                gathered(1)

            @pl.when(i == 5)
            def _():
                for r in range(2):
                    relay_dn(o, 0, r, grp=1 - side)

            @pl.when(i == 9)
            def _():
                relay_dn(e, 0, 0, sp=o)

            @pl.when(q == 0)
            def _():
                for source in (o, oe, e):
                    take_gu(source, 1 - side, j)

            g = jnp.dot(acts[q], wgu[0, j], preferred_element_type=F32)
            u = jnp.dot(acts[q], wgu[1, j], preferred_element_type=F32)
            hid[q, :, ds(j * tile, tile)] = (g * jax.nn.sigmoid(g) * u).astype(BF16)
            return carry

        lax.fori_loop(0, len(order), first, 0)

        def second(s, carry):
            i, q = s // 2, 1 - s % 2

            @pl.when(s == 0)
            def _():
                relay_dn(e, 0, 1, sp=o)
                dn(e, side, 0, 1, again=True, grp=1 - side).start()

            @pl.when(s == 4)
            def _():
                take_dn(o, 1 - side, 0)

            @pl.when(s == 5)
            def _():
                relay_dn(e, 1, 0, sp=o)

            @pl.when(s == 6)
            def _():
                take_dn(o, side, 1)
                take_dn(o, 1 - side, 1)

            @pl.when(s == 8)
            def _():
                relay_dn(oe, 0, 0, grp=1 - side)
                fold(3, 1)
                relay_dn(e, 1, 1, sp=o)
                fold(3, 0)
                relay_dn(oe, 0, 1, grp=1 - side)
                push(2)
                take_dn(e, 1 - side, 0)

            @pl.when(s == 10)
            def _():
                fold(4, 1)
                fold(4, 0)
                push(3)
                relay_dn(oe, 1, 0, grp=1 - side)
                take_dn(oe, 1 - side, 0)

            @pl.when(s == 12)
            def _():
                fold(5, 1)
                relay_dn(oe, 1, 1, grp=1 - side)
                fold(5, 0)
                push(4)
                take_dn(e, 1 - side, 1)

            @pl.when(s == 14)
            def _():
                fold(6, 1)
                fold(6, 0)
                push(5)
                take_dn(oe, 1 - side, 1)

            product(q, i)

            @pl.when((s > 1) & (s < 8))
            def _():
                fold(i - 1, q)

            return carry

        lax.fori_loop(0, 2 * chunks, second, 0)
        fold(chunks - 1, 1)
        fold(chunks - 1, 0)
        push(chunks - 2)

        for i in range(chunks):
            xo(0, i).wait_recv()
            at = ds((2 * sources[i] + sides[i]) * dw, dw)
            total = part[0, i, ds(me * own, own), :].astype(F32) + got[0, i, chip].astype(F32) + xgot[0, i].astype(F32)
            out_ref[:, at] = (mid[:, at].astype(F32) + 0.5 * total).astype(BF16)

        for source in (place, e, o, oe):
            sent_gu(source, side, 0, PIECES)
        sent_gu(e, side, 0, 1, again=True)
        sent(wd.at[e, 0, : dr // 2, :], dsd.at[e, 1 - side])
        for source in (place, e, oe):
            sent_dn(source, side, 0, 2)
        sent_dn(o, side, 0, 1)
        sent_dn(place, 1 - side, 1, 2)
        for q in range(2):
            for kind in range(3):
                sent(acts.at[q, ds(me * own, own), :], ag_s.at[q, kind])
            sent(got.at[q], cr_s.at[q])
        sent(xsend.at[0], xo_s.at[0])
        sent(xsend.at[1, : chunks - len(whole)], xo_s.at[1])
        sent(esend.at[:, 0], eo_s.at[0])
        sent(esend.at[: len(whole), 1], eo_s.at[1])

    @pl.when(outer)
    def _():
        for i in range(2):
            to_host(i).start()
        for p in (0, 2, 3, 4):
            send_gu(place, 1 - side, p, True, sp=m)
        for p in range(2):
            send_dn(side, p, sp=m)
        dn(place, 1 - side, 0, 0, True, sp=m).start()
        send_dn(1 - side, 1, sp=m)

        def finish(i):
            eo(i, 0).wait_recv()
            total = egot[0, i].astype(F32)
            if direct[i]:
                er(i).wait_recv()
                total += egot[1, i].astype(F32)
            at = ds((2 * sources[i] + sides[i]) * dw, dw)
            out_ref[:, at] = (mid[:, at].astype(F32) + 0.5 * total).astype(BF16)

        for i in range(chunks):
            if direct[i]:
                eo(i, 1).wait_recv()
                er(i).start()
            if i > 1:
                finish(i - 2)
        finish(chunks - 2)
        finish(chunks - 1)
        sent(acts.at[0, ds(me * own, own), :], ea_s.at[0])
        sent_gu(place, side, 0, PIECES)
        sent_gu(place, 1 - side, 0, PIECES - 1)
        sent_dn(place, side, 0, 2)
        sent(wd.at[place, 0, : dr + dr // 2, :], dsd.at[place, 1 - side])
        sent(erelay.at[: len(whole)], er_s.at[0])

    for k in range(1, count):

        @pl.when(place + k < count)
        def _(k=k):
            state_copy(0, k, place).wait_send()

        @pl.when(place >= k)
        def _(k=k):
            state_copy(1, k, place).wait_send()

    sent(rows.at[:, : 3 * width], a2a_s.at[0])
    for kind in range(3):
        sent(outh.at[ds(me * width, width), :], ow_s.at[kind])
    sent(rgot, rs_s.at[0])
    sent(rxs, rx_s.at[0])


def fast_body(
    queries,
    key_projected,
    values,
    output_gate_preact,
    forward_decay_logits,
    backward_decay_logits,
    decay_logit_shift,
    decay_spike_values,
    residual,
    head_norm_gain,
    output_projection,
    prenorm_gain,
    gate_projection,
    up_projection,
    down_projection,
):
    count = lax.axis_size("sp")
    tokens, lanes = queries.shape
    width = values.shape[1]
    own, model = residual.shape
    depth, hidden = gate_projection.shape
    dw = down_projection.shape[1] // 2
    chunks = 2 * count
    blocks = tokens // BLOCK
    dma = lambda *shape: pltpu.SemaphoreType.DMA(shape)
    state = (HEAD_V + 16, lanes)
    V = pltpu.VMEM
    scratch = [
        V((tokens, lanes), BF16),
        V((tokens, width), BF16),
        V((tokens, lanes), BF16),
        V((tokens, lanes), BF16),
        V(decay_logit_shift.shape, F32),
        V(decay_spike_values.shape, F32),
        V((tokens, lanes), BF16),
        V((tokens, width), BF16),
        V((1, width), F32),
        V((1, model), F32),
        dma(10),
        V((tokens, 2 * lanes), F32),
        V((tokens, 2 * lanes), BF16),
        V(state, BF16),
        V(state, BF16),
        V((count - 1,) + state, BF16),
        V((count - 1,) + state, BF16),
        V((HEAD_V, lanes), F32),
        V((HEAD_V, lanes), F32),
        V((blocks, 2 * HEAD_V, lanes), BF16),
        V((tokens, width), BF16),
        V((own, tokens // own * width), BF16),
        V((width, model // 2), BF16),
        V((tokens // own * width, model // 2), BF16),
        V((2, tokens, model // 4), BF16),
        V((2, 2, own, model // 4), BF16),
        V((2, own, model // 4), BF16),
        V((2, own, model // 4), BF16),
        V((own, 128), F32),
        V((own, model), BF16),
        V((own, model), BF16),
        V((2, tokens, model), BF16),
        V((2, PIECES, model, hidden // PIECES), BF16),
        V((count, 2, hidden, dw), BF16),
        V((2, tokens, hidden), BF16),
        V((2, chunks, tokens, dw), BF16),
        V((2, chunks, 2, own, dw), BF16),
        V((2, chunks, own, dw), BF16),
        V((2, chunks, own, dw), BF16),
        V((chunks, 2, own, dw), BF16),
        V((2, chunks, own, dw), BF16),
        V((chunks, own, dw), BF16),
        dma(5),
        dma(2, count - 1),
        dma(2, count - 1),
        dma(1),
        dma(tokens // own),
        dma(3),
        dma(4),
        dma(1),
        dma(2),
        dma(1),
        dma(2),
        dma(2, 3),
        dma(2, 4),
        dma(1),
        dma(2),
        dma(count, 2),
        dma(2, count, 2, PIECES),
        dma(count, 2),
        dma(count, 2, 2, 2),
        dma(2),
        dma(2, chunks),
        dma(2),
        dma(2, chunks),
        dma(2),
        dma(chunks, 2),
        dma(1),
        dma(chunks),
    ]
    anywhere = pl.BlockSpec(memory_space=pl.ANY)
    return pl.pallas_call(
        layer_kernel,
        out_shape=pltpu.MemorySpace.VMEM((own, model), BF16),
        in_specs=[anywhere] * 15,
        out_specs=VMEM,
        scratch_shapes=scratch,
        compiler_params=pltpu.CompilerParams(
            collective_id=0, has_side_effects=True, vmem_limit_bytes=61000000
        ),
        cost_estimate=cost(3 * 10**10, 3 * 10**7),
        name="layer",
    )(
        key_projected,
        values,
        forward_decay_logits,
        backward_decay_logits,
        decay_logit_shift,
        decay_spike_values,
        queries,
        output_gate_preact,
        head_norm_gain[None, :],
        prenorm_gain[None, :],
        residual,
        output_projection,
        gate_projection,
        up_projection,
        down_projection,
    )


def solution(mesh):
    in_specs = (
        P(("grp", "sp"), "tp"),
        P(("grp", "sp"), "tp"),
        P(("grp", "sp"), "tp"),
        P(("grp", "sp"), "tp"),
        P(("grp", "sp"), "tp"),
        P(("grp", "sp"), "tp"),
        P(None, "tp"),
        P("tp", ("grp", "sp")),
        P(("grp", "sp", "tp"), None),
        P("tp"),
        P("tp", None),
        P(),
        P("sp", "tp"),
        P("sp", "tp"),
        P("tp", "sp"),
    )
    out_specs = P(("grp", "sp", "tp"), None)

    def run(*args):
        lanes = args[0].shape[1]
        sizes = (mesh.shape["grp"], mesh.shape["sp"], mesh.shape["tp"])
        fits = lanes == 2 * KEY_CHANNELS and sizes == (2, 4, 4)
        return fast_body(*args) if fits else body(*args)

    return jax.shard_map(run, mesh=mesh, in_specs=in_specs, out_specs=out_specs, check_vma=False)
```

```python
import functools

import jax
import jax.numpy as jnp
from jax import lax
from jax.experimental import pallas as pl
from jax.experimental.pallas import tpu as pltpu
from jax.sharding import PartitionSpec as P


KEY_CHANNELS = 64
HEAD_V = 128
BLOCK = 64
GATE_DENOMINATOR = 16.0
EPSILON = 1e-06
F32, BF16 = jnp.float32, jnp.bfloat16


def nt(a, b):
    return lax.dot_general(a, b, (((1,), (1,)), ((), ())), preferred_element_type=F32)


def tn(a, b):
    return lax.dot_general(a, b, (((0,), (0,)), ((), ())), preferred_element_type=F32)


def first_head(shape):
    return lax.broadcasted_iota(jnp.int32, shape, 1) < KEY_CHANNELS


VMEM = pl.BlockSpec(memory_space=pltpu.VMEM)


def cost(flops, size):
    return pl.CostEstimate(flops=flops, bytes_accessed=size, transcendentals=0)


def entering(value, axis, join, neutral, backward):
    count = lax.axis_size(axis)
    place = lax.axis_index(axis)
    ahead = count - 1 - place if backward else place
    gathered = jax.tree.map(
        lambda a, kind: lax.all_gather(a.astype(kind), axis), value, (jnp.bfloat16, jnp.bfloat16)
    )
    state = jax.tree.map(lambda a, e: jnp.zeros_like(a) + jnp.asarray(e, a.dtype), value, neutral)

    def one(lap, state):
        source = count - 1 - lap if backward else lap
        return join(
            state,
            jax.tree.map(
                lambda a, own: lax.dynamic_index_in_dim(a, source, 0, False).astype(own.dtype),
                gathered,
                value,
            ),
        )

    return lax.fori_loop(0, ahead, one, state)


def block_sweep(query_in, key_in, values_in, log_decay, span):
    sequence_length, head_count, key_dim = key_in.shape
    block_count = sequence_length // span

    def blocks(tensor):
        return jnp.transpose(
            tensor.reshape(block_count, span, head_count, tensor.shape[-1]), (0, 2, 1, 3)
        )

    lower_mask = jnp.tril(jnp.ones((span, span), dtype=bool))[:, :, None]

    def advance(carried, inputs):
        memory, offset = carried
        key_blk, value_blk, decay_blk, query_blk = inputs
        within = jnp.cumsum(decay_blk, axis=1)
        ending = within[:, -1, :]
        memory_next = jnp.exp(ending)[:, :, None] * memory + jnp.einsum(
            "hjd,hje->hde",
            key_blk * jnp.exp(ending[:, None, :] - within),
            value_blk,
            precision=lax.Precision.HIGHEST,
        )
        result = jnp.einsum(
            "hid,hde->hie", query_blk * jnp.exp(within), memory, precision=lax.Precision.HIGHEST
        )
        spread = jnp.exp(
            jnp.where(lower_mask, within[:, :, None, :] - within[:, None, :, :], -jnp.inf)
        )
        scores = jnp.einsum(
            "hid,hjd,hijd->hij", query_blk, key_blk, spread, precision=lax.Precision.HIGHEST
        )
        result = result + jnp.einsum(
            "hij,hje->hie", scores, value_blk, precision=lax.Precision.HIGHEST
        )
        reached = query_blk * jnp.exp(within + offset[:, None, :])
        return ((memory_next, offset + ending), (result, reached))

    start_memory = jnp.zeros((head_count, key_dim, values_in.shape[-1]), jnp.float32)
    start_offset = jnp.zeros((head_count, key_dim), jnp.float32)
    (memory, decay_total), (outputs, reached) = lax.scan(
        advance,
        (start_memory, start_offset),
        (blocks(key_in), blocks(values_in), blocks(log_decay), blocks(query_in)),
    )

    def unblock(tensor):
        return jnp.transpose(tensor, (0, 2, 1, 3)).reshape(
            sequence_length, head_count, tensor.shape[-1]
        )

    return (unblock(outputs), unblock(reached), memory, decay_total)


def head_mix(combined, head_norm_gain, output_gate_preact):
    sequence_length, head_count, width = combined.shape
    inverse = lax.rsqrt(jnp.mean(combined * combined, axis=-1, keepdims=True) + EPSILON)
    gate_act = jax.nn.silu(
        output_gate_preact.astype(jnp.float32).reshape(sequence_length, head_count, width)
    )
    weighted = combined * inverse * head_norm_gain.reshape(head_count, width) * gate_act
    return weighted.reshape(sequence_length, head_count * width).astype(jnp.bfloat16)


def row_norm(mid_rows, prenorm_gain):
    wide = mid_rows.astype(jnp.float32)
    inverse = lax.rsqrt(jnp.mean(wide * wide, axis=-1, keepdims=True) + EPSILON)
    return (wide * inverse * prenorm_gain).astype(jnp.bfloat16)


def combine_states(earlier, later):
    decay_early, memory_early = earlier
    decay_late, memory_late = later
    return (decay_early * decay_late, decay_late[:, :, None] * memory_early + memory_late)


def body(
    queries,
    key_projected,
    values,
    output_gate_preact,
    forward_decay_logits,
    backward_decay_logits,
    decay_logit_shift,
    decay_spike_values,
    residual,
    head_norm_gain,
    output_projection,
    prenorm_gain,
    gate_projection,
    up_projection,
    down_projection,
):
    sequence_length = queries.shape[0]
    local_heads = queries.shape[1] // KEY_CHANNELS
    query_f = queries.astype(jnp.float32).reshape(
        sequence_length, local_heads, KEY_CHANNELS
    ) * KEY_CHANNELS ** (-0.5)
    keys_f = key_projected.astype(jnp.float32).reshape(sequence_length, local_heads, KEY_CHANNELS)
    values_f = values.astype(jnp.float32).reshape(sequence_length, local_heads, HEAD_V)
    decay_spikes = jnp.transpose(decay_spike_values)[:, :, None]
    logit_shifts = decay_logit_shift.reshape(2, local_heads, KEY_CHANNELS)
    forward_decay = (
        jax.nn.log_sigmoid(
            forward_decay_logits.astype(jnp.float32).reshape(
                sequence_length, local_heads, KEY_CHANNELS
            )
            + logit_shifts[0]
        )
        / GATE_DENOMINATOR
        + decay_spikes
    )
    backward_decay = (
        jax.nn.log_sigmoid(
            backward_decay_logits.astype(jnp.float32).reshape(
                sequence_length, local_heads, KEY_CHANNELS
            )
            + logit_shifts[1]
        )
        / GATE_DENOMINATOR
        + decay_spikes
    )
    fwd_out, fwd_reach, fwd_memory, fwd_total = block_sweep(
        query_f, keys_f, values_f, forward_decay, BLOCK
    )
    bwd_out, bwd_reach, bwd_memory, bwd_total = block_sweep(
        query_f[::-1], keys_f[::-1], values_f[::-1], backward_decay[::-1], BLOCK
    )
    identity = (jnp.ones_like(fwd_total), jnp.zeros_like(fwd_memory))
    fwd_incoming = entering(
        (jnp.exp(fwd_total), fwd_memory), "sp", combine_states, identity, False
    )[1]
    bwd_incoming = entering((jnp.exp(bwd_total), bwd_memory), "sp", combine_states, identity, True)[
        1
    ]
    fwd_full = fwd_out + jnp.einsum(
        "lhd,hde->lhe", fwd_reach, fwd_incoming, precision=lax.Precision.HIGHEST
    )
    bwd_full = bwd_out + jnp.einsum(
        "lhd,hde->lhe", bwd_reach, bwd_incoming, precision=lax.Precision.HIGHEST
    )
    attended = head_mix(fwd_full + bwd_full[::-1], head_norm_gain, output_gate_preact)
    token_rows = lax.all_to_all(attended, "tp", split_axis=0, concat_axis=1, tiled=True)
    whole_out = lax.all_gather(output_projection, "tp", axis=0, tiled=True)
    projected = jnp.dot(token_rows, whole_out, preferred_element_type=jnp.float32)
    mid_rows = (residual.astype(jnp.float32) + projected).astype(jnp.bfloat16)
    normed = row_norm(mid_rows, prenorm_gain)
    fetched = (
        lax.all_gather(gate_projection, "sp", axis=0, tiled=True),
        lax.all_gather(up_projection, "sp", axis=0, tiled=True),
        lax.all_gather(down_projection, "sp", axis=1, tiled=True),
    )
    gate_full, up_full, down_full = fetched
    piece = lax.all_gather(normed, "tp", axis=0, tiled=True)
    gate_part = jnp.dot(piece, gate_full, preferred_element_type=jnp.float32)
    up_part = jnp.dot(piece, up_full, preferred_element_type=jnp.float32)
    hidden = (jax.nn.silu(gate_part) * up_part).astype(jnp.bfloat16)
    summed = lax.psum_scatter(
        jnp.dot(hidden, down_full, preferred_element_type=jnp.float32).astype(jnp.bfloat16),
        "tp",
        scatter_dimension=0,
        tiled=True,
    ).astype(jnp.float32)
    return (mid_rows.astype(jnp.float32) + 0.5 * summed).astype(jnp.bfloat16)


MESH = pl.DeviceIdType.MESH
PIECES = 5


def log_decay(logits, shift, spike):
    x = logits.astype(F32) + shift
    soft = jnp.minimum(x, 0.0) - jnp.log1p(jnp.exp(-jnp.abs(x)))
    return soft / GATE_DENOMINATOR + spike


def own_states(k_ref, v_ref, fd_ref, bd_ref, shift_ref, spike_ref, within_ref, kd_ref, fwd_ref, bwd_ref):
    tokens, lanes = k_ref.shape
    blocks = tokens // BLOCK
    row = lax.broadcasted_iota(jnp.int32, (2 * BLOCK, 2 * BLOCK), 0)
    col = lax.broadcasted_iota(jnp.int32, (2 * BLOCK, 2 * BLOCK), 1)
    r, c = row % BLOCK, col % BLOCK
    ahead = jnp.where(row < BLOCK, r - c, c - r)
    tri = jnp.where(ahead >= 0, 1.0, 0.0).astype(BF16)
    half = first_head((BLOCK, lanes))
    spikes = jnp.transpose(jnp.concatenate([spike_ref[...]] * 4, axis=0))
    ends = []
    for b in range(blocks):
        at = slice(b * BLOCK, (b + 1) * BLOCK)
        spike = jnp.where(half, spikes[at, 0:1], spikes[at, 1:2])
        parts = [log_decay(ref[at, :], shift_ref[n : n + 1, :], spike) for n, ref in enumerate((fd_ref, bd_ref))]
        d = jnp.concatenate(parts, axis=1)
        hi = d.astype(BF16)
        lo = (d - hi.astype(F32)).astype(BF16)
        both = jnp.dot(tri, jnp.concatenate([hi, lo], axis=0), preferred_element_type=F32)
        fwd, bwd = both[:BLOCK, :lanes], both[BLOCK:, lanes:]
        within_ref[at, :lanes] = fwd
        within_ref[at, lanes:] = bwd
        ends.append((fwd[BLOCK - 1 :, :], bwd[:1, :]))
    zero = jnp.zeros((1, lanes), F32)
    after, before = [zero] * blocks, [zero] * blocks
    for b in range(1, blocks):
        before[b] = before[b - 1] + ends[b - 1][1]
        after[blocks - 1 - b] = after[blocks - b] + ends[blocks - b][0]
    totals = after[0] + ends[0][0], before[-1] + ends[-1][1]
    for b in range(blocks):
        at = slice(b * BLOCK, (b + 1) * BLOCK)
        key = k_ref[at, :].astype(F32)
        kd_ref[at, :lanes] = (key * jnp.exp((ends[b][0] + after[b]) - within_ref[at, :lanes])).astype(BF16)
        kd_ref[at, lanes:] = (key * jnp.exp((ends[b][1] + before[b]) - within_ref[at, lanes:])).astype(BF16)
    full = tn(v_ref[...], kd_ref[...])
    mine = first_head((HEAD_V, lanes))
    for n, ref in enumerate((fwd_ref, bwd_ref)):
        u = full[:, n * lanes : (n + 1) * lanes]
        ref[:HEAD_V, :] = jnp.where(mine, u[:HEAD_V], u[HEAD_V:]).astype(BF16)
        ref[HEAD_V:, :] = jnp.broadcast_to(jnp.exp(totals[n]), (16, lanes)).astype(BF16)


def spread(state):
    mine = first_head(state.shape)
    return jnp.concatenate([jnp.where(mine, state, 0.0), jnp.where(mine, 0.0, state)], axis=0).astype(BF16)


def pack(u):
    top = u[:HEAD_V]
    return jnp.where(first_head(top.shape), top, u[HEAD_V:])


def backward_states(k_ref, v_ref, within_ref, state, held_ref):
    tokens, lanes = k_ref.shape
    for b in reversed(range(tokens // BLOCK)):
        at = slice(b * BLOCK, (b + 1) * BLOCK)
        held_ref[b] = spread(state)
        within = within_ref[at, lanes:]
        end = within[:1, :]
        kd = (k_ref[at, :].astype(F32) * jnp.exp(end - within)).astype(BF16)
        state = state * jnp.exp(end) + pack(tn(v_ref[at, :], kd))


def attend(q_ref, k_ref, v_ref, within_ref, gate_ref, gain_ref, fwd_state, held_ref, out_ref):
    tokens, lanes = k_ref.shape
    row = lax.broadcasted_iota(jnp.int32, (2 * BLOCK, BLOCK), 0) % BLOCK
    col = lax.broadcasted_iota(jnp.int32, (2 * BLOCK, BLOCK), 1)
    half = first_head((BLOCK, lanes))
    for b in range(tokens // BLOCK):
        at = slice(b * BLOCK, (b + 1) * BLOCK)
        query = q_ref[at, :].astype(F32) * KEY_CHANNELS ** (-0.5)
        key = k_ref[at, :].astype(F32)
        value = v_ref[at, :]
        scores, reach = [], []
        for n in range(2):
            within = within_ref[at, n * lanes : (n + 1) * lanes]
            pivot = within[BLOCK // 2 - 1 + n : BLOCK // 2 + n, :]
            near = (query * jnp.exp(within - pivot)).astype(BF16)
            far = (key * jnp.exp(pivot - within)).astype(BF16)
            zero = jnp.zeros_like(near)
            pair = jnp.concatenate([jnp.where(half, near, zero), jnp.where(half, zero, near)], axis=0)
            scores.append(nt(pair, far))
            reach.append((query * jnp.exp(within)).astype(BF16))
        score = (jnp.where(col <= row, scores[0], 0.0) + jnp.where(col >= row, scores[1], 0.0)).astype(BF16)
        states = jnp.concatenate([spread(fwd_state), held_ref[b]], axis=1)
        result = nt(jnp.concatenate(reach, axis=1), states)
        for h in range(2):
            lane = slice(h * HEAD_V, (h + 1) * HEAD_V)
            x = result[:, lane] + jnp.dot(
                score[h * BLOCK : (h + 1) * BLOCK], value[:, lane], preferred_element_type=F32
            )
            inverse = lax.rsqrt(jnp.mean(x * x, axis=-1, keepdims=True) + EPSILON)
            g = gate_ref[at, lane].astype(F32)
            out_ref[at, lane] = (x * inverse * gain_ref[:, lane] * (g * jax.nn.sigmoid(g))).astype(BF16)
        within = within_ref[at, :lanes]
        end = within[BLOCK - 1 :, :]
        kd = (key * jnp.exp(end - within)).astype(BF16)
        fwd_state = fwd_state * jnp.exp(end) + pack(tn(value, kd))


def pick(i, table):
    value = table[0]
    for n, item in enumerate(table[1:], 1):
        value = jnp.where(i == n, item, value)
    return value


def ds(first, size):
    return pl.ds(pl.multiple_of(first, size if size % 128 == 0 else 16), size)


def layer_kernel(
    k_hbm, v_hbm, fd_hbm, bd_hbm, shift_hbm, spike_hbm, q_hbm, gate_hbm, gain_hbm, norm_hbm,
    res_hbm, out_hbm, g_hbm, u_hbm, d_hbm,
    out_ref,
    k_ref, v_ref, fd_ref, bd_ref, shift_ref, spike_ref, q_ref, gate_ref, gain_ref, norm_ref, in_s,
    within, kd, fown, bown, fgot, bgot, fstate, bstate, held, attended, rows, outl, outh, pout, rgot, rxs, rxg, squares, res, mid, acts,
    wgu, wd, hid, part, got, xsend, xgot, esend, egot, erelay,
    loc, st_s, st_r, a2a_s, a2a_r, ow_s, ow_r, rs_s, rs_r, rx_s, rx_r, ag_s, ag_r, ea_s, ea_r, gs, gr, dsd, drv, cr_s, cr_r, xo_s, xo_r,
    eo_s, eo_r, er_s, er_r,
):
    count = lax.axis_size("sp")
    side, place, me = lax.axis_index("grp"), lax.axis_index("sp"), lax.axis_index("tp")
    chip, core = me // 2, me % 2
    tc, tx, td = 2 * chip + 1 - core, 2 * (1 - chip) + core, 2 * (1 - chip) + 1 - core
    upper = place // 2
    e, m, o, oe = 3 * upper, 1 + upper, 2 - upper, 3 - 3 * upper
    middle = place * (count - 1 - place) > 0
    outer = jnp.logical_not(middle)
    own = res.shape[0]
    width = attended.shape[1]
    model = mid.shape[1]
    depth, hidden = g_hbm.shape
    tile = hidden // PIECES
    hr = depth // 2
    dr = hidden // 2
    dw = wd.shape[3]
    chunks = part.shape[1]
    wide = pout.shape[2]
    parts = pout.shape[0]
    nrow = own // 2

    def remote(src, dst, send, recv, **dev):
        return pltpu.make_async_remote_copy(
            src_ref=src, dst_ref=dst, send_sem=send, recv_sem=recv, device_id=dev, device_id_type=MESH
        )

    def slot(source, dev):
        return source - jnp.where(source > dev.get("sp", place), 1, 0)

    def gu(n, source, half, p, local=False, again=False, **dev):
        dst = wgu.at[n, p, ds(source * depth + half * hr, hr), :]
        src = (g_hbm, u_hbm)[n].at[ds(half * hr, hr), ds(p * tile, tile)] if local else dst
        send = gs.at[source, 1 - half if again else half]
        return remote(src, dst, send, gr.at[n, slot(source, dev), half, p], **(dev or dict(sp=o)))

    def dn(source, half, p, r, local=False, again=False, **dev):
        dst = wd.at[source, p, ds(half * dr + r * (dr // 2), dr // 2), :]
        src = d_hbm.at[ds(half * dr + r * (dr // 2), dr // 2), p * dw : (p + 1) * dw] if local else dst
        send = dsd.at[source, 1 - half if again else half]
        return remote(src, dst, send, drv.at[slot(source, dev), half, p, r], **(dev or dict(sp=o)))

    def send_gu(source, half, p, local=False, again=False, **dev):
        for n in range(2):
            gu(n, source, half, p, local, again, **dev).start()

    def take_gu(source, half, p):
        for n in range(2):
            gu(n, source, half, p).wait_recv()

    def relay_one(n, source, p, **dev):
        gu(n, source, side, p).wait_recv()
        gu(n, source, side, p, **dev).start()

    def relay_gu(source, p, **dev):
        for n in range(2):
            relay_one(n, source, p, **dev)

    def send_dn(half, p, **dev):
        for r in range(2):
            dn(place, half, p, r, True, **dev).start()

    def take_dn(source, half, p):
        for r in range(2):
            dn(source, half, p, r).wait_recv()

    def relay_dn(source, p, r, **dev):
        dn(source, side, p, r).wait_recv()
        dn(source, side, p, r, **dev).start()

    def sent(ref, sem):
        remote(ref, ref, sem, sem, sp=o).wait_send()

    def sent_gu(source, half, low, high, again=False):
        at = ds(source * depth + half * hr, hr)
        sent(wgu.at[:, low:high, at, :], gs.at[source, 1 - half if again else half])

    def sent_dn(source, half, low, high):
        sent(wd.at[source, low:high, ds(half * dr, dr), :], dsd.at[source, half])

    def landed(ref, sem):
        remote(ref, ref, sem, sem, sp=o).wait_recv()

    def ow(kind, block, i, dev, local=False):
        half = width // 2
        dst = outh.at[ds(block * width + i * half, half), :]
        src = out_hbm.at[i * half : (i + 1) * half, model // 2 :] if local else dst
        return remote(src, dst, ow_s.at[kind], ow_r.at[i if kind == 0 else 1 + kind], tp=dev)

    def relay_ow(i):
        ow(0, tx, i, tc).wait_recv()
        ow(2, tx, i, tc).start()

    def a2a(block, dev):
        src = attended.at[ds(dev * own, own), :]
        return remote(src, rows.at[:, ds(block * width, width)], a2a_s.at[0], a2a_r.at[block], tp=dev)

    def rs(c, j):
        block = 2 * j + 1 - core
        return remote(pout.at[c, ds(block * own, own), :], rgot.at[c, j], rs_s.at[0], rs_r.at[c], tp=tc)

    def rx(c):
        return remote(rxs.at[c], rxg.at[c], rx_s.at[0], rx_r.at[c], tp=tx)

    def ag(q, kind, block, i, dev):
        at = acts.at[q, ds(block * own + i * nrow, nrow), :]
        return remote(at, at, ag_s.at[q, kind], ag_r.at[q, i if kind == 0 else 1 + kind], tp=dev)

    def to_host(i):
        at = ds(me * own + i * nrow, nrow)
        return remote(acts.at[0, at, :], acts.at[1, at, :], ea_s.at[0], ea_r.at[i], sp=m)

    def gathered(q):
        for kind, block in ((1, tc), (2, td)):
            landed(acts.at[q, ds(block * own, own), :], ag_r.at[q, 1 + kind])

    def state_copy(n, k, dev):
        src, dst = ((fown, fgot), (bown, bgot))[n]
        return remote(src, dst.at[k - 1], st_s.at[n, k - 1], st_r.at[n, k - 1], sp=dev)

    def cr(q, i, j):
        block = 2 * j + 1 - core
        return remote(part.at[q, i, ds(block * own, own), :], got.at[q, i, j], cr_s.at[q], cr_r.at[q, i], tp=tc)

    def xo(q, i):
        return remote(xsend.at[q, i], xgot.at[q, i], xo_s.at[q], xo_r.at[q, i], tp=tx)

    def eo(i, n):
        dst = egot.at[0, i] if n == 0 else erelay.at[i]
        return remote(esend.at[i, n], dst, eo_s.at[n], eo_r.at[i, n], sp=e)

    def er(i):
        return remote(erelay.at[i], egot.at[1, i], er_s.at[0], er_r.at[i], tp=tx)

    own_copies = []
    for p in range(PIECES):
        for n in range(2):
            own_copies.append(
                pltpu.make_async_copy(
                    (g_hbm, u_hbm)[n].at[:, p * tile : (p + 1) * tile],
                    wgu.at[n, p, ds(place * depth, depth), :],
                    loc.at[0],
                )
            )
    for p in range(2):
        own_copies.append(pltpu.make_async_copy(d_hbm.at[:, p * dw : (p + 1) * dw], wd.at[place, p], loc.at[1]))
    own_gu = wgu.at[:, :, ds(place * depth, depth), :]
    own_waits = [
        pltpu.make_async_copy(own_gu, own_gu, loc.at[0]),
        pltpu.make_async_copy(wd.at[place], wd.at[place], loc.at[1]),
    ]
    own_low = pltpu.make_async_copy(out_hbm.at[:, : model // 2], outl, loc.at[2])
    own_high = pltpu.make_async_copy(out_hbm.at[:, model // 2 :], outh.at[ds(me * width, width), :], loc.at[4])
    own_res = pltpu.make_async_copy(res_hbm, res, loc.at[3])

    barrier = pltpu.get_barrier_semaphore()
    friends = [dict(sp=lax.rem(place + k, count)) for k in range(1, count)]
    friends += [dict(grp=1 - side)] + [dict(tp=t) for t in (tc, tx, td)]
    for friend in friends:
        pl.semaphore_signal(barrier, inc=1, device_id=friend, device_id_type=MESH)
    loads = [
        pltpu.make_async_copy(src, dst, in_s.at[n])
        for n, (src, dst) in enumerate(
            (
                (k_hbm, k_ref),
                (v_hbm, v_ref),
                (fd_hbm, fd_ref),
                (bd_hbm, bd_ref),
                (shift_hbm, shift_ref),
                (spike_hbm, spike_ref),
                (q_hbm, q_ref),
                (gate_hbm, gate_ref),
                (gain_hbm, gain_ref),
                (norm_hbm, norm_ref),
            )
        )
    ]
    for load in loads:
        load.start()
    own_low.start()
    own_high.start()
    own_res.start()
    for load in loads[:6]:
        load.wait()
    own_states(k_ref, v_ref, fd_ref, bd_ref, shift_ref, spike_ref, within, kd, fown, bown)
    pl.semaphore_wait(barrier, len(friends))

    for k in range(1, count):

        @pl.when(place + k < count)
        def _(k=k):
            state_copy(0, k, place + k).start()

        @pl.when(place >= k)
        def _(k=k):
            state_copy(1, k, place - k).start()

    @pl.when(middle)
    def _():
        for p in range(PIECES):
            send_gu(place, side, p, True, sp=o)

    @pl.when(outer)
    def _():
        for p in range(PIECES):
            send_gu(place, side, p, True, sp=m)

    for i in range(2):
        ow(0, me, i, tx, True).start()
        ow(1, me, i, tc, True).start()

    @pl.when(middle)
    def _():
        for copy in own_copies:
            copy.start()

    for load in loads[6:]:
        load.wait()
    fstate[...] = jnp.zeros_like(fstate)
    bstate[...] = jnp.zeros_like(bstate)
    for k in reversed(range(1, count)):

        @pl.when(place >= k)
        def _(k=k):
            state_copy(0, k, place).wait_recv()
            decay = fgot[k - 1, HEAD_V : HEAD_V + 1, :].astype(F32)
            fstate[...] = fstate[...] * decay + fgot[k - 1, :HEAD_V, :].astype(F32)

        @pl.when(place + k < count)
        def _(k=k):
            state_copy(1, k, place).wait_recv()
            decay = bgot[k - 1, HEAD_V : HEAD_V + 1, :].astype(F32)
            bstate[...] = bstate[...] * decay + bgot[k - 1, :HEAD_V, :].astype(F32)

    backward_states(k_ref, v_ref, within, bstate[...], held)
    attend(q_ref, k_ref, v_ref, within, gate_ref, gain_ref, fstate[...], held, attended)
    others = (tx, td, tc)
    for t in others:
        a2a(me, t).start()
    rows[:, ds(me * width, width)] = attended[ds(me * own, own), :]
    own_low.wait()
    for c in range(parts):
        at = slice(c * wide, (c + 1) * wide)
        pout[c] = jnp.dot(attended[...], outl[:, at], preferred_element_type=F32).astype(BF16)
        for j in range(2):
            rs(c, j).start()
    @pl.when(middle)
    def _():
        relay_one(0, o, 0, grp=1 - side)

    relay_ow(0)
    for c in range(parts):
        landed(rgot.at[c], rs_r.at[c])
        rxs[c] = (pout[c, ds(tx * own, own), :].astype(F32) + rgot[c, 1 - chip].astype(F32)).astype(BF16)
        rx(c).start()

    def mix(at, projected):
        mixed = (res[:, at].astype(F32) + projected).astype(BF16)
        mid[:, at] = mixed
        mixed = mixed.astype(F32)
        return jnp.sum(mixed * mixed, axis=-1, keepdims=True)

    @pl.when(middle)
    def _():
        relay_one(1, o, 0, grp=1 - side)
        relay_gu(e, 0, sp=o)

    relay_ow(1)

    @pl.when(middle)
    def _():
        relay_gu(o, 1, grp=1 - side)
        relay_gu(e, 1, sp=o)

    for t in others:
        a2a(t, t).wait_recv()
    for kind, t in ((1, tc), (2, td)):
        landed(outh.at[ds(t * width, width), :], ow_r.at[1 + kind])
    own_high.wait()
    own_res.wait()
    total = jnp.zeros((own, 1), F32)
    for n in range(parts):
        high = slice(n * wide, (n + 1) * wide)
        projected = jnp.dot(rows[...], outh[:, high], preferred_element_type=F32)
        total += mix(slice(model // 2 + n * wide, model // 2 + (n + 1) * wide), projected)
    squares[...] = jnp.broadcast_to(total, squares.shape)

    @pl.when(middle)
    def _():
        relay_gu(o, 2, grp=1 - side)
        relay_gu(e, 2, sp=o)

    total = squares[:, :1]
    for n in range(parts):
        rx(n).wait_recv()
        projected = pout[n, ds(me * own, own), :].astype(F32) + rgot[n, chip].astype(F32) + rxg[n].astype(F32)
        total += mix(slice(n * wide, (n + 1) * wide), projected)
    inverse = lax.rsqrt(total / model + EPSILON)
    for n in range(2 * parts):
        at = slice(n * wide, (n + 1) * wide)
        acts[0, ds(me * own, own), at] = (mid[:, at].astype(F32) * inverse * norm_ref[:, at]).astype(BF16)

    direct = (1, 1, 1, 0, 0, 0, 0, 1)
    whole = [i for i, d in enumerate(direct) if d]

    def straight(i):
        return direct[i] if isinstance(i, int) else pick(i, direct)

    sources = (m, m, o, o, e, oe, e, oe)
    sides = (0, 1, 0, 1, 0, 0, 1, 1)

    @pl.when(middle)
    def _():
        for i in range(2):
            ag(0, 0, me, i, tx).start()
            ag(0, 1, me, i, tc).start()
        for p in range(3, PIECES):
            relay_gu(o, p, grp=1 - side)
            relay_gu(e, p, sp=o)
        send_gu(e, side, 1, again=True, grp=1 - side)
        for p in range(2):
            send_dn(side, p, sp=o)
        send_dn(1 - side, 1, sp=o)
        for copy in own_waits:
            copy.wait()

        def relay_own(i):
            ag(0, 0, tx, i, tc).wait_recv()
            ag(0, 2, tx, i, tc).start()

        def relay_hosted(i):
            to_host(i).wait_recv()
            ag(1, 0, me, i, tx).start()
            ag(1, 1, me, i, tc).start()

        def pass_hosted(i):
            ag(1, 0, tx, i, tc).wait_recv()
            ag(1, 2, tx, i, tc).start()

        relay_gu(oe, 0, grp=1 - side)
        relay_own(0)
        relay_hosted(0)
        relay_gu(oe, 1, grp=1 - side)
        relay_own(1)
        relay_gu(oe, 2, grp=1 - side)
        relay_hosted(1)

        order = [(0, 0), (0, 1), (0, 2), (1, 0), (0, 3), (1, 1), (1, 2), (1, 3), (0, 4), (1, 4)]

        def fold(i, q):
            landed(got.at[q, i], cr_r.at[q, i])

            def both(block, j):
                return part[q, i, ds(block * own, own), :].astype(F32) + got[q, i, j].astype(F32)

            @pl.when(jnp.logical_or(q == 0, straight(i) == 0))
            def _():
                xsend[q, i] = both(tx, 1 - chip).astype(BF16)
                xo(q, i).start()

            @pl.when(jnp.logical_and(q == 1, straight(i) == 1))
            def _():
                esend[i, 1] = both(tx, 1 - chip).astype(BF16)
                eo(i, 1).start()
                esend[i, 0] = both(me, chip).astype(BF16)
                eo(i, 0).start()

        def push(i):
            if direct[i]:
                return
            xo(1, i).wait_recv()
            mixed = part[1, i, ds(me * own, own), :].astype(F32) + got[1, i, chip].astype(F32)
            esend[i, 0] = (mixed + xgot[1, i].astype(F32)).astype(BF16)
            eo(i, 0).start()

        def product(q, i):
            weight = wd[pick(i, sources), pick(i, sides)]
            part[q, i] = jnp.dot(hid[q], weight, preferred_element_type=F32).astype(BF16)
            for j in range(2):
                cr(q, i, j).start()

        def first(i, carry):
            q, j = pick(i, [a for a, _ in order]), pick(i, [b for _, b in order])

            @pl.when(i == 0)
            def _():
                gathered(0)

            @pl.when(i == 1)
            def _():
                pass_hosted(0)
                relay_gu(oe, 3, grp=1 - side)

            @pl.when(i == 2)
            def _():
                relay_gu(oe, 4, grp=1 - side)
                pass_hosted(1)

            @pl.when(i == 3)
            def _():
                gathered(1)

            @pl.when(i == 5)
            def _():
                for r in range(2):
                    relay_dn(o, 0, r, grp=1 - side)

            @pl.when(i == 9)
            def _():
                relay_dn(e, 0, 0, sp=o)

            @pl.when(q == 0)
            def _():
                for source in (o, oe, e):
                    take_gu(source, 1 - side, j)

            g = jnp.dot(acts[q], wgu[0, j], preferred_element_type=F32)
            u = jnp.dot(acts[q], wgu[1, j], preferred_element_type=F32)
            hid[q, :, ds(j * tile, tile)] = (g * jax.nn.sigmoid(g) * u).astype(BF16)
            return carry

        lax.fori_loop(0, len(order), first, 0)

        def second(s, carry):
            i, q = s // 2, 1 - s % 2

            @pl.when(s == 0)
            def _():
                relay_dn(e, 0, 1, sp=o)
                dn(e, side, 0, 1, again=True, grp=1 - side).start()

            @pl.when(s == 4)
            def _():
                take_dn(o, 1 - side, 0)

            @pl.when(s == 5)
            def _():
                relay_dn(e, 1, 0, sp=o)

            @pl.when(s == 6)
            def _():
                take_dn(o, side, 1)
                take_dn(o, 1 - side, 1)

            @pl.when(s == 8)
            def _():
                relay_dn(oe, 0, 0, grp=1 - side)
                fold(3, 1)
                relay_dn(e, 1, 1, sp=o)
                fold(3, 0)
                relay_dn(oe, 0, 1, grp=1 - side)
                push(2)
                take_dn(e, 1 - side, 0)

            @pl.when(s == 10)
            def _():
                push(3)
                relay_dn(oe, 1, 0, grp=1 - side)
                fold(4, 1)
                fold(4, 0)
                take_dn(oe, 1 - side, 0)

            @pl.when(s == 12)
            def _():
                relay_dn(oe, 1, 1, grp=1 - side)
                fold(5, 1)
                push(4)
                take_dn(e, 1 - side, 1)

            @pl.when(s == 14)
            def _():
                fold(6, 1)
                push(5)
                take_dn(oe, 1 - side, 1)

            product(q, i)

            @pl.when(((s > 1) & (s < 8)) | (s == 12) | (s == 14))
            def _():
                fold(i - 1, jnp.where(s < 8, q, 0))

            return carry

        lax.fori_loop(0, 2 * chunks, second, 0)
        fold(chunks - 1, 1)
        fold(chunks - 1, 0)
        push(chunks - 2)

        for i in range(chunks):
            xo(0, i).wait_recv()
            at = ds((2 * sources[i] + sides[i]) * dw, dw)
            total = part[0, i, ds(me * own, own), :].astype(F32) + got[0, i, chip].astype(F32) + xgot[0, i].astype(F32)
            out_ref[:, at] = (mid[:, at].astype(F32) + 0.5 * total).astype(BF16)

        for source in (place, e, o, oe):
            sent_gu(source, side, 0, PIECES)
        sent_gu(e, side, 0, 1, again=True)
        sent(wd.at[e, 0, : dr // 2, :], dsd.at[e, 1 - side])
        for source in (place, e, oe):
            sent_dn(source, side, 0, 2)
        sent_dn(o, side, 0, 1)
        sent_dn(place, 1 - side, 1, 2)
        for q in range(2):
            for kind in range(3):
                sent(acts.at[q, ds(me * own, own), :], ag_s.at[q, kind])
            sent(got.at[q], cr_s.at[q])
        sent(xsend.at[0], xo_s.at[0])
        sent(xsend.at[1, : chunks - len(whole)], xo_s.at[1])
        sent(esend.at[:, 0], eo_s.at[0])
        sent(esend.at[: len(whole), 1], eo_s.at[1])

    @pl.when(outer)
    def _():
        for i in range(2):
            to_host(i).start()
        for p in (0, 2, 3, 4):
            send_gu(place, 1 - side, p, True, sp=m)
        for p in range(2):
            send_dn(side, p, sp=m)
        dn(place, 1 - side, 0, 0, True, sp=m).start()
        send_dn(1 - side, 1, sp=m)

        def finish(i):
            eo(i, 0).wait_recv()
            total = egot[0, i].astype(F32)
            if direct[i]:
                er(i).wait_recv()
                total += egot[1, i].astype(F32)
            at = ds((2 * sources[i] + sides[i]) * dw, dw)
            out_ref[:, at] = (mid[:, at].astype(F32) + 0.5 * total).astype(BF16)

        for i in range(chunks):
            if direct[i]:
                eo(i, 1).wait_recv()
                er(i).start()
            if i > 1:
                finish(i - 2)
        finish(chunks - 2)
        finish(chunks - 1)
        sent(acts.at[0, ds(me * own, own), :], ea_s.at[0])
        sent_gu(place, side, 0, PIECES)
        sent_gu(place, 1 - side, 0, PIECES - 1)
        sent_dn(place, side, 0, 2)
        sent(wd.at[place, 0, : dr + dr // 2, :], dsd.at[place, 1 - side])
        sent(erelay.at[: len(whole)], er_s.at[0])

    for k in range(1, count):

        @pl.when(place + k < count)
        def _(k=k):
            state_copy(0, k, place).wait_send()

        @pl.when(place >= k)
        def _(k=k):
            state_copy(1, k, place).wait_send()

    sent(rows.at[:, : 3 * width], a2a_s.at[0])
    for kind in range(3):
        sent(outh.at[ds(me * width, width), :], ow_s.at[kind])
    sent(rgot, rs_s.at[0])
    sent(rxs, rx_s.at[0])


def fast_body(
    queries,
    key_projected,
    values,
    output_gate_preact,
    forward_decay_logits,
    backward_decay_logits,
    decay_logit_shift,
    decay_spike_values,
    residual,
    head_norm_gain,
    output_projection,
    prenorm_gain,
    gate_projection,
    up_projection,
    down_projection,
):
    count = lax.axis_size("sp")
    tokens, lanes = queries.shape
    width = values.shape[1]
    own, model = residual.shape
    depth, hidden = gate_projection.shape
    dw = down_projection.shape[1] // 2
    chunks = 2 * count
    blocks = tokens // BLOCK
    dma = lambda *shape: pltpu.SemaphoreType.DMA(shape)
    state = (HEAD_V + 16, lanes)
    V = pltpu.VMEM
    scratch = [
        V((tokens, lanes), BF16),
        V((tokens, width), BF16),
        V((tokens, lanes), BF16),
        V((tokens, lanes), BF16),
        V(decay_logit_shift.shape, F32),
        V(decay_spike_values.shape, F32),
        V((tokens, lanes), BF16),
        V((tokens, width), BF16),
        V((1, width), F32),
        V((1, model), F32),
        dma(10),
        V((tokens, 2 * lanes), F32),
        V((tokens, 2 * lanes), BF16),
        V(state, BF16),
        V(state, BF16),
        V((count - 1,) + state, BF16),
        V((count - 1,) + state, BF16),
        V((HEAD_V, lanes), F32),
        V((HEAD_V, lanes), F32),
        V((blocks, 2 * HEAD_V, lanes), BF16),
        V((tokens, width), BF16),
        V((own, tokens // own * width), BF16),
        V((width, model // 2), BF16),
        V((tokens // own * width, model // 2), BF16),
        V((2, tokens, model // 4), BF16),
        V((2, 2, own, model // 4), BF16),
        V((2, own, model // 4), BF16),
        V((2, own, model // 4), BF16),
        V((own, 128), F32),
        V((own, model), BF16),
        V((own, model), BF16),
        V((2, tokens, model), BF16),
        V((2, PIECES, model, hidden // PIECES), BF16),
        V((count, 2, hidden, dw), BF16),
        V((2, tokens, hidden), BF16),
        V((2, chunks, tokens, dw), BF16),
        V((2, chunks, 2, own, dw), BF16),
        V((2, chunks, own, dw), BF16),
        V((2, chunks, own, dw), BF16),
        V((chunks, 2, own, dw), BF16),
        V((2, chunks, own, dw), BF16),
        V((chunks, own, dw), BF16),
        dma(5),
        dma(2, count - 1),
        dma(2, count - 1),
        dma(1),
        dma(tokens // own),
        dma(3),
        dma(4),
        dma(1),
        dma(2),
        dma(1),
        dma(2),
        dma(2, 3),
        dma(2, 4),
        dma(1),
        dma(2),
        dma(count, 2),
        dma(2, count - 1, 2, PIECES),
        dma(count, 2),
        dma(count - 1, 2, 2, 2),
        dma(2),
        dma(2, chunks),
        dma(2),
        dma(2, chunks),
        dma(2),
        dma(chunks, 2),
        dma(1),
        dma(chunks),
    ]
    anywhere = pl.BlockSpec(memory_space=pl.ANY)
    return pl.pallas_call(
        layer_kernel,
        out_shape=pltpu.MemorySpace.VMEM((own, model), BF16),
        in_specs=[anywhere] * 15,
        out_specs=VMEM,
        scratch_shapes=scratch,
        compiler_params=pltpu.CompilerParams(
            collective_id=0, has_side_effects=True, vmem_limit_bytes=61000000
        ),
        cost_estimate=cost(3 * 10**10, 3 * 10**7),
        name="layer",
    )(
        key_projected,
        values,
        forward_decay_logits,
        backward_decay_logits,
        decay_logit_shift,
        decay_spike_values,
        queries,
        output_gate_preact,
        head_norm_gain[None, :],
        prenorm_gain[None, :],
        residual,
        output_projection,
        gate_projection,
        up_projection,
        down_projection,
    )


def solution(mesh):
    in_specs = (
        P(("grp", "sp"), "tp"),
        P(("grp", "sp"), "tp"),
        P(("grp", "sp"), "tp"),
        P(("grp", "sp"), "tp"),
        P(("grp", "sp"), "tp"),
        P(("grp", "sp"), "tp"),
        P(None, "tp"),
        P("tp", ("grp", "sp")),
        P(("grp", "sp", "tp"), None),
        P("tp"),
        P("tp", None),
        P(),
        P("sp", "tp"),
        P("sp", "tp"),
        P("tp", "sp"),
    )
    out_specs = P(("grp", "sp", "tp"), None)

    def run(*args):
        lanes = args[0].shape[1]
        sizes = (mesh.shape["grp"], mesh.shape["sp"], mesh.shape["tp"])
        fits = lanes == 2 * KEY_CHANNELS and sizes == (2, 4, 4)
        return fast_body(*args) if fits else body(*args)

    return jax.shard_map(run, mesh=mesh, in_specs=in_specs, out_specs=out_specs, check_vma=False)
```

```python
import functools

import jax
import jax.numpy as jnp
from jax import lax
from jax.experimental import pallas as pl
from jax.experimental.pallas import tpu as pltpu
from jax.sharding import PartitionSpec as P


KEY_CHANNELS = 64
HEAD_V = 128
BLOCK = 64
GATE_DENOMINATOR = 16.0
EPSILON = 1e-06
F32, BF16 = jnp.float32, jnp.bfloat16


def nt(a, b):
    return lax.dot_general(a, b, (((1,), (1,)), ((), ())), preferred_element_type=F32)


def tn(a, b):
    return lax.dot_general(a, b, (((0,), (0,)), ((), ())), preferred_element_type=F32)


def first_head(shape):
    return lax.broadcasted_iota(jnp.int32, shape, 1) < KEY_CHANNELS


VMEM = pl.BlockSpec(memory_space=pltpu.VMEM)


def cost(flops, size):
    return pl.CostEstimate(flops=flops, bytes_accessed=size, transcendentals=0)


def entering(value, axis, join, neutral, backward):
    count = lax.axis_size(axis)
    place = lax.axis_index(axis)
    ahead = count - 1 - place if backward else place
    gathered = jax.tree.map(
        lambda a, kind: lax.all_gather(a.astype(kind), axis), value, (jnp.bfloat16, jnp.bfloat16)
    )
    state = jax.tree.map(lambda a, e: jnp.zeros_like(a) + jnp.asarray(e, a.dtype), value, neutral)

    def one(lap, state):
        source = count - 1 - lap if backward else lap
        return join(
            state,
            jax.tree.map(
                lambda a, own: lax.dynamic_index_in_dim(a, source, 0, False).astype(own.dtype),
                gathered,
                value,
            ),
        )

    return lax.fori_loop(0, ahead, one, state)


def block_sweep(query_in, key_in, values_in, log_decay, span):
    sequence_length, head_count, key_dim = key_in.shape
    block_count = sequence_length // span

    def blocks(tensor):
        return jnp.transpose(
            tensor.reshape(block_count, span, head_count, tensor.shape[-1]), (0, 2, 1, 3)
        )

    lower_mask = jnp.tril(jnp.ones((span, span), dtype=bool))[:, :, None]

    def advance(carried, inputs):
        memory, offset = carried
        key_blk, value_blk, decay_blk, query_blk = inputs
        within = jnp.cumsum(decay_blk, axis=1)
        ending = within[:, -1, :]
        memory_next = jnp.exp(ending)[:, :, None] * memory + jnp.einsum(
            "hjd,hje->hde",
            key_blk * jnp.exp(ending[:, None, :] - within),
            value_blk,
            precision=lax.Precision.HIGHEST,
        )
        result = jnp.einsum(
            "hid,hde->hie", query_blk * jnp.exp(within), memory, precision=lax.Precision.HIGHEST
        )
        spread = jnp.exp(
            jnp.where(lower_mask, within[:, :, None, :] - within[:, None, :, :], -jnp.inf)
        )
        scores = jnp.einsum(
            "hid,hjd,hijd->hij", query_blk, key_blk, spread, precision=lax.Precision.HIGHEST
        )
        result = result + jnp.einsum(
            "hij,hje->hie", scores, value_blk, precision=lax.Precision.HIGHEST
        )
        reached = query_blk * jnp.exp(within + offset[:, None, :])
        return ((memory_next, offset + ending), (result, reached))

    start_memory = jnp.zeros((head_count, key_dim, values_in.shape[-1]), jnp.float32)
    start_offset = jnp.zeros((head_count, key_dim), jnp.float32)
    (memory, decay_total), (outputs, reached) = lax.scan(
        advance,
        (start_memory, start_offset),
        (blocks(key_in), blocks(values_in), blocks(log_decay), blocks(query_in)),
    )

    def unblock(tensor):
        return jnp.transpose(tensor, (0, 2, 1, 3)).reshape(
            sequence_length, head_count, tensor.shape[-1]
        )

    return (unblock(outputs), unblock(reached), memory, decay_total)


def head_mix(combined, head_norm_gain, output_gate_preact):
    sequence_length, head_count, width = combined.shape
    inverse = lax.rsqrt(jnp.mean(combined * combined, axis=-1, keepdims=True) + EPSILON)
    gate_act = jax.nn.silu(
        output_gate_preact.astype(jnp.float32).reshape(sequence_length, head_count, width)
    )
    weighted = combined * inverse * head_norm_gain.reshape(head_count, width) * gate_act
    return weighted.reshape(sequence_length, head_count * width).astype(jnp.bfloat16)


def row_norm(mid_rows, prenorm_gain):
    wide = mid_rows.astype(jnp.float32)
    inverse = lax.rsqrt(jnp.mean(wide * wide, axis=-1, keepdims=True) + EPSILON)
    return (wide * inverse * prenorm_gain).astype(jnp.bfloat16)


def combine_states(earlier, later):
    decay_early, memory_early = earlier
    decay_late, memory_late = later
    return (decay_early * decay_late, decay_late[:, :, None] * memory_early + memory_late)


def body(
    queries,
    key_projected,
    values,
    output_gate_preact,
    forward_decay_logits,
    backward_decay_logits,
    decay_logit_shift,
    decay_spike_values,
    residual,
    head_norm_gain,
    output_projection,
    prenorm_gain,
    gate_projection,
    up_projection,
    down_projection,
):
    sequence_length = queries.shape[0]
    local_heads = queries.shape[1] // KEY_CHANNELS
    query_f = queries.astype(jnp.float32).reshape(
        sequence_length, local_heads, KEY_CHANNELS
    ) * KEY_CHANNELS ** (-0.5)
    keys_f = key_projected.astype(jnp.float32).reshape(sequence_length, local_heads, KEY_CHANNELS)
    values_f = values.astype(jnp.float32).reshape(sequence_length, local_heads, HEAD_V)
    decay_spikes = jnp.transpose(decay_spike_values)[:, :, None]
    logit_shifts = decay_logit_shift.reshape(2, local_heads, KEY_CHANNELS)
    forward_decay = (
        jax.nn.log_sigmoid(
            forward_decay_logits.astype(jnp.float32).reshape(
                sequence_length, local_heads, KEY_CHANNELS
            )
            + logit_shifts[0]
        )
        / GATE_DENOMINATOR
        + decay_spikes
    )
    backward_decay = (
        jax.nn.log_sigmoid(
            backward_decay_logits.astype(jnp.float32).reshape(
                sequence_length, local_heads, KEY_CHANNELS
            )
            + logit_shifts[1]
        )
        / GATE_DENOMINATOR
        + decay_spikes
    )
    fwd_out, fwd_reach, fwd_memory, fwd_total = block_sweep(
        query_f, keys_f, values_f, forward_decay, BLOCK
    )
    bwd_out, bwd_reach, bwd_memory, bwd_total = block_sweep(
        query_f[::-1], keys_f[::-1], values_f[::-1], backward_decay[::-1], BLOCK
    )
    identity = (jnp.ones_like(fwd_total), jnp.zeros_like(fwd_memory))
    fwd_incoming = entering(
        (jnp.exp(fwd_total), fwd_memory), "sp", combine_states, identity, False
    )[1]
    bwd_incoming = entering((jnp.exp(bwd_total), bwd_memory), "sp", combine_states, identity, True)[
        1
    ]
    fwd_full = fwd_out + jnp.einsum(
        "lhd,hde->lhe", fwd_reach, fwd_incoming, precision=lax.Precision.HIGHEST
    )
    bwd_full = bwd_out + jnp.einsum(
        "lhd,hde->lhe", bwd_reach, bwd_incoming, precision=lax.Precision.HIGHEST
    )
    attended = head_mix(fwd_full + bwd_full[::-1], head_norm_gain, output_gate_preact)
    token_rows = lax.all_to_all(attended, "tp", split_axis=0, concat_axis=1, tiled=True)
    whole_out = lax.all_gather(output_projection, "tp", axis=0, tiled=True)
    projected = jnp.dot(token_rows, whole_out, preferred_element_type=jnp.float32)
    mid_rows = (residual.astype(jnp.float32) + projected).astype(jnp.bfloat16)
    normed = row_norm(mid_rows, prenorm_gain)
    fetched = (
        lax.all_gather(gate_projection, "sp", axis=0, tiled=True),
        lax.all_gather(up_projection, "sp", axis=0, tiled=True),
        lax.all_gather(down_projection, "sp", axis=1, tiled=True),
    )
    gate_full, up_full, down_full = fetched
    piece = lax.all_gather(normed, "tp", axis=0, tiled=True)
    gate_part = jnp.dot(piece, gate_full, preferred_element_type=jnp.float32)
    up_part = jnp.dot(piece, up_full, preferred_element_type=jnp.float32)
    hidden = (jax.nn.silu(gate_part) * up_part).astype(jnp.bfloat16)
    summed = lax.psum_scatter(
        jnp.dot(hidden, down_full, preferred_element_type=jnp.float32).astype(jnp.bfloat16),
        "tp",
        scatter_dimension=0,
        tiled=True,
    ).astype(jnp.float32)
    return (mid_rows.astype(jnp.float32) + 0.5 * summed).astype(jnp.bfloat16)


MESH = pl.DeviceIdType.MESH
PIECES = 5


def log_decay(logits, shift, spike):
    x = logits.astype(F32) + shift
    soft = jnp.minimum(x, 0.0) - jnp.log1p(jnp.exp(-jnp.abs(x)))
    return soft / GATE_DENOMINATOR + spike


def own_states(k_ref, v_ref, fd_ref, bd_ref, shift_ref, spike_ref, within_ref, kd_ref, fwd_ref, bwd_ref):
    tokens, lanes = k_ref.shape
    blocks = tokens // BLOCK
    row = lax.broadcasted_iota(jnp.int32, (2 * BLOCK, 2 * BLOCK), 0)
    col = lax.broadcasted_iota(jnp.int32, (2 * BLOCK, 2 * BLOCK), 1)
    r, c = row % BLOCK, col % BLOCK
    ahead = jnp.where(row < BLOCK, r - c, c - r)
    tri = jnp.where(ahead >= 0, 1.0, 0.0).astype(BF16)
    half = first_head((BLOCK, lanes))
    spikes = jnp.transpose(jnp.concatenate([spike_ref[...]] * 4, axis=0))
    ends = []
    for b in range(blocks):
        at = slice(b * BLOCK, (b + 1) * BLOCK)
        spike = jnp.where(half, spikes[at, 0:1], spikes[at, 1:2])
        parts = [log_decay(ref[at, :], shift_ref[n : n + 1, :], spike) for n, ref in enumerate((fd_ref, bd_ref))]
        d = jnp.concatenate(parts, axis=1)
        hi = d.astype(BF16)
        lo = (d - hi.astype(F32)).astype(BF16)
        both = jnp.dot(tri, jnp.concatenate([hi, lo], axis=0), preferred_element_type=F32)
        fwd, bwd = both[:BLOCK, :lanes], both[BLOCK:, lanes:]
        within_ref[at, :lanes] = fwd
        within_ref[at, lanes:] = bwd
        ends.append((fwd[BLOCK - 1 :, :], bwd[:1, :]))
    zero = jnp.zeros((1, lanes), F32)
    after, before = [zero] * blocks, [zero] * blocks
    for b in range(1, blocks):
        before[b] = before[b - 1] + ends[b - 1][1]
        after[blocks - 1 - b] = after[blocks - b] + ends[blocks - b][0]
    totals = after[0] + ends[0][0], before[-1] + ends[-1][1]
    for b in range(blocks):
        at = slice(b * BLOCK, (b + 1) * BLOCK)
        key = k_ref[at, :].astype(F32)
        kd_ref[at, :lanes] = (key * jnp.exp((ends[b][0] + after[b]) - within_ref[at, :lanes])).astype(BF16)
        kd_ref[at, lanes:] = (key * jnp.exp((ends[b][1] + before[b]) - within_ref[at, lanes:])).astype(BF16)
    full = tn(v_ref[...], kd_ref[...])
    mine = first_head((HEAD_V, lanes))
    for n, ref in enumerate((fwd_ref, bwd_ref)):
        u = full[:, n * lanes : (n + 1) * lanes]
        ref[:HEAD_V, :] = jnp.where(mine, u[:HEAD_V], u[HEAD_V:]).astype(BF16)
        ref[HEAD_V:, :] = jnp.broadcast_to(jnp.exp(totals[n]), (16, lanes)).astype(BF16)


def spread(state):
    mine = first_head(state.shape)
    return jnp.concatenate([jnp.where(mine, state, 0.0), jnp.where(mine, 0.0, state)], axis=0).astype(BF16)


def pack(u):
    top = u[:HEAD_V]
    return jnp.where(first_head(top.shape), top, u[HEAD_V:])


def backward_states(k_ref, v_ref, within_ref, state, held_ref):
    tokens, lanes = k_ref.shape
    for b in reversed(range(tokens // BLOCK)):
        at = slice(b * BLOCK, (b + 1) * BLOCK)
        held_ref[b] = spread(state)
        within = within_ref[at, lanes:]
        end = within[:1, :]
        kd = (k_ref[at, :].astype(F32) * jnp.exp(end - within)).astype(BF16)
        state = state * jnp.exp(end) + pack(tn(v_ref[at, :], kd))


def attend(q_ref, k_ref, v_ref, within_ref, gate_ref, gain_ref, fwd_state, held_ref, out_ref):
    tokens, lanes = k_ref.shape
    row = lax.broadcasted_iota(jnp.int32, (2 * BLOCK, BLOCK), 0) % BLOCK
    col = lax.broadcasted_iota(jnp.int32, (2 * BLOCK, BLOCK), 1)
    half = first_head((BLOCK, lanes))
    for b in range(tokens // BLOCK):
        at = slice(b * BLOCK, (b + 1) * BLOCK)
        query = q_ref[at, :].astype(F32) * KEY_CHANNELS ** (-0.5)
        key = k_ref[at, :].astype(F32)
        value = v_ref[at, :]
        scores, reach = [], []
        for n in range(2):
            within = within_ref[at, n * lanes : (n + 1) * lanes]
            pivot = within[BLOCK // 2 - 1 + n : BLOCK // 2 + n, :]
            near = (query * jnp.exp(within - pivot)).astype(BF16)
            far = (key * jnp.exp(pivot - within)).astype(BF16)
            zero = jnp.zeros_like(near)
            pair = jnp.concatenate([jnp.where(half, near, zero), jnp.where(half, zero, near)], axis=0)
            scores.append(nt(pair, far))
            reach.append((query * jnp.exp(within)).astype(BF16))
        score = (jnp.where(col <= row, scores[0], 0.0) + jnp.where(col >= row, scores[1], 0.0)).astype(BF16)
        states = jnp.concatenate([spread(fwd_state), held_ref[b]], axis=1)
        result = nt(jnp.concatenate(reach, axis=1), states)
        for h in range(2):
            lane = slice(h * HEAD_V, (h + 1) * HEAD_V)
            x = result[:, lane] + jnp.dot(
                score[h * BLOCK : (h + 1) * BLOCK], value[:, lane], preferred_element_type=F32
            )
            inverse = lax.rsqrt(jnp.mean(x * x, axis=-1, keepdims=True) + EPSILON)
            g = gate_ref[at, lane].astype(F32)
            out_ref[at, lane] = (x * inverse * gain_ref[:, lane] * (g * jax.nn.sigmoid(g))).astype(BF16)
        within = within_ref[at, :lanes]
        end = within[BLOCK - 1 :, :]
        kd = (key * jnp.exp(end - within)).astype(BF16)
        fwd_state = fwd_state * jnp.exp(end) + pack(tn(value, kd))


def pick(i, table):
    value = table[0]
    for n, item in enumerate(table[1:], 1):
        value = jnp.where(i == n, item, value)
    return value


def ds(first, size):
    return pl.ds(pl.multiple_of(first, size if size % 128 == 0 else 16), size)


def layer_kernel(
    k_hbm, v_hbm, fd_hbm, bd_hbm, shift_hbm, spike_hbm, q_hbm, gate_hbm, gain_hbm, norm_hbm,
    res_hbm, out_hbm, g_hbm, u_hbm, d_hbm,
    out_ref,
    k_ref, v_ref, fd_ref, bd_ref, shift_ref, spike_ref, q_ref, gate_ref, gain_ref, norm_ref, in_s,
    within, kd, fown, bown, fgot, bgot, fstate, bstate, held, attended, rows, outl, outh, pout, rgot, rxs, rxg, squares, res, mid, acts,
    wgu, wd, hid, part, got, xsend, xgot, esend, egot, erelay,
    loc, st_s, st_r, a2a_s, a2a_r, ow_s, ow_r, rs_s, rs_r, rx_s, rx_r, ag_s, ag_r, ea_s, ea_r, gs, gr, dsd, drv, cr_s, cr_r, xo_s, xo_r,
    eo_s, eo_r, er_s, er_r,
):
    count = lax.axis_size("sp")
    side, place, me = lax.axis_index("grp"), lax.axis_index("sp"), lax.axis_index("tp")
    chip, core = me // 2, me % 2
    tc, tx, td = 2 * chip + 1 - core, 2 * (1 - chip) + core, 2 * (1 - chip) + 1 - core
    upper = place // 2
    e, m, o, oe = 3 * upper, 1 + upper, 2 - upper, 3 - 3 * upper
    middle = place * (count - 1 - place) > 0
    outer = jnp.logical_not(middle)
    own = res.shape[0]
    width = attended.shape[1]
    model = mid.shape[1]
    depth, hidden = g_hbm.shape
    tile = hidden // PIECES
    hr = depth // 2
    dr = hidden // 2
    dw = wd.shape[3]
    chunks = part.shape[1]
    wide = pout.shape[2]
    parts = pout.shape[0]
    nrow = own // 2

    def remote(src, dst, send, recv, **dev):
        return pltpu.make_async_remote_copy(
            src_ref=src, dst_ref=dst, send_sem=send, recv_sem=recv, device_id=dev, device_id_type=MESH
        )

    def slot(source, dev):
        return source - jnp.where(source > dev.get("sp", place), 1, 0)

    def gu(n, source, half, p, local=False, again=False, **dev):
        dst = wgu.at[n, p, ds(source * depth + half * hr, hr), :]
        src = (g_hbm, u_hbm)[n].at[ds(half * hr, hr), ds(p * tile, tile)] if local else dst
        send = gs.at[source, 1 - half if again else half]
        return remote(src, dst, send, gr.at[n, slot(source, dev), half, p], **(dev or dict(sp=o)))

    def dn(source, half, p, r, local=False, again=False, **dev):
        dst = wd.at[source, p, ds(half * dr + r * (dr // 2), dr // 2), :]
        src = d_hbm.at[ds(half * dr + r * (dr // 2), dr // 2), p * dw : (p + 1) * dw] if local else dst
        send = dsd.at[source, 1 - half if again else half]
        return remote(src, dst, send, drv.at[slot(source, dev), half, p, r], **(dev or dict(sp=o)))

    def send_gu(source, half, p, local=False, again=False, **dev):
        for n in range(2):
            gu(n, source, half, p, local, again, **dev).start()

    def take_gu(source, half, p):
        for n in range(2):
            gu(n, source, half, p).wait_recv()

    def relay_one(n, source, p, **dev):
        gu(n, source, side, p).wait_recv()
        gu(n, source, side, p, **dev).start()

    def relay_gu(source, p, **dev):
        for n in range(2):
            relay_one(n, source, p, **dev)

    def send_dn(half, p, **dev):
        for r in range(2):
            dn(place, half, p, r, True, **dev).start()

    def take_dn(source, half, p):
        for r in range(2):
            dn(source, half, p, r).wait_recv()

    def relay_dn(source, p, r, **dev):
        dn(source, side, p, r).wait_recv()
        dn(source, side, p, r, **dev).start()

    def sent(ref, sem):
        remote(ref, ref, sem, sem, sp=o).wait_send()

    def sent_gu(source, half, low, high, again=False):
        at = ds(source * depth + half * hr, hr)
        sent(wgu.at[:, low:high, at, :], gs.at[source, 1 - half if again else half])

    def sent_dn(source, half, low, high):
        sent(wd.at[source, low:high, ds(half * dr, dr), :], dsd.at[source, half])

    def landed(ref, sem):
        remote(ref, ref, sem, sem, sp=o).wait_recv()

    def ow(kind, block, i, dev, local=False):
        half = width // 2
        dst = outh.at[ds(block * width + i * half, half), :]
        src = out_hbm.at[i * half : (i + 1) * half, model // 2 :] if local else dst
        return remote(src, dst, ow_s.at[kind], ow_r.at[i if kind == 0 else 1 + kind], tp=dev)

    def relay_ow(i):
        ow(0, tx, i, tc).wait_recv()
        ow(2, tx, i, tc).start()

    def a2a(block, dev):
        src = attended.at[ds(dev * own, own), :]
        return remote(src, rows.at[:, ds(block * width, width)], a2a_s.at[0], a2a_r.at[block], tp=dev)

    def rs(c, j):
        block = 2 * j + 1 - core
        return remote(pout.at[c, ds(block * own, own), :], rgot.at[c, j], rs_s.at[0], rs_r.at[c], tp=tc)

    def rx(c):
        return remote(rxs.at[c], rxg.at[c], rx_s.at[0], rx_r.at[c], tp=tx)

    def ag(q, kind, block, i, dev):
        at = acts.at[q, ds(block * own + i * nrow, nrow), :]
        return remote(at, at, ag_s.at[q, kind], ag_r.at[q, i if kind == 0 else 1 + kind], tp=dev)

    def to_host(i):
        at = ds(me * own + i * nrow, nrow)
        return remote(acts.at[0, at, :], acts.at[1, at, :], ea_s.at[0], ea_r.at[i], sp=m)

    def gathered(q):
        for kind, block in ((1, tc), (2, td)):
            landed(acts.at[q, ds(block * own, own), :], ag_r.at[q, 1 + kind])

    def state_copy(n, k, dev):
        src, dst = ((fown, fgot), (bown, bgot))[n]
        return remote(src, dst.at[k - 1], st_s.at[n, k - 1], st_r.at[n, k - 1], sp=dev)

    def cr(q, i, j):
        block = 2 * j + 1 - core
        return remote(part.at[q, i, ds(block * own, own), :], got.at[q, i, j], cr_s.at[q], cr_r.at[q, i], tp=tc)

    def xo(q, i):
        return remote(xsend.at[q, i], xgot.at[q, i], xo_s.at[q], xo_r.at[q, i], tp=tx)

    def eo(i, n):
        dst = egot.at[0, i] if n == 0 else erelay.at[i]
        return remote(esend.at[i, n], dst, eo_s.at[n], eo_r.at[i, n], sp=e)

    def er(i):
        return remote(erelay.at[i], egot.at[1, i], er_s.at[0], er_r.at[i], tp=tx)

    own_copies = []
    for p in range(PIECES):
        for n in range(2):
            own_copies.append(
                pltpu.make_async_copy(
                    (g_hbm, u_hbm)[n].at[:, p * tile : (p + 1) * tile],
                    wgu.at[n, p, ds(place * depth, depth), :],
                    loc.at[0],
                )
            )
    for p in range(2):
        own_copies.append(pltpu.make_async_copy(d_hbm.at[:, p * dw : (p + 1) * dw], wd.at[place, p], loc.at[1]))
    own_gu = wgu.at[:, :, ds(place * depth, depth), :]
    own_waits = [
        pltpu.make_async_copy(own_gu, own_gu, loc.at[0]),
        pltpu.make_async_copy(wd.at[place], wd.at[place], loc.at[1]),
    ]
    own_low = pltpu.make_async_copy(out_hbm.at[:, : model // 2], outl, loc.at[2])
    own_high = pltpu.make_async_copy(out_hbm.at[:, model // 2 :], outh.at[ds(me * width, width), :], loc.at[4])
    own_res = pltpu.make_async_copy(res_hbm, res, loc.at[3])

    barrier = pltpu.get_barrier_semaphore()
    friends = [dict(sp=lax.rem(place + k, count)) for k in range(1, count)]
    friends += [dict(grp=1 - side)] + [dict(tp=t) for t in (tc, tx, td)]
    for friend in friends:
        pl.semaphore_signal(barrier, inc=1, device_id=friend, device_id_type=MESH)
    loads = [
        pltpu.make_async_copy(src, dst, in_s.at[n])
        for n, (src, dst) in enumerate(
            (
                (k_hbm, k_ref),
                (v_hbm, v_ref),
                (fd_hbm, fd_ref),
                (bd_hbm, bd_ref),
                (shift_hbm, shift_ref),
                (spike_hbm, spike_ref),
                (q_hbm, q_ref),
                (gate_hbm, gate_ref),
                (gain_hbm, gain_ref),
                (norm_hbm, norm_ref),
            )
        )
    ]
    for load in loads:
        load.start()
    own_low.start()
    own_high.start()
    own_res.start()
    for load in loads[:6]:
        load.wait()
    own_states(k_ref, v_ref, fd_ref, bd_ref, shift_ref, spike_ref, within, kd, fown, bown)
    pl.semaphore_wait(barrier, len(friends))

    for k in range(1, count):

        @pl.when(place + k < count)
        def _(k=k):
            state_copy(0, k, place + k).start()

        @pl.when(place >= k)
        def _(k=k):
            state_copy(1, k, place - k).start()

    @pl.when(middle)
    def _():
        for p in range(PIECES):
            send_gu(place, side, p, True, sp=o)

    @pl.when(outer)
    def _():
        for p in range(PIECES):
            send_gu(place, side, p, True, sp=m)

    for i in range(2):
        ow(0, me, i, tx, True).start()
        ow(1, me, i, tc, True).start()

    @pl.when(middle)
    def _():
        for copy in own_copies:
            copy.start()

    for load in loads[6:]:
        load.wait()
    fstate[...] = jnp.zeros_like(fstate)
    bstate[...] = jnp.zeros_like(bstate)
    for k in reversed(range(1, count)):

        @pl.when(place >= k)
        def _(k=k):
            state_copy(0, k, place).wait_recv()
            decay = fgot[k - 1, HEAD_V : HEAD_V + 1, :].astype(F32)
            fstate[...] = fstate[...] * decay + fgot[k - 1, :HEAD_V, :].astype(F32)

        @pl.when(place + k < count)
        def _(k=k):
            state_copy(1, k, place).wait_recv()
            decay = bgot[k - 1, HEAD_V : HEAD_V + 1, :].astype(F32)
            bstate[...] = bstate[...] * decay + bgot[k - 1, :HEAD_V, :].astype(F32)

    backward_states(k_ref, v_ref, within, bstate[...], held)
    attend(q_ref, k_ref, v_ref, within, gate_ref, gain_ref, fstate[...], held, attended)
    others = (tx, td, tc)
    for t in others:
        a2a(me, t).start()
    rows[:, ds(me * width, width)] = attended[ds(me * own, own), :]
    own_low.wait()
    for c in range(parts):
        at = slice(c * wide, (c + 1) * wide)
        pout[c] = jnp.dot(attended[...], outl[:, at], preferred_element_type=F32).astype(BF16)
        for j in range(2):
            rs(c, j).start()
    @pl.when(middle)
    def _():
        relay_one(0, o, 0, grp=1 - side)

    relay_ow(0)
    for c in range(parts):
        landed(rgot.at[c], rs_r.at[c])
        rxs[c] = (pout[c, ds(tx * own, own), :].astype(F32) + rgot[c, 1 - chip].astype(F32)).astype(BF16)
        rx(c).start()

    def mix(at, projected):
        mixed = (res[:, at].astype(F32) + projected).astype(BF16)
        mid[:, at] = mixed
        mixed = mixed.astype(F32)
        return jnp.sum(mixed * mixed, axis=-1, keepdims=True)

    @pl.when(middle)
    def _():
        relay_one(1, o, 0, grp=1 - side)
        relay_gu(e, 0, sp=o)

    relay_ow(1)

    @pl.when(middle)
    def _():
        relay_gu(o, 1, grp=1 - side)
        relay_gu(e, 1, sp=o)

    for t in others:
        a2a(t, t).wait_recv()
    for kind, t in ((1, tc), (2, td)):
        landed(outh.at[ds(t * width, width), :], ow_r.at[1 + kind])
    own_high.wait()
    own_res.wait()
    total = jnp.zeros((own, 1), F32)
    for n in range(parts):
        high = slice(n * wide, (n + 1) * wide)
        projected = jnp.dot(rows[...], outh[:, high], preferred_element_type=F32)
        total += mix(slice(model // 2 + n * wide, model // 2 + (n + 1) * wide), projected)
    squares[...] = jnp.broadcast_to(total, squares.shape)

    @pl.when(middle)
    def _():
        relay_gu(o, 2, grp=1 - side)
        relay_gu(e, 2, sp=o)

    total = squares[:, :1]
    for n in range(parts):
        rx(n).wait_recv()
        projected = pout[n, ds(me * own, own), :].astype(F32) + rgot[n, chip].astype(F32) + rxg[n].astype(F32)
        total += mix(slice(n * wide, (n + 1) * wide), projected)
    inverse = lax.rsqrt(total / model + EPSILON)
    for n in range(2 * parts):
        at = slice(n * wide, (n + 1) * wide)
        acts[0, ds(me * own, own), at] = (mid[:, at].astype(F32) * inverse * norm_ref[:, at]).astype(BF16)

    direct = (1, 1, 1, 0, 0, 0, 0, 1)
    whole = [i for i, d in enumerate(direct) if d]

    def straight(i):
        return direct[i] if isinstance(i, int) else pick(i, direct)

    sources = (m, m, o, o, e, oe, e, oe)
    sides = (0, 1, 0, 1, 0, 0, 1, 1)

    @pl.when(middle)
    def _():
        for i in range(2):
            ag(0, 0, me, i, tx).start()
            ag(0, 1, me, i, tc).start()
        for p in range(3, PIECES):
            relay_gu(o, p, grp=1 - side)
            relay_gu(e, p, sp=o)
        send_gu(e, side, 1, again=True, grp=1 - side)
        for p in range(2):
            send_dn(side, p, sp=o)
        send_dn(1 - side, 1, sp=o)
        for copy in own_waits:
            copy.wait()

        def relay_own(i):
            ag(0, 0, tx, i, tc).wait_recv()
            ag(0, 2, tx, i, tc).start()

        def relay_hosted(i):
            to_host(i).wait_recv()
            ag(1, 0, me, i, tx).start()
            ag(1, 1, me, i, tc).start()

        def pass_hosted(i):
            ag(1, 0, tx, i, tc).wait_recv()
            ag(1, 2, tx, i, tc).start()

        relay_gu(oe, 0, grp=1 - side)
        relay_own(0)
        relay_hosted(0)
        relay_gu(oe, 1, grp=1 - side)
        relay_own(1)
        relay_gu(oe, 2, grp=1 - side)
        relay_hosted(1)

        order = [(0, 0), (0, 1), (0, 2), (1, 0), (0, 3), (1, 1), (1, 2), (1, 3), (0, 4), (1, 4)]

        def fold(i, q):
            landed(got.at[q, i], cr_r.at[q, i])

            def both(block, j):
                return part[q, i, ds(block * own, own), :].astype(F32) + got[q, i, j].astype(F32)

            @pl.when(jnp.logical_or(q == 0, straight(i) == 0))
            def _():
                xsend[q, i] = both(tx, 1 - chip).astype(BF16)
                xo(q, i).start()

            @pl.when(jnp.logical_and(q == 1, straight(i) == 1))
            def _():
                esend[i, 1] = both(tx, 1 - chip).astype(BF16)
                eo(i, 1).start()
                esend[i, 0] = both(me, chip).astype(BF16)
                eo(i, 0).start()

        def push(i):
            if direct[i]:
                return
            xo(1, i).wait_recv()
            mixed = part[1, i, ds(me * own, own), :].astype(F32) + got[1, i, chip].astype(F32)
            esend[i, 0] = (mixed + xgot[1, i].astype(F32)).astype(BF16)
            eo(i, 0).start()

        def product(q, i):
            weight = wd[pick(i, sources), pick(i, sides)]
            part[q, i] = jnp.dot(hid[q], weight, preferred_element_type=F32).astype(BF16)
            for j in range(2):
                cr(q, i, j).start()

        def first(i, carry):
            q, j = pick(i, [a for a, _ in order]), pick(i, [b for _, b in order])

            @pl.when(i == 0)
            def _():
                gathered(0)

            @pl.when(i == 1)
            def _():
                pass_hosted(0)
                relay_gu(oe, 3, grp=1 - side)

            @pl.when(i == 2)
            def _():
                relay_gu(oe, 4, grp=1 - side)
                pass_hosted(1)

            @pl.when(i == 3)
            def _():
                gathered(1)

            @pl.when(i == 5)
            def _():
                for r in range(2):
                    relay_dn(o, 0, r, grp=1 - side)

            @pl.when(i == 9)
            def _():
                relay_dn(e, 0, 0, sp=o)

            @pl.when(q == 0)
            def _():
                for source in (o, oe, e):
                    take_gu(source, 1 - side, j)

            g = jnp.dot(acts[q], wgu[0, j], preferred_element_type=F32)
            u = jnp.dot(acts[q], wgu[1, j], preferred_element_type=F32)
            hid[q, :, ds(j * tile, tile)] = (g * jax.nn.sigmoid(g) * u).astype(BF16)
            return carry

        lax.fori_loop(0, len(order), first, 0)

        def second(s, carry):
            i, q = s // 2, 1 - s % 2

            @pl.when(s == 0)
            def _():
                relay_dn(e, 0, 1, sp=o)
                dn(e, side, 0, 1, again=True, grp=1 - side).start()

            @pl.when(s == 4)
            def _():
                take_dn(o, 1 - side, 0)

            @pl.when(s == 5)
            def _():
                relay_dn(e, 1, 0, sp=o)

            @pl.when(s == 6)
            def _():
                take_dn(o, side, 1)
                take_dn(o, 1 - side, 1)

            @pl.when(s == 8)
            def _():
                relay_dn(oe, 0, 0, grp=1 - side)
                fold(3, 1)
                relay_dn(e, 1, 1, sp=o)
                fold(3, 0)
                relay_dn(oe, 0, 1, grp=1 - side)
                push(2)
                take_dn(e, 1 - side, 0)

            @pl.when(s == 10)
            def _():
                push(3)
                relay_dn(oe, 1, 0, grp=1 - side)
                fold(4, 1)
                fold(4, 0)
                take_dn(oe, 1 - side, 0)

            @pl.when(s == 12)
            def _():
                relay_dn(oe, 1, 1, grp=1 - side)
                fold(5, 1)
                push(4)
                take_dn(e, 1 - side, 1)

            @pl.when(s == 14)
            def _():
                fold(6, 1)
                push(5)
                take_dn(oe, 1 - side, 1)

            product(q, i)

            @pl.when((s > 1) & (s < 8))
            def _():
                fold(i - 1, q)

            @pl.when(s == 14)
            def _():
                fold(chunks - 3, 0)

            return carry

        lax.fori_loop(0, 2 * chunks, second, 0)
        fold(chunks - 1, 1)
        fold(chunks - 2, 0)
        fold(chunks - 1, 0)
        push(chunks - 2)

        for i in range(chunks):
            xo(0, i).wait_recv()
            at = ds((2 * sources[i] + sides[i]) * dw, dw)
            total = part[0, i, ds(me * own, own), :].astype(F32) + got[0, i, chip].astype(F32) + xgot[0, i].astype(F32)
            out_ref[:, at] = (mid[:, at].astype(F32) + 0.5 * total).astype(BF16)

        for source in (place, e, o, oe):
            sent_gu(source, side, 0, PIECES)
        sent_gu(e, side, 0, 1, again=True)
        sent(wd.at[e, 0, : dr // 2, :], dsd.at[e, 1 - side])
        for source in (place, e, oe):
            sent_dn(source, side, 0, 2)
        sent_dn(o, side, 0, 1)
        sent_dn(place, 1 - side, 1, 2)
        for q in range(2):
            for kind in range(3):
                sent(acts.at[q, ds(me * own, own), :], ag_s.at[q, kind])
            sent(got.at[q], cr_s.at[q])
        sent(xsend.at[0], xo_s.at[0])
        sent(xsend.at[1, : chunks - len(whole)], xo_s.at[1])
        sent(esend.at[:, 0], eo_s.at[0])
        sent(esend.at[: len(whole), 1], eo_s.at[1])

    @pl.when(outer)
    def _():
        for i in range(2):
            to_host(i).start()
        for p in (0, 2, 3, 4):
            send_gu(place, 1 - side, p, True, sp=m)
        for p in range(2):
            send_dn(side, p, sp=m)
        dn(place, 1 - side, 0, 0, True, sp=m).start()
        send_dn(1 - side, 1, sp=m)

        def finish(i):
            eo(i, 0).wait_recv()
            total = egot[0, i].astype(F32)
            if direct[i]:
                er(i).wait_recv()
                total += egot[1, i].astype(F32)
            at = ds((2 * sources[i] + sides[i]) * dw, dw)
            out_ref[:, at] = (mid[:, at].astype(F32) + 0.5 * total).astype(BF16)

        for i in range(chunks):
            if direct[i]:
                eo(i, 1).wait_recv()
                er(i).start()
            if i > 1:
                finish(i - 2)
        finish(chunks - 2)
        finish(chunks - 1)
        sent(acts.at[0, ds(me * own, own), :], ea_s.at[0])
        sent_gu(place, side, 0, PIECES)
        sent_gu(place, 1 - side, 0, PIECES - 1)
        sent_dn(place, side, 0, 2)
        sent(wd.at[place, 0, : dr + dr // 2, :], dsd.at[place, 1 - side])
        sent(erelay.at[: len(whole)], er_s.at[0])

    for k in range(1, count):

        @pl.when(place + k < count)
        def _(k=k):
            state_copy(0, k, place).wait_send()

        @pl.when(place >= k)
        def _(k=k):
            state_copy(1, k, place).wait_send()

    sent(rows.at[:, : 3 * width], a2a_s.at[0])
    for kind in range(3):
        sent(outh.at[ds(me * width, width), :], ow_s.at[kind])
    sent(rgot, rs_s.at[0])
    sent(rxs, rx_s.at[0])


def fast_body(
    queries,
    key_projected,
    values,
    output_gate_preact,
    forward_decay_logits,
    backward_decay_logits,
    decay_logit_shift,
    decay_spike_values,
    residual,
    head_norm_gain,
    output_projection,
    prenorm_gain,
    gate_projection,
    up_projection,
    down_projection,
):
    count = lax.axis_size("sp")
    tokens, lanes = queries.shape
    width = values.shape[1]
    own, model = residual.shape
    depth, hidden = gate_projection.shape
    dw = down_projection.shape[1] // 2
    chunks = 2 * count
    blocks = tokens // BLOCK
    dma = lambda *shape: pltpu.SemaphoreType.DMA(shape)
    state = (HEAD_V + 16, lanes)
    V = pltpu.VMEM
    scratch = [
        V((tokens, lanes), BF16),
        V((tokens, width), BF16),
        V((tokens, lanes), BF16),
        V((tokens, lanes), BF16),
        V(decay_logit_shift.shape, F32),
        V(decay_spike_values.shape, F32),
        V((tokens, lanes), BF16),
        V((tokens, width), BF16),
        V((1, width), F32),
        V((1, model), F32),
        dma(10),
        V((tokens, 2 * lanes), F32),
        V((tokens, 2 * lanes), BF16),
        V(state, BF16),
        V(state, BF16),
        V((count - 1,) + state, BF16),
        V((count - 1,) + state, BF16),
        V((HEAD_V, lanes), F32),
        V((HEAD_V, lanes), F32),
        V((blocks, 2 * HEAD_V, lanes), BF16),
        V((tokens, width), BF16),
        V((own, tokens // own * width), BF16),
        V((width, model // 2), BF16),
        V((tokens // own * width, model // 2), BF16),
        V((2, tokens, model // 4), BF16),
        V((2, 2, own, model // 4), BF16),
        V((2, own, model // 4), BF16),
        V((2, own, model // 4), BF16),
        V((own, 128), F32),
        V((own, model), BF16),
        V((own, model), BF16),
        V((2, tokens, model), BF16),
        V((2, PIECES, model, hidden // PIECES), BF16),
        V((count, 2, hidden, dw), BF16),
        V((2, tokens, hidden), BF16),
        V((2, chunks, tokens, dw), BF16),
        V((2, chunks, 2, own, dw), BF16),
        V((2, chunks, own, dw), BF16),
        V((2, chunks, own, dw), BF16),
        V((chunks, 2, own, dw), BF16),
        V((2, chunks, own, dw), BF16),
        V((chunks, own, dw), BF16),
        dma(5),
        dma(2, count - 1),
        dma(2, count - 1),
        dma(1),
        dma(tokens // own),
        dma(3),
        dma(4),
        dma(1),
        dma(2),
        dma(1),
        dma(2),
        dma(2, 3),
        dma(2, 4),
        dma(1),
        dma(2),
        dma(count, 2),
        dma(2, count - 1, 2, PIECES),
        dma(count, 2),
        dma(count - 1, 2, 2, 2),
        dma(2),
        dma(2, chunks),
        dma(2),
        dma(2, chunks),
        dma(2),
        dma(chunks, 2),
        dma(1),
        dma(chunks),
    ]
    anywhere = pl.BlockSpec(memory_space=pl.ANY)
    return pl.pallas_call(
        layer_kernel,
        out_shape=pltpu.MemorySpace.VMEM((own, model), BF16),
        in_specs=[anywhere] * 15,
        out_specs=VMEM,
        scratch_shapes=scratch,
        compiler_params=pltpu.CompilerParams(
            collective_id=0, has_side_effects=True, vmem_limit_bytes=61000000
        ),
        cost_estimate=cost(3 * 10**10, 3 * 10**7),
        name="layer",
    )(
        key_projected,
        values,
        forward_decay_logits,
        backward_decay_logits,
        decay_logit_shift,
        decay_spike_values,
        queries,
        output_gate_preact,
        head_norm_gain[None, :],
        prenorm_gain[None, :],
        residual,
        output_projection,
        gate_projection,
        up_projection,
        down_projection,
    )


def solution(mesh):
    in_specs = (
        P(("grp", "sp"), "tp"),
        P(("grp", "sp"), "tp"),
        P(("grp", "sp"), "tp"),
        P(("grp", "sp"), "tp"),
        P(("grp", "sp"), "tp"),
        P(("grp", "sp"), "tp"),
        P(None, "tp"),
        P("tp", ("grp", "sp")),
        P(("grp", "sp", "tp"), None),
        P("tp"),
        P("tp", None),
        P(),
        P("sp", "tp"),
        P("sp", "tp"),
        P("tp", "sp"),
    )
    out_specs = P(("grp", "sp", "tp"), None)

    def run(*args):
        lanes = args[0].shape[1]
        sizes = (mesh.shape["grp"], mesh.shape["sp"], mesh.shape["tp"])
        fits = lanes == 2 * KEY_CHANNELS and sizes == (2, 4, 4)
        return fast_body(*args) if fits else body(*args)

    return jax.shard_map(run, mesh=mesh, in_specs=in_specs, out_specs=out_specs, check_vma=False)
```
